512 devices in a mesh: sp: 32 (over z, x), tp: 16 (over y, core).
Axes of the slice: x: 4, y: 8, z: 8, core: 2. Of those that a mesh axis runs over, the one named last changes fastest.
Arguments:
- skip_stream_entering: bfloat16 [4096, 2048], P('sp', 'tp'), may hold values from -24 to 24
- unfiltered_channel_feed: bfloat16 [4096, 2048], P('sp', 'tp'), may hold values from -6 to 6
- unfiltered_state_entry: bfloat16 [4096, 2048], P('sp', 'tp'), may hold values from -6 to 6
- unfiltered_state_exit: bfloat16 [4096, 2048], P('sp', 'tp'), may hold values from -6 to 6
- final_valve_preactivation: bfloat16 [4096, 2048], P('sp', 'tp'), may hold values from -6 to 6
- increment_preactivation: float32 [2, 32, 4096], P(None, 'tp', 'sp'), may hold values from -8 to 8
- summed_attenuation_both_ways: float32 [2, 32, 4096], P(None, 'tp', 'sp'), may hold values from -0.7 to 0, as said below
- channel_fading_speed: float32 [2, 32], P(None, 'tp'), may hold values from 4.8828125e-05 to 0.03, as said below
- channel_feed_filter: float32 [5, 2048], P(None, 'tp'), may hold values from -2.5 to 2.5
- state_entry_filter: float32 [5, 2048], P(None, 'tp'), may hold values from -2.5 to 2.5
- state_exit_filter: float32 [5, 2048], P(None, 'tp'), may hold values from -2.5 to 2.5
- clustered_rescale_factor: float32 [2048], P('tp'), may hold values from 0.1 to 1.9
- final_projection_weights: bfloat16 [2048, 2048], P(None, 'tp'), may hold values from -0.125 to 0.125
- specialist_rescale_factor: float32 [2048], replicated, may hold values from 0.1 to 1.9
- item_specialist_couple: int32 [4096, 2], P('sp'), may hold values from 0 to 31, all different within a row; in each aligned block of 128 rows (0 to 127, 128 to 255, ...) at most 16 rows name the same one
- selected_cluster_likelihood: float32 [4096], P('sp'), may hold values from 0.3 to 1
- selected_twin_scores_raw: float32 [4096, 2], P('sp'), may hold values from -6 to 6
- specialist_gating_weights: bfloat16 [32, 2048, 4096], P('sp', None, 'tp'), may hold values from -0.125 to 0.125
- specialist_raising_weights: bfloat16 [32, 2048, 4096], P('sp', None, 'tp'), may hold values from -0.125 to 0.125
- specialist_lowering_weights: bfloat16 [32, 4096, 2048], P('sp', 'tp'), may hold values from -0.09375 to 0.09375
Outputs:
- layer_out: bfloat16 [4096, 2048], P('sp', 'tp')
The draws below stay inside these ranges and needn't reach their ends.
Inputs may be any that keep to these rules, and one draw needn't show every extreme that they name: For every head, dt times channel_fading_speed at the rate of the draw sets how far a state is carried; summed_attenuation_both_ways holds a few sharp losses of state. `summed_attenuation_both_ways`: mostly zero. `item_specialist_couple`: the two experts of a row differ. Among the rows of one index of sp (aligned blocks of 128 rows) no expert is named by more than 16 rows, a bound that some expert reaches in some blocks.
All inputs are finite; a program needn't handle non-finite values.
Results may differ from the reference program's by a relative error of at most 0.0095.
Values may be sent and summed in bfloat16 or wider, within the bound.
No kernel may reach another device: no remote copies, remote signals or barrier semaphores. Data moves between devices by JAX's collectives and lax.ppermute only.
A program may use at most 64 MiB of HBM per device.

```python
import math
import jax
import jax.numpy as jnp
import numpy as np
from jax import lax

D = 2048
HEADS = 32
HD = 64
GROUPS = 16
NS = 128
CONV = 5
D_EXPERT = 4096
TOP = 2
TOK_DEV = 128
TOKENS = 4096
INNER = 2048
EXPERTS = 32
CAP = 16
N_TP = 16


def draw_channel_fading_speed(key, part):
    uniform_part = jax.random.uniform(key, (2, HEADS), jnp.float32)
    lowest = 0.2 / TOKENS
    highest = 0.03
    return jnp.exp(math.log(lowest) + uniform_part * (math.log(highest) - math.log(lowest)))


def draw_increment_preactivation(key, part):
    first_key, second_key = jax.random.split(key)
    base = jax.random.normal(first_key, (2, HEADS, TOKENS), jnp.float32)
    offsets = jax.random.uniform(second_key, (2, 1, TOKENS // TOK_DEV), jnp.float32, -1.0, 1.0)
    offsets = jnp.repeat(offsets, TOK_DEV, axis=2)
    values = base + offsets
    return jnp.clip(values, -8.0, 8.0)


def draw_summed_attenuation_both_ways(key, part):
    first_key, second_key = jax.random.split(key)
    chosen = jax.random.randint(first_key, (2, HEADS, TOKENS), 0, TOKENS) < 3
    amount = jax.random.uniform(second_key, (2, HEADS, TOKENS), jnp.float32, 0.22, 0.69)
    return jnp.where(chosen, -amount, 0.0)


def draw_skip_stream_entering(key, part):
    first_key, second_key = jax.random.split(key, 2)
    base = jax.random.normal(first_key, (TOKENS, D), jnp.float32)
    columns = jnp.exp(math.log(4.0) * jnp.arange(D, dtype=jnp.float32) / D)
    row_scale = jax.random.uniform(second_key, (TOKENS, 1), jnp.float32, 0.6, 1.6)
    values = base * row_scale * columns
    return jnp.clip(values, -24.0, 24.0).astype(jnp.bfloat16)


def block_levels(key, extent, cuts, low, top_value):
    gain, own = 1.0, jax.random.fold_in(key, 6)
    for axis_at, blocks in cuts:
        heights = jnp.exp(jax.random.uniform(jax.random.fold_in(own, axis_at), (blocks,), jnp.float32, low / len(cuts), top_value / len(cuts)))
        gain = gain * jnp.repeat(heights, extent[axis_at] // blocks).reshape([-1 if axis == axis_at else 1 for axis in range(len(extent))])
    return gain


def deal_out(key, own, number, rows, count, top, bound, lean):
    order = jax.random.permutation(key, count)
    packed, ordinary = portions_of(count, rows * top, bound, lean, True), portions_of(count, rows * top, bound, lean, False)
    places = jnp.arange(count)

    def named(tallies, rotation):
        used = int((tallies > 0).sum())
        fixed = max(1, used // 4)
        shifted = fixed + (places - fixed + rotation * (used - fixed)) % max(1, count - fixed)
        return jnp.zeros((count,), jnp.int32).at[order[jnp.where(places < fixed, places, shifted)]].set(jnp.asarray(tallies, jnp.int32))

    tallies = jnp.where(number % 4 == 0, named(packed, number // 4), named(ordinary, number - number // 4 - 1))
    mixed = jax.random.permutation(jax.random.fold_in(own, 3), count)
    source_of, receiver = mixed[0:count // 2 * 2:2], mixed[1:count // 2 * 2:2]
    room = jnp.minimum(tallies[source_of] - 1, bound - tallies[receiver]) // 2
    room = jnp.where((source_of == order[0]) | (receiver == order[0]) | (tallies[receiver] == 0), 0, jnp.maximum(room, 0))
    shifted = jax.random.randint(jax.random.fold_in(own, 4), (count // 2,), 0, 1 << 20) % (room + 1)
    tallies = tallies.at[source_of].add(-shifted).at[receiver].add(shifted)
    labels = jnp.searchsorted(jnp.cumsum(tallies), jnp.arange(rows * top), side="right").astype(jnp.int32)
    table = labels.reshape(top, rows).T
    table = table[jax.random.permutation(jax.random.fold_in(own, 1), rows)]
    rotation = jax.random.randint(jax.random.fold_in(own, 2), (rows, 1), 0, top)
    return jnp.take_along_axis(table, (jnp.arange(top)[None, :] + rotation) % top, axis=1)


def portions_of(number_of, total, reach, skew, full):
    loads = [(1 << 20) // math.isqrt(grade ** skew) + 1 for grade in range(1, number_of + 1)]
    largest = reach if full else min(reach, max(-(-total // number_of), total * loads[0] // sum(loads)))
    least = 1 if total - largest >= number_of - 1 else 0
    counts, surplus = [largest] + [least] * (number_of - 1), total - largest - least * (number_of - 1)
    while surplus > 0:
        free = [i for i in range(1, number_of) if counts[i] < largest] or [i for i in range(1, number_of) if counts[i] < reach]
        whole, budget = sum([loads[i] for i in free]), surplus
        for i in free:
            more = min(reach - counts[i], max(1, budget * loads[i] // whole), surplus)
            counts[i] = counts[i] + more
            surplus = surplus - more
    return np.array(counts)


def noise(rng, shape, deviation, most, cuts=(), held_as=jnp.bfloat16):
    values = deviation * jax.random.normal(rng, shape, jnp.float32)
    if cuts:
        values = values * block_levels(rng, shape, cuts, -0.22, 0.18)
    return jnp.clip(values, -most, most).astype(held_as)


def setup_inputs(seed: int = 0) -> dict:
    key_of = jax.random.split(jax.random.key(seed), 21)
    skip_stream_entering = draw_skip_stream_entering(jax.random.fold_in(key_of[20], 71), 0)
    unfiltered_channel_feed = noise(key_of[1], (TOKENS, INNER), 1.0, 6.0, ((0, 32), (1, 16)))
    unfiltered_state_entry = noise(key_of[2], (TOKENS, GROUPS * NS), 1.0, 6.0, ((0, 32), (1, 16)))
    unfiltered_state_exit = noise(key_of[3], (TOKENS, GROUPS * NS), 1.0, 6.0, ((0, 32), (1, 16)))
    final_valve_preactivation = noise(key_of[4], (TOKENS, INNER), 1.0, 6.0, ((0, 32), (1, 16)))
    increment_preactivation = draw_increment_preactivation(jax.random.fold_in(key_of[20], 71), 0)
    summed_attenuation_both_ways = draw_summed_attenuation_both_ways(jax.random.fold_in(key_of[20], 71), 0)
    channel_fading_speed = draw_channel_fading_speed(jax.random.fold_in(key_of[20], 71), 0)
    channel_feed_filter = noise(key_of[8], (CONV, INNER), CONV ** -0.5, 2.5, ((1, 16),), jnp.float32)
    state_entry_filter = noise(key_of[9], (CONV, GROUPS * NS), CONV ** -0.5, 2.5, ((1, 16),), jnp.float32)
    state_exit_filter = noise(key_of[10], (CONV, GROUPS * NS), CONV ** -0.5, 2.5, ((1, 16),), jnp.float32)
    clustered_rescale_factor = jnp.clip(1.0 + 0.18 * jax.random.normal(key_of[11], (INNER,), jnp.float32), 0.1, 1.9)
    final_projection_weights = noise(key_of[12], (INNER, D), INNER ** -0.5, 0.125, ((1, 16),))
    specialist_rescale_factor = jnp.clip(1.0 + 0.18 * jax.random.normal(key_of[13], (D,), jnp.float32), 0.1, 1.9)
    item_specialist_couple_keys = jax.random.split(jax.random.fold_in(key_of[14], 1), TOKENS // TOK_DEV)
    item_specialist_couple_turns = jax.random.permutation(jax.random.fold_in(key_of[14], 3), TOKENS // TOK_DEV)
    item_specialist_couple = jax.vmap(lambda own, number: deal_out(jax.random.fold_in(key_of[14], 2), own, number, TOK_DEV, EXPERTS, TOP, CAP, 1))(item_specialist_couple_keys, item_specialist_couple_turns).reshape((TOKENS, TOP))
    selected_cluster_likelihood = jnp.clip(0.3 + 0.7 * jax.random.uniform(key_of[15], (TOKENS,), jnp.float32) ** block_levels(key_of[15], (TOKENS,), ((0, 32),), -0.2, 0.2), 0.3, 1.0)
    selected_twin_scores_raw = noise(key_of[16], (TOKENS, TOP), 1.5, 6.0, ((0, 32),), jnp.float32)
    specialist_gating_weights = noise(key_of[17], (EXPERTS, D, D_EXPERT), D ** -0.5, 0.125, ((0, 32), (2, 16)))
    specialist_raising_weights = noise(key_of[18], (EXPERTS, D, D_EXPERT), D ** -0.5, 0.125, ((0, 32), (2, 16)))
    specialist_lowering_weights = noise(key_of[19], (EXPERTS, D_EXPERT, D), D_EXPERT ** -0.5, 0.09375, ((0, 32), (1, 16)))
    return {"skip_stream_entering": skip_stream_entering, "unfiltered_channel_feed": unfiltered_channel_feed, "unfiltered_state_entry": unfiltered_state_entry, "unfiltered_state_exit": unfiltered_state_exit, "final_valve_preactivation": final_valve_preactivation, "increment_preactivation": increment_preactivation, "summed_attenuation_both_ways": summed_attenuation_both_ways, "channel_fading_speed": channel_fading_speed, "channel_feed_filter": channel_feed_filter, "state_entry_filter": state_entry_filter, "state_exit_filter": state_exit_filter, "clustered_rescale_factor": clustered_rescale_factor, "final_projection_weights": final_projection_weights, "specialist_rescale_factor": specialist_rescale_factor, "item_specialist_couple": item_specialist_couple, "selected_cluster_likelihood": selected_cluster_likelihood, "selected_twin_scores_raw": selected_twin_scores_raw, "specialist_gating_weights": specialist_gating_weights, "specialist_raising_weights": specialist_raising_weights, "specialist_lowering_weights": specialist_lowering_weights}


HIGHEST = lax.Precision.HIGHEST
group_eps = 1e-05
stream_eps = 1e-06

def conv_silu(values, kernel):
    tap_count = kernel.shape[0]
    half_taps = tap_count // 2
    length = values.shape[0]
    padded = jnp.pad(values.astype(jnp.float32), ((half_taps, half_taps), (0, 0)))
    summed = jnp.zeros(values.shape, jnp.float32)
    for offset in range(tap_count):
        summed = summed + kernel[offset].astype(jnp.float32) * padded[offset:offset + length]
    return jax.nn.silu(summed).astype(jnp.bfloat16)

def block_parts(x_block, b_block, c_block, step_f, step_b, log_f, log_b):
    head_count = x_block.shape[1]
    group_count = b_block.shape[1]
    per_group = head_count // group_count
    length = x_block.shape[0]
    group_scores = jnp.einsum('tgn,sgn->gts', c_block, b_block, precision=HIGHEST)
    scores = jnp.repeat(group_scores, per_group, axis=0)
    b_head = jnp.repeat(b_block, per_group, axis=1)
    c_head = jnp.repeat(c_block, per_group, axis=1)
    forward = jnp.cumsum(log_f, axis=1)
    backward = jnp.flip(jnp.cumsum(jnp.flip(log_b, 1), axis=1), 1)
    row_index = lax.broadcasted_iota(jnp.int32, (length, length), 0)
    col_index = lax.broadcasted_iota(jnp.int32, (length, length), 1)
    lower_mask = (col_index <= row_index)[None]
    upper_mask = (col_index >= row_index)[None]
    decay_fwd = jnp.where(lower_mask, jnp.exp(jnp.minimum(forward[:, :, None] - forward[:, None, :], 0.0)), 0.0)
    decay_bwd = jnp.where(upper_mask, jnp.exp(jnp.minimum(backward[:, :, None] - backward[:, None, :], 0.0)), 0.0)
    mixing = scores * (decay_fwd * step_f[:, None, :] + decay_bwd * step_b[:, None, :])
    within = jnp.einsum('hts,shp->thp', mixing, x_block, precision=HIGHEST)
    weight_fwd = jnp.exp(forward[:, -1:] - forward) * step_f
    weight_bwd = jnp.exp(backward[:, :1] - backward) * step_b
    state_fwd = jnp.einsum('hs,shp,shn->hpn', weight_fwd, x_block, b_head, precision=HIGHEST)
    state_bwd = jnp.einsum('hs,shp,shn->hpn', weight_bwd, x_block, b_head, precision=HIGHEST)
    return (within, state_fwd, state_bwd, forward[:, -1], backward[:, 0], jnp.exp(forward), jnp.exp(backward), c_head)

def read_state(c_head, factor, state):
    return jnp.einsum('thn,hpn->thp', c_head, state, precision=HIGHEST) * jnp.transpose(factor)[:, :, None]

def carry_step(carried, items):
    state, total = items
    return (carried * jnp.exp(total)[:, None, None] + state, carried)

def reference(skip_stream_entering, unfiltered_channel_feed, unfiltered_state_entry, unfiltered_state_exit, final_valve_preactivation, increment_preactivation, summed_attenuation_both_ways, channel_fading_speed, channel_feed_filter, state_entry_filter, state_exit_filter, clustered_rescale_factor, final_projection_weights, specialist_rescale_factor, item_specialist_couple, selected_cluster_likelihood, selected_twin_scores_raw, specialist_gating_weights, specialist_raising_weights, specialist_lowering_weights):
    length = skip_stream_entering.shape[0]
    blocks = length // TOK_DEV
    x_conv = conv_silu(unfiltered_channel_feed, channel_feed_filter).astype(jnp.float32).reshape(blocks, TOK_DEV, HEADS, HD)
    b_conv = conv_silu(unfiltered_state_entry, state_entry_filter).astype(jnp.float32).reshape(blocks, TOK_DEV, GROUPS, NS)
    c_conv = conv_silu(unfiltered_state_exit, state_exit_filter).astype(jnp.float32).reshape(blocks, TOK_DEV, GROUPS, NS)
    whole_increment_list = jax.nn.softplus(increment_preactivation)
    whole_attenuation_list = -whole_increment_list * channel_fading_speed[:, :, None] + summed_attenuation_both_ways

    def split_blocks(array):
        return jnp.moveaxis(array.reshape(HEADS, blocks, TOK_DEV), 1, 0)

    def one_block(items):
        return block_parts(*items)
    parts = lax.map(one_block, (x_conv, b_conv, c_conv, split_blocks(whole_increment_list[0]), split_blocks(whole_increment_list[1]), split_blocks(whole_attenuation_list[0]), split_blocks(whole_attenuation_list[1])))
    within, state_fwd, state_bwd, total_fwd, total_bwd, factor_fwd, factor_bwd, c_head = parts
    zero_state = jnp.zeros((HEADS, HD, NS), jnp.float32)
    _, incoming_fwd = lax.scan(carry_step, zero_state, (state_fwd, total_fwd))
    _, incoming_bwd = lax.scan(carry_step, zero_state, (state_bwd, total_bwd), reverse=True)
    readout = jax.vmap(read_state)(c_head, factor_fwd, incoming_fwd) + jax.vmap(read_state)(c_head, factor_bwd, incoming_bwd)
    mixer_out = (within + readout).reshape(length, HEADS * HD)
    gated = mixer_out * jax.nn.silu(final_valve_preactivation.astype(jnp.float32))
    grouped = gated.reshape(length, GROUPS, -1)
    grouped = grouped * lax.rsqrt(lax.optimization_barrier(jnp.mean(grouped * grouped, axis=-1, keepdims=True)) + group_eps)
    mixed = (grouped.reshape(length, HEADS * HD) * clustered_rescale_factor).astype(jnp.bfloat16)
    stream = (skip_stream_entering.astype(jnp.float32) + jnp.dot(mixed, final_projection_weights, preferred_element_type=jnp.float32)).astype(jnp.bfloat16)
    stream_f = stream.astype(jnp.float32)
    normal = (stream_f * lax.rsqrt(lax.optimization_barrier(jnp.mean(stream_f * stream_f, axis=-1, keepdims=True)) + stream_eps) * specialist_rescale_factor).astype(jnp.bfloat16)
    first = jax.nn.sigmoid(selected_twin_scores_raw[:, 0] - selected_twin_scores_raw[:, 1])
    route_weight = selected_cluster_likelihood[:, None] * jnp.stack([first, 1.0 - first], axis=1)
    slot_total = blocks * CAP
    piece_width = D_EXPERT // N_TP

    def expert_step(summed, expert):
        matched = item_specialist_couple == expert
        row_hit = jnp.any(matched, axis=1)
        order = jnp.argsort(1 - row_hit.astype(jnp.int32), stable=True)[:slot_total]
        valid = row_hit[order].astype(jnp.float32)
        token_weight = lax.optimization_barrier(jnp.sum(jnp.where(matched, route_weight, 0.0), axis=1))
        rows = normal[order]
        gate = jnp.dot(rows, specialist_gating_weights[expert], preferred_element_type=jnp.float32)
        upward = jnp.dot(rows, specialist_raising_weights[expert], preferred_element_type=jnp.float32)
        hidden = (jax.nn.silu(gate) * upward).astype(jnp.bfloat16)
        down = specialist_lowering_weights[expert]

        def add_piece(total, index):
            start = index * piece_width
            hidden_piece = lax.dynamic_slice_in_dim(hidden, start, piece_width, 1)
            down_piece = lax.dynamic_slice_in_dim(down, start, piece_width, 0)
            partial_value = jnp.dot(hidden_piece, down_piece, preferred_element_type=jnp.float32).astype(jnp.bfloat16)
            return (total + partial_value.astype(jnp.float32), None)
        answer_f, _ = lax.scan(add_piece, jnp.zeros((slot_total, D), jnp.float32), jnp.arange(N_TP, dtype=jnp.int32))
        answer = answer_f.astype(jnp.bfloat16)
        scaled = answer.astype(jnp.float32) * (token_weight[order] * valid)[:, None]
        return (summed.at[order].add(scaled), None)
    experts_sum, _ = lax.scan(expert_step, jnp.zeros((length, D), jnp.float32), jnp.arange(EXPERTS, dtype=jnp.int32))
    return (stream_f + experts_sum).astype(jnp.bfloat16)
```

```python
import functools

import jax
import jax.numpy as jnp
from jax import lax
from jax.experimental import pallas as pl
from jax.experimental.pallas import tpu as pltpu
from jax.sharding import Mesh
from jax.sharding import PartitionSpec as P

D = 2048
HD = 64
NS = 128
CONV = 5
SP = ("z", "x")
TP = ("y", "c")

HIGHEST = lax.Precision.HIGHEST
group_eps = 1e-05
stream_eps = 1e-06


def extended(cells, width):
    count = lax.axis_size(SP)
    head = cells[:width]
    tail = cells[-width:]
    return jnp.concatenate(
        [
            lax.ppermute(tail, SP, [(i, i + 1) for i in range(count - 1)]),
            cells,
            lax.ppermute(head, SP, [(i + 1, i) for i in range(count - 1)]),
        ],
        axis=0,
    )


def to_all(shard, axis):
    peers = lax.axis_size(axis)
    copies = jnp.broadcast_to(shard[None], (peers, *shard.shape))
    return lax.all_to_all(copies, axis, 0, 0, tiled=True)


def split_pair(value):
    high = value.astype(jnp.bfloat16)
    low = (value - high.astype(jnp.float32)).astype(jnp.bfloat16)
    return high, low


def log_rows(logs):
    high, low = split_pair(logs)
    both = jnp.stack([high, low])[:, :, None]
    rows = jnp.broadcast_to(both, (*both.shape[:2], NS)).reshape(-1, NS)
    return jnp.pad(rows, ((0, 16 - rows.shape[0]), (0, 0)))


def logs_of(rows, heads):
    values = rows[..., : 2 * heads, 0].astype(jnp.float32)
    return values[..., :heads] + values[..., heads:]


def block_parts(x_short, b_short, c_short, step_f, step_b, log_f, log_b):
    head_count = x_short.shape[1]
    length = x_short.shape[0]
    scores = jnp.einsum("tn,sn->ts", c_short, b_short, preferred_element_type=jnp.float32)
    x_block = x_short.astype(jnp.float32)
    b_block = b_short.astype(jnp.float32)
    forward = jnp.cumsum(log_f, axis=1)
    backward = jnp.flip(jnp.cumsum(jnp.flip(log_b, 1), axis=1), 1)
    row_index = lax.broadcasted_iota(jnp.int32, (length, length), 0)
    col_index = lax.broadcasted_iota(jnp.int32, (length, length), 1)
    lower_mask = (col_index <= row_index)[None]
    upper_mask = (col_index >= row_index)[None]
    decay_fwd = jnp.where(
        lower_mask, jnp.exp(jnp.minimum(forward[:, :, None] - forward[:, None, :], 0.0)), 0.0
    )
    decay_bwd = jnp.where(
        upper_mask, jnp.exp(jnp.minimum(backward[:, :, None] - backward[:, None, :], 0.0)), 0.0
    )
    mixing = scores[None] * (decay_fwd * step_f[:, None, :] + decay_bwd * step_b[:, None, :])
    within = jnp.einsum("hts,shp->thp", mixing, x_block, precision=HIGHEST)
    weight_fwd = jnp.exp(forward[:, -1:] - forward) * step_f
    weight_bwd = jnp.exp(backward[:, :1] - backward) * step_b
    state_fwd = jnp.einsum("hs,shp,sn->hpn", weight_fwd, x_block, b_block, precision=HIGHEST)
    state_bwd = jnp.einsum("hs,shp,sn->hpn", weight_bwd, x_block, b_block, precision=HIGHEST)
    return (
        within,
        state_fwd,
        state_bwd,
        forward[:, -1],
        backward[:, 0],
        jnp.exp(forward),
        jnp.exp(backward),
    )


def read_state(c_block, factor, state):
    return (
        jnp.einsum("tn,hpn->thp", c_block, state, precision=HIGHEST)
        * jnp.transpose(factor)[:, :, None]
    )


def shares(logs, place, reverse):
    count = logs.shape[0]
    spot = lax.broadcasted_iota(jnp.int32, (count, 1), 0)
    later = lax.broadcasted_iota(jnp.int32, (count, count), 1)
    each = lax.broadcasted_iota(jnp.int32, (count, count), 0)
    if reverse:
        between = (later < each) & (later > place)
        counts = spot > place
    else:
        between = (later > each) & (later < place)
        counts = spot < place
    passed = jnp.sum(jnp.where(between[:, :, None], logs[None], 0.0), axis=1)
    return jnp.where(counts, jnp.exp(passed), 0.0)


def weighted(factors, states):
    heads = factors.shape[1]
    parts = states.reshape(states.shape[0], heads, HD, NS).astype(jnp.float32)
    return jnp.sum(jnp.where(factors[:, :, None, None] > 0, parts, 0.0) * factors[:, :, None, None], axis=0)


def carried_in(state_fwd, state_bwd, total_fwd, total_bwd):
    heads = total_fwd.shape[0]
    rows = heads * HD
    my_x, my_z = lax.axis_index("x"), lax.axis_index("z")
    count_x, count_z = lax.axis_size("x"), lax.axis_size("z")
    message = jnp.concatenate(
        [
            state_fwd.reshape(rows, NS).astype(jnp.bfloat16),
            state_bwd.reshape(rows, NS).astype(jnp.bfloat16),
            log_rows(total_fwd),
            log_rows(total_bwd),
        ],
        axis=0,
    )
    seen = to_all(message, "x")
    logs_f = logs_of(seen[:, 2 * rows : 2 * rows + 16], heads)
    logs_b = logs_of(seen[:, 2 * rows + 16 : 2 * rows + 32], heads)
    states_f, states_b = seen[:, :rows], seen[:, rows : 2 * rows]
    near_f = weighted(shares(logs_f, my_x, False), states_f)
    near_b = weighted(shares(logs_b, my_x, True), states_b)
    row_f = weighted(shares(logs_f, count_x, False), states_f)
    row_b = weighted(shares(logs_b, -1, True), states_b)
    spot = lax.broadcasted_iota(jnp.int32, (count_x, 1), 0)
    ahead_f = jnp.sum(jnp.where(spot < my_x, logs_f, 0.0), axis=0)
    ahead_b = jnp.sum(jnp.where(spot > my_x, logs_b, 0.0), axis=0)
    out_f = jnp.concatenate(
        [row_f.reshape(rows, NS).astype(jnp.bfloat16), log_rows(jnp.sum(logs_f, axis=0))], axis=0
    )
    out_b = jnp.concatenate(
        [row_b.reshape(rows, NS).astype(jnp.bfloat16), log_rows(jnp.sum(logs_b, axis=0))], axis=0
    )
    far = lax.broadcasted_iota(jnp.int32, (count_z, 1, 1), 0)
    got = lax.all_to_all(jnp.where(far > my_z, out_f[None], out_b[None]), "z", 0, 0, tiled=True)
    logs = logs_of(got[:, rows : rows + 16], heads)
    far_f = weighted(shares(logs, my_z, False), got[:, :rows])
    far_b = weighted(shares(logs, my_z, True), got[:, :rows])
    incoming_f = far_f * jnp.exp(ahead_f)[:, None, None] + near_f
    incoming_b = far_b * jnp.exp(ahead_b)[:, None, None] + near_b
    return incoming_f, incoming_b


def expert_kernel(chunk, rows_ref, gain_ref, gate_ref, up_ref, down_ref, out_ref, normal):
    cores, places = rows_ref.shape[0], rows_ref.shape[1]

    def step(i, carry):
        at = pl.ds(pl.multiple_of(i * chunk, chunk), chunk)
        squares = jnp.zeros((chunk, 128), jnp.float32)
        for y in range(places):
            for c in range(cores):
                part = rows_ref[c, y, at, :].astype(jnp.float32)
                squares = squares + part * part
        scale = lax.rsqrt(jnp.sum(squares, axis=1, keepdims=True) / D + stream_eps)
        for y in range(places):
            for c in range(cores):
                k = y * cores + c
                part = rows_ref[c, y, at, :].astype(jnp.float32)
                normal[:, k * 128 : (k + 1) * 128] = (
                    part * scale * gain_ref[:, k * 128 : (k + 1) * 128]
                ).astype(jnp.bfloat16)
        whole = normal[...]
        gate = jnp.dot(whole, gate_ref[...], preferred_element_type=jnp.float32)
        upward = jnp.dot(whole, up_ref[...], preferred_element_type=jnp.float32)
        hidden = (jax.nn.silu(gate) * upward).astype(jnp.bfloat16)
        for y in range(places):
            k = y * cores
            part = jnp.dot(
                hidden,
                down_ref[:, k * 128 : (k + cores) * 128],
                preferred_element_type=jnp.float32,
            ).astype(jnp.bfloat16)
            for c in range(cores):
                out_ref[c, y, at, :] = part[:, c * 128 : (c + 1) * 128]
        return carry

    lax.fori_loop(0, rows_ref.shape[2] // chunk, step, 0)


def expert(rows, gain, weight_gate, weight_up, weight_down):
    chunk = 256
    full = pl.BlockSpec(memory_space=pltpu.VMEM)
    return pl.pallas_call(
        functools.partial(expert_kernel, chunk),
        out_shape=jax.ShapeDtypeStruct(rows.shape, jnp.bfloat16),
        in_specs=[full] * 5,
        out_specs=full,
        scratch_shapes=[pltpu.VMEM((chunk, D), jnp.bfloat16)],
        name="expert",
    )(rows, gain, weight_gate, weight_up, weight_down)


def body(
    skip_stream_entering,
    unfiltered_channel_feed,
    unfiltered_state_entry,
    unfiltered_state_exit,
    final_valve_preactivation,
    increment_preactivation,
    summed_attenuation_both_ways,
    channel_fading_speed,
    channel_feed_filter,
    state_entry_filter,
    state_exit_filter,
    clustered_rescale_factor,
    final_projection_weights,
    specialist_rescale_factor,
    item_specialist_couple,
    selected_cluster_likelihood,
    selected_twin_scores_raw,
    specialist_gating_weights,
    specialist_raising_weights,
    specialist_lowering_weights,
):
    tokens_here = skip_stream_entering.shape[0]
    heads_here = increment_preactivation.shape[1]
    width = unfiltered_channel_feed.shape[1]
    joined = jnp.concatenate(
        [unfiltered_channel_feed, unfiltered_state_entry, unfiltered_state_exit], axis=1
    )
    padded = extended(joined, CONV // 2)
    kernel = jnp.concatenate([channel_feed_filter, state_entry_filter, state_exit_filter], axis=1)
    summed = jnp.zeros(joined.shape, jnp.float32)
    for offset in range(CONV):
        summed = summed + kernel[offset] * padded[offset : offset + tokens_here].astype(jnp.float32)
    conv_out = jax.nn.silu(summed).astype(jnp.bfloat16)
    x_conv = conv_out[:, :width].reshape(tokens_here, heads_here, HD)
    b_conv = conv_out[:, width : 2 * width]
    c_conv = conv_out[:, 2 * width :]
    steps = jax.nn.softplus(increment_preactivation)
    logs = -steps * channel_fading_speed[:, :, None] + summed_attenuation_both_ways
    within, state_fwd, state_bwd, total_fwd, total_bwd, factor_fwd, factor_bwd = block_parts(
        x_conv, b_conv, c_conv, steps[0], steps[1], logs[0], logs[1]
    )
    incoming_fwd, incoming_bwd = carried_in(state_fwd, state_bwd, total_fwd, total_bwd)
    c_block = c_conv.astype(jnp.float32)
    mixer_out = (
        within
        + read_state(c_block, factor_fwd, incoming_fwd)
        + read_state(c_block, factor_bwd, incoming_bwd)
    )
    gated = mixer_out.reshape(tokens_here, width) * jax.nn.silu(
        final_valve_preactivation.astype(jnp.float32)
    )
    gated = gated * lax.rsqrt(jnp.mean(gated * gated, axis=-1, keepdims=True) + group_eps)
    mixed = (gated * clustered_rescale_factor).astype(jnp.bfloat16)

    peers_y, peers_c = lax.axis_size("y"), lax.axis_size("c")
    gathered = lax.all_gather(to_all(mixed, "y"), "c", axis=1)
    projected = jnp.einsum(
        "kti,kij->tj",
        gathered.reshape(peers_y * peers_c, tokens_here, width),
        final_projection_weights.reshape(peers_y * peers_c, width, width),
        preferred_element_type=jnp.float32,
    )
    stream = (skip_stream_entering.astype(jnp.float32) + projected).astype(jnp.bfloat16)

    expert_total = lax.axis_size(SP)
    capacity = 4 * tokens_here // expert_total
    slots = expert_total * capacity
    named = lax.broadcasted_iota(jnp.int32, (tokens_here, expert_total), 1)
    hit = [item_specialist_couple[:, k : k + 1] == named for k in range(2)]
    earlier = lax.broadcasted_iota(jnp.int32, (tokens_here, tokens_here), 0) > (
        lax.broadcasted_iota(jnp.int32, (tokens_here, tokens_here), 1)
    )
    ranking = jnp.dot(
        earlier.astype(jnp.bfloat16),
        (hit[0] | hit[1]).astype(jnp.bfloat16),
        preferred_element_type=jnp.float32,
    )
    slot_iota = lax.broadcasted_iota(jnp.int32, (tokens_here, slots), 1)
    chosen = []
    for k in range(2):
        rank = jnp.sum(jnp.where(hit[k], ranking, 0.0), axis=1, keepdims=True).astype(jnp.int32)
        chosen.append(item_specialist_couple[:, k : k + 1] * capacity + rank == slot_iota)
    outgoing = lax.dot_general(
        (chosen[0] | chosen[1]).astype(jnp.bfloat16),
        stream,
        (((0,), (0,)), ((), ())),
        preferred_element_type=jnp.float32,
    ).astype(jnp.bfloat16)
    arrived = lax.all_to_all(
        outgoing.reshape(expert_total, capacity, width), SP, 0, 0, tiled=True
    ).reshape(slots, width)
    rows = to_all(to_all(arrived, "y"), "c")
    partial_out = expert(
        rows,
        specialist_rescale_factor.reshape(1, D),
        specialist_gating_weights[0],
        specialist_raising_weights[0],
        specialist_lowering_weights[0],
    )
    pair = lax.all_to_all(partial_out, "c", 0, 0, tiled=True)
    pair = jnp.sum(pair.astype(jnp.float32), axis=0).astype(jnp.bfloat16)
    whole = lax.all_to_all(pair, "y", 0, 0, tiled=True)
    answer = jnp.sum(whole.astype(jnp.float32), axis=0).astype(jnp.bfloat16)
    returned = lax.all_to_all(
        answer.reshape(expert_total, capacity, width), SP, 0, 0, tiled=True
    ).reshape(slots, width)
    first = jax.nn.sigmoid(selected_twin_scores_raw[:, :1] - selected_twin_scores_raw[:, 1:])
    likelihood = selected_cluster_likelihood[:, None]
    total = stream.astype(jnp.float32)
    for k, weight in enumerate((likelihood * first, likelihood * (1.0 - first))):
        picked = jnp.dot(
            chosen[k].astype(jnp.bfloat16), returned, preferred_element_type=jnp.float32
        )
        total = total + weight * picked
    return total.astype(jnp.bfloat16)


def solution(mesh):
    sizes = dict(mesh.shape)
    torus = Mesh(mesh.devices.reshape(8, 4, sizes["tp"] // 2, 2), ("z", "x", "y", "c"))
    return jax.shard_map(
        body,
        mesh=torus,
        in_specs=(
            P(SP, TP),
            P(SP, TP),
            P(SP, TP),
            P(SP, TP),
            P(SP, TP),
            P(None, TP, SP),
            P(None, TP, SP),
            P(None, TP),
            P(None, TP),
            P(None, TP),
            P(None, TP),
            P(TP),
            P(None, TP),
            P(),
            P(SP, None),
            P(SP),
            P(SP, None),
            P(SP, None, TP),
            P(SP, None, TP),
            P(SP, TP, None),
        ),
        out_specs=P(SP, TP),
        check_vma=False,
    )
```

```python
import functools

import jax
import jax.numpy as jnp
from jax import lax
from jax.experimental import pallas as pl
from jax.experimental.pallas import tpu as pltpu
from jax.sharding import Mesh
from jax.sharding import PartitionSpec as P

D = 2048
HD = 64
NS = 128
CONV = 5
SP = ("z", "x")
TP = ("y", "c")

HIGHEST = lax.Precision.HIGHEST
group_eps = 1e-05
stream_eps = 1e-06

VMEM = pl.BlockSpec(memory_space=pltpu.VMEM)
SMEM = pl.BlockSpec(memory_space=pltpu.SMEM)
MIB = 1 << 20


def call(kernel, name, outs, args, flops=1000, scratch=(), room=8, smem=0):
    shapes = [jax.ShapeDtypeStruct(shape, dtype) for shape, dtype in outs]
    moved = sum(a.size * a.dtype.itemsize for a in args) + sum(
        o.size * o.dtype.itemsize for o in shapes
    )
    return pl.pallas_call(
        kernel,
        out_shape=shapes,
        in_specs=[SMEM] * smem + [VMEM] * (len(args) - smem),
        out_specs=[VMEM] * len(shapes),
        scratch_shapes=list(scratch),
        compiler_params=pltpu.CompilerParams(vmem_limit_bytes=room * MIB),
        cost_estimate=pl.CostEstimate(flops=flops, bytes_accessed=moved, transcendentals=0),
        name=name,
    )(*args)


def exact_dot(a, b):
    return jnp.dot(a, b, precision=HIGHEST, preferred_element_type=jnp.float32)


def dot_rows(a, b, precision=None):
    return lax.dot_general(
        a,
        b,
        (((1,), (1,)), ((), ())),
        precision=precision,
        preferred_element_type=jnp.float32,
    )


def iota(shape, dim):
    return lax.broadcasted_iota(jnp.int32, shape, dim)


def table_kernel(capacity, step_ref, fade_ref, speed_ref, named_ref, like_ref, score_ref, row_ref, col_ref):
    length = row_ref.shape[1]
    for d in range(2):
        raw = step_ref[d]
        step = jnp.maximum(raw, 0.0) + jnp.log1p(jnp.exp(-jnp.abs(raw)))
        row_ref[2 * d : 2 * d + 2, :] = -step * speed_ref[d] + fade_ref[d]
        row_ref[4 + 2 * d : 6 + 2 * d, :] = step
    whole = row_ref[0:8, :]
    lane, line = iota(whole.shape, 1), iota(whole.shape, 0)
    ahead = behind = whole
    reach = 1
    while reach < length:
        ahead = ahead + jnp.where(lane >= reach, pltpu.roll(ahead, reach, 1), 0.0)
        behind = behind + jnp.where(lane < length - reach, pltpu.roll(behind, length - reach, 1), 0.0)
        reach *= 2
    row_ref[0:8, :] = jnp.where(line < 2, ahead, jnp.where(line < 4, behind, whole))
    experts = 32
    expert = iota((experts, length), 0)
    hit = [named_ref[k : k + 1, :] == expert for k in range(2)]
    earlier = iota((length, length), 0) < iota((length, length), 1)
    ranking = jnp.dot(
        jnp.where(hit[0] | hit[1], 1.0, 0.0).astype(jnp.bfloat16),
        jnp.where(earlier, 1.0, 0.0).astype(jnp.bfloat16),
        preferred_element_type=jnp.float32,
    )
    place = ranking + expert.astype(jnp.float32) * capacity
    for k in range(2):
        row_ref[8 + k : 9 + k, :] = jnp.sum(jnp.where(hit[k], place, 0.0), axis=0, keepdims=True)
    first = jax.nn.sigmoid(score_ref[0:1, :] - score_ref[1:2, :])
    row_ref[10:11, :] = like_ref[...] * first
    row_ref[11:12, :] = like_ref[...] * (1.0 - first)
    row_ref[12:16, :] = jnp.zeros((4, length), jnp.float32)
    col_ref[...] = jnp.zeros_like(col_ref)
    col_ref[0:16, :] = row_ref[...]
    col_ref[...] = jnp.transpose(col_ref[...])


def conv_kernel(
    x_ref, b_ref, c_ref, before_ref, after_ref, kx_ref, kb_ref, kc_ref, col_ref,
    message_ref, xs_ref, bs_ref, cs_ref, padded,
):
    length, width = x_ref.shape
    parts = []
    for n, (ref, taps) in enumerate(((x_ref, kx_ref), (b_ref, kb_ref), (c_ref, kc_ref))):
        lanes = slice(n * width, (n + 1) * width)
        padded[8 : 8 + length, :] = ref[...].astype(jnp.float32)
        padded[6:8, :] = before_ref[:, lanes]
        padded[8 + length : 10 + length, :] = after_ref[:, lanes]
        total = jnp.zeros((length, width), jnp.float32)
        for k in range(CONV):
            total = total + taps[k : k + 1, :] * padded[6 + k : 6 + k + length, :]
        parts.append(jax.nn.silu(total).astype(jnp.bfloat16))
    xs_ref[...], bs_ref[...], cs_ref[...] = parts
    x_block = parts[0].astype(jnp.float32)
    b_block = parts[1].astype(jnp.float32)
    left = iota((length, width), 1) < HD
    logs = jnp.zeros((16, width), jnp.float32)
    line = iota((16, width), 0)
    for d, last in ((0, length - 1), (1, 0)):
        weight = []
        for h in range(2):
            k = 2 * d + h
            end = col_ref[last : last + 1, k : k + 1]
            weight.append(jnp.exp(end - col_ref[:, k : k + 1]) * col_ref[:, 4 + k : 5 + k])
            high = end.astype(jnp.bfloat16).astype(jnp.float32)
            logs = jnp.where(line == 4 * d + h, high, logs)
            logs = jnp.where(line == 4 * d + 2 + h, end - high, logs)
        scaled = x_block * jnp.where(left, weight[0], weight[1])
        state = exact_dot(jnp.transpose(scaled), b_block).astype(jnp.bfloat16)
        for peer in range(message_ref.shape[0]):
            message_ref[peer, d * width : (d + 1) * width, :] = state
    for peer in range(message_ref.shape[0]):
        message_ref[peer, 2 * width :, :] = logs.astype(jnp.bfloat16)


def within_kernel(xs_ref, bs_ref, cs_ref, row_ref, col_ref, out_ref):
    length, width = xs_ref.shape
    scores = dot_rows(cs_ref[...], bs_ref[...])
    x_block = xs_ref[...].astype(jnp.float32)
    to, since = iota((length, length), 0), iota((length, length), 1)
    sides = []
    for h in range(2):
        both = jnp.zeros((length, length), jnp.float32)
        for d in range(2):
            k = 2 * d + h
            seen = since <= to if d == 0 else since >= to
            passed = col_ref[:, k : k + 1] - row_ref[k : k + 1, :]
            decay = jnp.where(seen, jnp.exp(jnp.minimum(passed, 0.0)), 0.0)
            both = both + decay * row_ref[4 + k : 5 + k, :]
        sides.append(exact_dot(scores * both, x_block))
    out_ref[...] = jnp.where(iota((length, width), 1) < HD, sides[0], sides[1])


def log_pair(tile, d):
    return [tile[4 * d + h : 4 * d + h + 1, :] + tile[4 * d + 2 + h : 4 * d + 3 + h, :] for h in range(2)]


def by_head(pair, rows):
    return jnp.where(iota((rows, 128), 0) < HD, pair[0], pair[1])


def row_kernel(place_ref, seen_ref, message_ref, near_ref, ahead_ref):
    my_x, my_z = place_ref[0], place_ref[1]
    peers, rows = seen_ref.shape[0], near_ref.shape[1]
    line = iota((16, 128), 0)
    out = []
    ahead_ref[...] = jnp.zeros_like(ahead_ref)
    for d in range(2):
        total = near = jnp.zeros((rows, 128), jnp.float32)
        far = [jnp.zeros((1, 128), jnp.float32)] * 2
        ahead = list(far)
        for k in range(peers) if d == 0 else reversed(range(peers)):
            logs = log_pair(seen_ref[k, 2 * rows :, :].astype(jnp.float32), d)
            near = jnp.where(k == my_x, total, near)
            passed = k < my_x if d == 0 else k > my_x
            state = seen_ref[k, d * rows : (d + 1) * rows, :].astype(jnp.float32)
            total = total * jnp.exp(by_head(logs, rows)) + state
            for h in range(2):
                far[h] = far[h] + logs[h]
                ahead[h] = ahead[h] + jnp.where(passed, logs[h], 0.0)
        near_ref[d] = near
        tile = jnp.zeros((16, 128), jnp.float32)
        for h in range(2):
            ahead_ref[2 * d + h : 2 * d + h + 1, :] = ahead[h]
            high = far[h].astype(jnp.bfloat16).astype(jnp.float32)
            tile = jnp.where(line == h, high, tile)
            tile = jnp.where(line == 2 + h, far[h] - high, tile)
        out.append((total, tile))
    for k in range(message_ref.shape[0]):
        onward = k > my_z
        message_ref[k, :rows, :] = jnp.where(onward, out[0][0], out[1][0]).astype(jnp.bfloat16)
        message_ref[k, rows:, :] = jnp.where(onward, out[0][1], out[1][1]).astype(jnp.bfloat16)


def mixed_kernel(
    place_ref, got_ref, near_ref, ahead_ref, cs_ref, within_ref, col_ref, valve_ref, gain_ref, out_ref
):
    my_z = place_ref[1]
    peers, rows = got_ref.shape[0], near_ref.shape[1]
    length = cs_ref.shape[0]
    c_block = cs_ref[...].astype(jnp.float32)
    left = iota((length, rows), 1) < HD
    mixer = within_ref[...]
    for d in range(2):
        state = jnp.zeros((rows, 128), jnp.float32)
        for k in range(peers) if d == 0 else reversed(range(peers)):
            passed = k < my_z if d == 0 else k > my_z
            logs = log_pair(got_ref[k, rows:, :].astype(jnp.float32), 0)
            onto = state * jnp.exp(by_head(logs, rows)) + got_ref[k, :rows, :].astype(jnp.float32)
            state = jnp.where(passed, onto, state)
        ahead = [ahead_ref[2 * d + h : 2 * d + h + 1, :] for h in range(2)]
        state = state * jnp.exp(by_head(ahead, rows)) + near_ref[d]
        factor = jnp.exp(
            jnp.where(left, col_ref[:, 2 * d : 2 * d + 1], col_ref[:, 2 * d + 1 : 2 * d + 2])
        )
        mixer = mixer + dot_rows(c_block, state, HIGHEST) * factor
    gated = mixer * jax.nn.silu(valve_ref[...].astype(jnp.float32))
    gated = gated * lax.rsqrt(jnp.mean(gated * gated, axis=-1, keepdims=True) + group_eps)
    mixed = (gated * gain_ref[...]).astype(jnp.bfloat16)
    for k in range(out_ref.shape[0]):
        out_ref[k] = mixed


def stream_kernel(mixed_ref, weight_ref, skip_ref, row_ref, stream_ref, out_ref):
    length, width = skip_ref.shape
    places = mixed_ref.shape[0]
    total = skip_ref[...].astype(jnp.float32)
    product = jnp.zeros((length, width), jnp.float32)
    for y in range(places):
        both = jnp.concatenate([mixed_ref[y, :length, :], mixed_ref[y, length:, :]], axis=1)
        product = product + jnp.dot(
            both, weight_ref[2 * y * width : 2 * (y + 1) * width, :], preferred_element_type=jnp.float32
        )
    stream = (total + product).astype(jnp.bfloat16)
    stream_ref[...] = stream
    slot = iota((out_ref.shape[0], length), 0).astype(jnp.float32)
    chosen = (row_ref[8:9, :] == slot) | (row_ref[9:10, :] == slot)
    out_ref[...] = jnp.dot(
        jnp.where(chosen, 1.0, 0.0).astype(jnp.bfloat16), stream, preferred_element_type=jnp.float32
    ).astype(jnp.bfloat16)


def half_products(rows_ref, gain_ref, gate_ref, up_ref, core, at, scaled):
    places = rows_ref.shape[0]
    squares = jnp.zeros((at.size, 128), jnp.float32)
    for y in range(places):
        part = rows_ref[y, at, :].astype(jnp.float32)
        squares = squares + part * part
        scaled[:, y * 128 : (y + 1) * 128] = (part * gain_ref[y, pl.ds(core, 1), :]).astype(
            jnp.bfloat16
        )
    whole = scaled[...]
    gate = jnp.dot(whole, gate_ref[...], preferred_element_type=jnp.float32)
    upward = jnp.dot(whole, up_ref[...], preferred_element_type=jnp.float32)
    return jnp.sum(squares, axis=1, keepdims=True), gate, upward


def pick_half(core, weight_ref, half):
    for y in range(half.shape[0] // 128):
        half[y * 128 : (y + 1) * 128, :] = weight_ref[y, core]


def first_half_kernel(
    chunk, place_ref, rows_ref, gain_ref, gate_ref, up_ref, squares_ref, gate_out, up_out, scaled, gate_half, up_half
):
    core = place_ref[2]
    pick_half(core, gate_ref, gate_half)
    pick_half(core, up_ref, up_half)

    def step(i, carry):
        at = pl.ds(pl.multiple_of(i * chunk, chunk), chunk)
        squares, gate, upward = half_products(
            rows_ref, gain_ref, gate_half, up_half, core, at, scaled
        )
        squares_ref[at, :] = jnp.broadcast_to(squares, (chunk, 128))
        gate_out[at, :] = gate
        up_out[at, :] = upward
        return carry

    lax.fori_loop(0, rows_ref.shape[1] // chunk, step, 0)


def second_half_kernel(
    chunk, place_ref, rows_ref, gain_ref, gate_ref, up_ref, down_ref, squares_ref, gate_in, up_in,
    hidden_ref, out_ref, scaled, gate_half, up_half, down_half,
):
    other = 1 - place_ref[2]
    pick_half(other, gate_ref, gate_half)
    pick_half(other, up_ref, up_half)
    for y in range(rows_ref.shape[0]):
        at = pl.ds(pl.multiple_of((2 * y + other) * 128, 128), 128)
        down_half[:, y * 128 : (y + 1) * 128] = down_ref[:, at]

    def step(i, carry):
        at = pl.ds(pl.multiple_of(i * chunk, chunk), chunk)
        squares, gate, upward = half_products(
            rows_ref, gain_ref, gate_half, up_half, other, at, scaled
        )
        squares = squares + squares_ref[at, 0:1]
        scale = lax.rsqrt(squares / D + stream_eps)
        gate = (gate + gate_in[at, :]) * scale
        upward = (upward + up_in[at, :]) * scale
        hidden = (jax.nn.silu(gate) * upward).astype(jnp.bfloat16)
        hidden_ref[at, :] = hidden
        part = jnp.dot(hidden, down_half[...], preferred_element_type=jnp.float32)
        for y in range(rows_ref.shape[0]):
            out_ref[y, at, :] = part[:, y * 128 : (y + 1) * 128].astype(jnp.bfloat16)
        return carry

    lax.fori_loop(0, rows_ref.shape[1] // chunk, step, 0)


def own_half_kernel(chunk, place_ref, hidden_ref, down_ref, out_ref, down_half):
    core = place_ref[2]
    for y in range(out_ref.shape[0]):
        at = pl.ds(pl.multiple_of((2 * y + core) * 128, 128), 128)
        down_half[:, y * 128 : (y + 1) * 128] = down_ref[:, at]

    def step(i, carry):
        at = pl.ds(pl.multiple_of(i * chunk, chunk), chunk)
        part = jnp.dot(hidden_ref[at, :], down_half[...], preferred_element_type=jnp.float32)
        for y in range(out_ref.shape[0]):
            out_ref[y, at, :] = part[:, y * 128 : (y + 1) * 128].astype(jnp.bfloat16)
        return carry

    lax.fori_loop(0, hidden_ref.shape[0] // chunk, step, 0)


def final_kernel(returned_ref, stream_ref, col_ref, out_ref):
    length = stream_ref.shape[0]
    slot = iota((length, returned_ref.shape[0]), 1).astype(jnp.float32)
    returned = returned_ref[...]
    total = stream_ref[...].astype(jnp.float32)
    for k in range(2):
        chosen = jnp.where(col_ref[:, 8 + k : 9 + k] == slot, 1.0, 0.0).astype(jnp.bfloat16)
        picked = jnp.dot(chosen, returned, preferred_element_type=jnp.float32)
        total = total + col_ref[:, 10 + k : 11 + k] * picked
    out_ref[...] = total.astype(jnp.bfloat16)


def swapped(value):
    return lax.ppermute(value, "c", [(0, 1), (1, 0)])


def to_all(shard, axis):
    peers = lax.axis_size(axis)
    copies = jnp.broadcast_to(shard[None], (peers, *shard.shape))
    return lax.all_to_all(copies, axis, 0, 0, tiled=True)


def body(
    skip_stream_entering,
    unfiltered_channel_feed,
    unfiltered_state_entry,
    unfiltered_state_exit,
    final_valve_preactivation,
    increment_preactivation,
    summed_attenuation_both_ways,
    channel_fading_speed,
    channel_feed_filter,
    state_entry_filter,
    state_exit_filter,
    clustered_rescale_factor,
    final_projection_weights,
    specialist_rescale_factor,
    item_specialist_couple,
    selected_cluster_likelihood,
    selected_twin_scores_raw,
    specialist_gating_weights,
    specialist_raising_weights,
    specialist_lowering_weights,
):
    f32, bf16 = jnp.float32, jnp.bfloat16
    length, width = unfiltered_channel_feed.shape
    blocks = lax.axis_size(SP)
    peers_x, peers_y, peers_z = (lax.axis_size(a) for a in ("x", "y", "z"))
    capacity = 4 * length // blocks
    slots = blocks * capacity
    place = jnp.stack([lax.axis_index("x"), lax.axis_index("z"), lax.axis_index("c")]).astype(jnp.int32)

    rim = CONV // 2
    feeds = (unfiltered_channel_feed, unfiltered_state_entry, unfiltered_state_exit)
    tail = jnp.concatenate([a[-rim:] for a in feeds], axis=1).astype(f32)
    top = jnp.concatenate([a[:rim] for a in feeds], axis=1).astype(f32)
    before = lax.ppermute(tail, SP, [(i, i + 1) for i in range(blocks - 1)])
    after = lax.ppermute(top, SP, [(i + 1, i) for i in range(blocks - 1)])

    rows, cols = call(
        functools.partial(table_kernel, capacity),
        "table",
        [((16, length), f32), ((length, length), f32)],
        (
            increment_preactivation,
            summed_attenuation_both_ways,
            channel_fading_speed[:, :, None],
            item_specialist_couple.T,
            selected_cluster_likelihood[None],
            selected_twin_scores_raw.T,
        ),
        flops=4_000_000,
    )
    message, x_conv, b_conv, c_conv = call(
        conv_kernel,
        "conv",
        [((peers_x, 2 * width + 16, NS), bf16)] + [((length, width), bf16)] * 3,
        (*feeds, before, after, channel_feed_filter, state_entry_filter, state_exit_filter, cols),
        flops=4_000_000,
        scratch=[pltpu.VMEM((length + 16, width), f32)],
    )
    seen = lax.all_to_all(message, "x", 0, 0, tiled=True)
    (within,) = call(
        within_kernel,
        "within",
        [((length, width), f32)],
        (x_conv, b_conv, c_conv, rows, cols),
        flops=40_000_000,
    )
    onward, near, ahead = call(
        row_kernel,
        "row",
        [((peers_z, width + 16, NS), bf16), ((2, width, NS), f32), ((8, NS), f32)],
        (place, seen),
        smem=1,
    )
    got = lax.all_to_all(onward, "z", 0, 0, tiled=True)
    (copies,) = call(
        mixed_kernel,
        "mixed",
        [((peers_y, length, width), bf16)],
        (
            place, got, near, ahead, c_conv, within, cols,
            final_valve_preactivation, clustered_rescale_factor[None],
        ),
        smem=1,
    )
    gathered = lax.all_gather(
        lax.all_to_all(copies, "y", 0, 0, tiled=True), "c", axis=1, tiled=True
    )
    stream, outgoing = call(
        stream_kernel,
        "stream",
        [((length, width), bf16), ((slots, width), bf16)],
        (gathered, final_projection_weights, skip_stream_entering, rows),
    )
    arrived = lax.all_to_all(
        outgoing.reshape(blocks, capacity, width), SP, 0, 0, tiled=True
    ).reshape(slots, width)
    own = to_all(arrived, "y")
    theirs = swapped(own)
    chunk = 256
    wide = (peers_y, 2, 128)
    gain = specialist_rescale_factor.reshape(wide)
    weight_gate = specialist_gating_weights.reshape(*wide, -1)
    weight_up = specialist_raising_weights.reshape(*wide, -1)
    weight_down = specialist_lowering_weights[0]
    units = weight_down.shape[0]
    half = pltpu.VMEM((D // 2, units), bf16)
    down_half = pltpu.VMEM((units, D // 2), bf16)
    scaled = pltpu.VMEM((chunk, D // 2), bf16)
    squares, gate, upward = call(
        functools.partial(first_half_kernel, chunk),
        "first_half",
        [((slots, 128), f32), ((slots, units), f32), ((slots, units), f32)],
        (place, own, gain, weight_gate, weight_up),
        flops=4 * slots * units * D // 2,
        scratch=[scaled, half, half],
        smem=1,
        room=16,
    )
    hidden, sent = call(
        functools.partial(second_half_kernel, chunk),
        "second_half",
        [((slots, units), bf16), ((peers_y, slots, width), bf16)],
        (place, theirs, gain, weight_gate, weight_up, weight_down, squares, gate, upward),
        flops=6 * slots * units * D // 2,
        scratch=[scaled, half, half, down_half],
        smem=1,
        room=20,
    )
    partner = swapped(sent)
    (kept,) = call(
        functools.partial(own_half_kernel, chunk),
        "own_half",
        [((peers_y, slots, width), bf16)],
        (place, hidden, weight_down),
        flops=2 * slots * units * D // 2,
        scratch=[down_half],
        smem=1,
        room=12,
    )
    pair = (kept.astype(f32) + partner.astype(f32)).astype(bf16)
    whole = lax.all_to_all(pair, "y", 0, 0, tiled=True)
    answer = jnp.sum(whole.astype(f32), axis=0).astype(bf16)
    returned = lax.all_to_all(
        answer.reshape(blocks, capacity, width), SP, 0, 0, tiled=True
    ).reshape(slots, width)
    (out,) = call(final_kernel, "final", [((length, width), bf16)], (returned, stream, cols))
    return out


def solution(mesh):
    sizes = dict(mesh.shape)
    torus = Mesh(mesh.devices.reshape(8, 4, sizes["tp"] // 2, 2), ("z", "x", "y", "c"))
    return jax.shard_map(
        body,
        mesh=torus,
        in_specs=(
            P(SP, TP),
            P(SP, TP),
            P(SP, TP),
            P(SP, TP),
            P(SP, TP),
            P(None, TP, SP),
            P(None, TP, SP),
            P(None, TP),
            P(None, TP),
            P(None, TP),
            P(None, TP),
            P(TP),
            P(None, TP),
            P(),
            P(SP, None),
            P(SP),
            P(SP, None),
            P(SP, None, TP),
            P(SP, None, TP),
            P(SP, TP, None),
        ),
        out_specs=P(SP, TP),
        check_vma=False,
    )
```

```python
import functools

import jax
import jax.numpy as jnp
from jax import lax
from jax.experimental import pallas as pl
from jax.experimental.pallas import tpu as pltpu
from jax.sharding import Mesh
from jax.sharding import PartitionSpec as P

D = 2048
HD = 64
NS = 128
CONV = 5
SP = ("z", "x")
TP = ("y", "c")

HIGHEST = lax.Precision.HIGHEST
group_eps = 1e-05
stream_eps = 1e-06

VMEM = pl.BlockSpec(memory_space=pltpu.VMEM)
SMEM = pl.BlockSpec(memory_space=pltpu.SMEM)
HBM = pl.BlockSpec(memory_space=pltpu.HBM)
MIB = 1 << 20


def call(kernel, name, outs, args, flops=1000, scratch=(), room=8, smem=0, hbm=0):
    shapes = [jax.ShapeDtypeStruct(shape, dtype) for shape, dtype in outs]
    moved = sum(a.size * a.dtype.itemsize for a in args) + sum(
        o.size * o.dtype.itemsize for o in shapes
    )
    args = list(args)
    for n in range(smem, smem + hbm):
        args[n] = pltpu.with_memory_space_constraint(args[n], pltpu.HBM)
    return pl.pallas_call(
        kernel,
        out_shape=shapes,
        in_specs=[SMEM] * smem + [HBM] * hbm + [VMEM] * (len(args) - smem - hbm),
        out_specs=[VMEM] * len(shapes),
        scratch_shapes=list(scratch),
        compiler_params=pltpu.CompilerParams(vmem_limit_bytes=room * MIB),
        cost_estimate=pl.CostEstimate(flops=flops, bytes_accessed=moved, transcendentals=0),
        name=name,
    )(*args)


def exact_dot(a, b):
    return jnp.dot(a, b, precision=HIGHEST, preferred_element_type=jnp.float32)


def dot_rows(a, b, precision=None):
    return lax.dot_general(
        a,
        b,
        (((1,), (1,)), ((), ())),
        precision=precision,
        preferred_element_type=jnp.float32,
    )


def iota(shape, dim):
    return lax.broadcasted_iota(jnp.int32, shape, dim)


def fetch(pairs, done):
    copies = [pltpu.make_async_copy(a, b, done.at[n]) for n, (a, b) in enumerate(pairs)]
    for copy in copies:
        copy.start()
    for copy in copies:
        copy.wait()


def rim_kernel(place_ref, x_in, b_in, c_in, even_ref, odd_ref, x_ref, b_ref, c_ref, done):
    fetch(((x_in, x_ref), (b_in, b_ref), (c_in, c_ref)), done)
    even = place_ref[3] == 0
    length, width = x_ref.shape
    for n, ref in enumerate((x_ref, b_ref, c_ref)):
        lanes = slice(n * width, (n + 1) * width)
        top = ref[0:16, :].astype(jnp.float32)[0:2]
        tail = ref[length - 16 : length, :].astype(jnp.float32)[14:16]
        even_ref[:, lanes] = jnp.where(even, tail, top)
        odd_ref[:, lanes] = jnp.where(even, top, tail)


def table_kernel(
    capacity, step_in, fade_in, speed_in, named_in, like_in, score_in, kx_in, kb_in, kc_in,
    row_ref, col_ref, kx_ref, kb_ref, kc_ref,
    step_ref, fade_ref, speed_ref, named_ref, like_ref, score_ref, done,
):
    fetch(
        (
            (step_in, step_ref), (fade_in, fade_ref), (speed_in, speed_ref), (named_in, named_ref),
            (like_in, like_ref), (score_in, score_ref), (kx_in, kx_ref), (kb_in, kb_ref), (kc_in, kc_ref),
        ),
        done,
    )
    length = row_ref.shape[1]
    for d in range(2):
        raw = step_ref[d]
        step = jnp.maximum(raw, 0.0) + jnp.log1p(jnp.exp(-jnp.abs(raw)))
        row_ref[4 + 2 * d : 6 + 2 * d, :] = step
        for h in range(2):
            k = 2 * d + h
            row_ref[k : k + 1, :] = (
                -step[h : h + 1] * speed_ref[d : d + 1, h : h + 1] + fade_ref[d][h : h + 1]
            )
    whole = row_ref[0:8, :]
    lane, line = iota(whole.shape, 1), iota(whole.shape, 0)
    ahead = behind = whole
    reach = 1
    while reach < length:
        ahead = ahead + jnp.where(lane >= reach, pltpu.roll(ahead, reach, 1), 0.0)
        behind = behind + jnp.where(lane < length - reach, pltpu.roll(behind, length - reach, 1), 0.0)
        reach *= 2
    row_ref[0:8, :] = jnp.where(line < 2, ahead, jnp.where(line < 4, behind, whole))
    experts = 32
    expert = iota((experts, length), 0)
    hit = [named_ref[k : k + 1, :] == expert for k in range(2)]
    earlier = iota((length, length), 0) < iota((length, length), 1)
    ranking = jnp.dot(
        jnp.where(hit[0] | hit[1], 1.0, 0.0).astype(jnp.bfloat16),
        jnp.where(earlier, 1.0, 0.0).astype(jnp.bfloat16),
        preferred_element_type=jnp.float32,
    )
    place = ranking + expert.astype(jnp.float32) * capacity
    for k in range(2):
        row_ref[8 + k : 9 + k, :] = jnp.sum(jnp.where(hit[k], place, 0.0), axis=0, keepdims=True)
    first = jax.nn.sigmoid(score_ref[0:1, :] - score_ref[1:2, :])
    row_ref[10:11, :] = like_ref[...] * first
    row_ref[11:12, :] = like_ref[...] * (1.0 - first)
    row_ref[12:16, :] = jnp.zeros((4, length), jnp.float32)
    col_ref[...] = jnp.zeros_like(col_ref)
    col_ref[0:16, :] = row_ref[...]
    col_ref[...] = jnp.transpose(col_ref[...])


def conv_kernel(
    place_ref, x_ref, b_ref, c_ref, even_ref, odd_ref, kx_ref, kb_ref, kc_ref, col_ref,
    message_ref, xs_ref, bs_ref, cs_ref, padded,
):
    length, width = x_ref.shape
    even = place_ref[3] == 0
    before = jnp.where(even, odd_ref[...], even_ref[...])
    after = jnp.where(even, even_ref[...], odd_ref[...])
    parts = []
    for n, (ref, taps) in enumerate(((x_ref, kx_ref), (b_ref, kb_ref), (c_ref, kc_ref))):
        lanes = slice(n * width, (n + 1) * width)
        padded[8 : 8 + length, :] = ref[...].astype(jnp.float32)
        padded[6:8, :] = before[:, lanes]
        padded[8 + length : 10 + length, :] = after[:, lanes]
        total = jnp.zeros((length, width), jnp.float32)
        for k in range(CONV):
            total = total + taps[k : k + 1, :] * padded[6 + k : 6 + k + length, :]
        parts.append(jax.nn.silu(total).astype(jnp.bfloat16))
    xs_ref[...], bs_ref[...], cs_ref[...] = parts
    x_block = parts[0].astype(jnp.float32)
    b_block = parts[1].astype(jnp.float32)
    left = iota((length, width), 1) < HD
    logs = jnp.zeros((16, width), jnp.float32)
    line = iota((16, width), 0)
    for d, last in ((0, length - 1), (1, 0)):
        weight = []
        for h in range(2):
            k = 2 * d + h
            end = col_ref[last : last + 1, k : k + 1]
            weight.append(jnp.exp(end - col_ref[:, k : k + 1]) * col_ref[:, 4 + k : 5 + k])
            high = end.astype(jnp.bfloat16).astype(jnp.float32)
            logs = jnp.where(line == 4 * d + h, high, logs)
            logs = jnp.where(line == 4 * d + 2 + h, end - high, logs)
        scaled = x_block * jnp.where(left, weight[0], weight[1])
        state = exact_dot(jnp.transpose(scaled), b_block).astype(jnp.bfloat16)
        for peer in range(message_ref.shape[0]):
            message_ref[peer, d * width : (d + 1) * width, :] = state
    for peer in range(message_ref.shape[0]):
        message_ref[peer, 2 * width :, :] = logs.astype(jnp.bfloat16)


def within(xs_ref, bs_ref, cs_ref, row_ref, col_ref):
    length, width = xs_ref.shape
    scores = dot_rows(cs_ref[...], bs_ref[...])
    x_block = xs_ref[...].astype(jnp.float32)
    to, since = iota((length, length), 0), iota((length, length), 1)
    sides = []
    for h in range(2):
        both = jnp.zeros((length, length), jnp.float32)
        for d in range(2):
            k = 2 * d + h
            seen = since <= to if d == 0 else since >= to
            passed = col_ref[:, k : k + 1] - row_ref[k : k + 1, :]
            decay = jnp.where(seen, jnp.exp(jnp.minimum(passed, 0.0)), 0.0)
            both = both + decay * row_ref[4 + k : 5 + k, :]
        sides.append(exact_dot(scores * both, x_block))
    return jnp.where(iota((length, width), 1) < HD, sides[0], sides[1])


def log_pair(tile, d):
    return [tile[4 * d + h : 4 * d + h + 1, :] + tile[4 * d + 2 + h : 4 * d + 3 + h, :] for h in range(2)]


def by_head(pair, rows):
    return jnp.where(iota((rows, 128), 0) < HD, pair[0], pair[1])


def row_kernel(place_ref, seen_ref, message_ref, near_ref, ahead_ref):
    my_x, my_z = place_ref[0], place_ref[1]
    peers, rows = seen_ref.shape[0], near_ref.shape[1]
    line = iota((16, 128), 0)
    out = []
    ahead_ref[...] = jnp.zeros_like(ahead_ref)
    for d in range(2):
        total = near = jnp.zeros((rows, 128), jnp.float32)
        far = [jnp.zeros((1, 128), jnp.float32)] * 2
        ahead = list(far)
        for k in range(peers) if d == 0 else reversed(range(peers)):
            logs = log_pair(seen_ref[k, 2 * rows :, :].astype(jnp.float32), d)
            near = jnp.where(k == my_x, total, near)
            passed = k < my_x if d == 0 else k > my_x
            state = seen_ref[k, d * rows : (d + 1) * rows, :].astype(jnp.float32)
            total = total * jnp.exp(by_head(logs, rows)) + state
            for h in range(2):
                far[h] = far[h] + logs[h]
                ahead[h] = ahead[h] + jnp.where(passed, logs[h], 0.0)
        near_ref[d] = near
        tile = jnp.zeros((16, 128), jnp.float32)
        for h in range(2):
            ahead_ref[2 * d + h : 2 * d + h + 1, :] = ahead[h]
            high = far[h].astype(jnp.bfloat16).astype(jnp.float32)
            tile = jnp.where(line == h, high, tile)
            tile = jnp.where(line == 2 + h, far[h] - high, tile)
        out.append((total, tile))
    for k in range(message_ref.shape[0]):
        onward = k > my_z
        message_ref[k, :rows, :] = jnp.where(onward, out[0][0], out[1][0]).astype(jnp.bfloat16)
        message_ref[k, rows:, :] = jnp.where(onward, out[0][1], out[1][1]).astype(jnp.bfloat16)


def mixed_kernel(
    place_ref, got_ref, near_ref, ahead_ref, xs_ref, bs_ref, cs_ref, row_ref, col_ref, valve_ref, gain_ref,
    out_ref,
):
    my_z = place_ref[1]
    peers, rows = got_ref.shape[0], near_ref.shape[1]
    length = cs_ref.shape[0]
    c_block = cs_ref[...].astype(jnp.float32)
    left = iota((length, rows), 1) < HD
    mixer = within(xs_ref, bs_ref, cs_ref, row_ref, col_ref)
    for d in range(2):
        state = jnp.zeros((rows, 128), jnp.float32)
        for k in range(peers) if d == 0 else reversed(range(peers)):
            passed = k < my_z if d == 0 else k > my_z
            logs = log_pair(got_ref[k, rows:, :].astype(jnp.float32), 0)
            onto = state * jnp.exp(by_head(logs, rows)) + got_ref[k, :rows, :].astype(jnp.float32)
            state = jnp.where(passed, onto, state)
        ahead = [ahead_ref[2 * d + h : 2 * d + h + 1, :] for h in range(2)]
        state = state * jnp.exp(by_head(ahead, rows)) + near_ref[d]
        factor = jnp.exp(
            jnp.where(left, col_ref[:, 2 * d : 2 * d + 1], col_ref[:, 2 * d + 1 : 2 * d + 2])
        )
        mixer = mixer + dot_rows(c_block, state, HIGHEST) * factor
    gated = mixer * jax.nn.silu(valve_ref[...].astype(jnp.float32))
    gated = gated * lax.rsqrt(jnp.mean(gated * gated, axis=-1, keepdims=True) + group_eps)
    mixed = (gated * gain_ref[...]).astype(jnp.bfloat16)
    for k in range(out_ref.shape[0]):
        out_ref[k] = mixed


def stream_kernel(mixed_ref, weight_ref, skip_ref, row_ref, stream_ref, out_ref):
    length, width = skip_ref.shape
    places = mixed_ref.shape[0]
    total = skip_ref[...].astype(jnp.float32)
    product = jnp.zeros((length, width), jnp.float32)
    for y in range(places):
        both = jnp.concatenate([mixed_ref[y, :length, :], mixed_ref[y, length:, :]], axis=1)
        product = product + jnp.dot(
            both, weight_ref[2 * y * width : 2 * (y + 1) * width, :], preferred_element_type=jnp.float32
        )
    stream = (total + product).astype(jnp.bfloat16)
    stream_ref[...] = stream
    slot = iota((out_ref.shape[0], length), 0).astype(jnp.float32)
    chosen = (row_ref[8:9, :] == slot) | (row_ref[9:10, :] == slot)
    out_ref[...] = jnp.dot(
        jnp.where(chosen, 1.0, 0.0).astype(jnp.bfloat16), stream, preferred_element_type=jnp.float32
    ).astype(jnp.bfloat16)


def half_products(rows_ref, gain_ref, gate_ref, up_ref, core, at, scaled):
    places = rows_ref.shape[0]
    squares = jnp.zeros((at.size, 128), jnp.float32)
    for y in range(places):
        part = rows_ref[y, at, :].astype(jnp.float32)
        squares = squares + part * part
        scaled[:, y * 128 : (y + 1) * 128] = (part * gain_ref[y, pl.ds(core, 1), :]).astype(
            jnp.bfloat16
        )
    whole = scaled[...]
    gate = jnp.dot(whole, gate_ref[...], preferred_element_type=jnp.float32)
    upward = jnp.dot(whole, up_ref[...], preferred_element_type=jnp.float32)
    return jnp.sum(squares, axis=1, keepdims=True), gate, upward


def pick_half(core, weight_ref, half):
    for y in range(half.shape[0] // 128):
        half[y * 128 : (y + 1) * 128, :] = weight_ref[y, core]


def first_half_kernel(
    chunk, place_ref, rows_ref, gain_ref, gate_ref, up_ref, squares_ref, gate_out, up_out, scaled, gate_half, up_half
):
    core = place_ref[2]
    pick_half(core, gate_ref, gate_half)
    pick_half(core, up_ref, up_half)

    def step(i, carry):
        at = pl.ds(pl.multiple_of(i * chunk, chunk), chunk)
        squares, gate, upward = half_products(
            rows_ref, gain_ref, gate_half, up_half, core, at, scaled
        )
        squares_ref[at, :] = jnp.broadcast_to(squares, (chunk, 128))
        gate_out[at, :] = gate
        up_out[at, :] = upward
        return carry

    lax.fori_loop(0, rows_ref.shape[1] // chunk, step, 0)


def second_half_kernel(
    chunk, place_ref, rows_ref, gain_ref, gate_ref, up_ref, down_ref, squares_ref, gate_in, up_in,
    hidden_ref, out_ref, scaled, gate_half, up_half, down_half,
):
    other = 1 - place_ref[2]
    pick_half(other, gate_ref, gate_half)
    pick_half(other, up_ref, up_half)
    for y in range(rows_ref.shape[0]):
        at = pl.ds(pl.multiple_of((2 * y + other) * 128, 128), 128)
        down_half[:, y * 128 : (y + 1) * 128] = down_ref[:, at]

    def step(i, carry):
        at = pl.ds(pl.multiple_of(i * chunk, chunk), chunk)
        squares, gate, upward = half_products(
            rows_ref, gain_ref, gate_half, up_half, other, at, scaled
        )
        squares = squares + squares_ref[at, 0:1]
        scale = lax.rsqrt(squares / D + stream_eps)
        gate = (gate + gate_in[at, :]) * scale
        upward = (upward + up_in[at, :]) * scale
        hidden = (jax.nn.silu(gate) * upward).astype(jnp.bfloat16)
        hidden_ref[at, :] = hidden
        part = jnp.dot(hidden, down_half[...], preferred_element_type=jnp.float32)
        for y in range(rows_ref.shape[0]):
            out_ref[y, at, :] = part[:, y * 128 : (y + 1) * 128].astype(jnp.bfloat16)
        return carry

    lax.fori_loop(0, rows_ref.shape[1] // chunk, step, 0)


def own_half_kernel(chunk, place_ref, hidden_ref, down_ref, out_ref, down_half):
    core = place_ref[2]
    for y in range(out_ref.shape[0]):
        at = pl.ds(pl.multiple_of((2 * y + core) * 128, 128), 128)
        down_half[:, y * 128 : (y + 1) * 128] = down_ref[:, at]

    def step(i, carry):
        at = pl.ds(pl.multiple_of(i * chunk, chunk), chunk)
        part = jnp.dot(hidden_ref[at, :], down_half[...], preferred_element_type=jnp.float32)
        for y in range(out_ref.shape[0]):
            out_ref[y, at, :] = part[:, y * 128 : (y + 1) * 128].astype(jnp.bfloat16)
        return carry

    lax.fori_loop(0, hidden_ref.shape[0] // chunk, step, 0)


def final_kernel(returned_ref, stream_ref, col_ref, out_ref):
    length = stream_ref.shape[0]
    slot = iota((length, returned_ref.shape[0]), 1).astype(jnp.float32)
    returned = returned_ref[...]
    total = stream_ref[...].astype(jnp.float32)
    for k in range(2):
        chosen = jnp.where(col_ref[:, 8 + k : 9 + k] == slot, 1.0, 0.0).astype(jnp.bfloat16)
        picked = jnp.dot(chosen, returned, preferred_element_type=jnp.float32)
        total = total + col_ref[:, 10 + k : 11 + k] * picked
    out_ref[...] = total.astype(jnp.bfloat16)


def swapped(value):
    return lax.ppermute(value, "c", [(0, 1), (1, 0)])


def to_all(shard, axis):
    peers = lax.axis_size(axis)
    copies = jnp.broadcast_to(shard[None], (peers, *shard.shape))
    return lax.all_to_all(copies, axis, 0, 0, tiled=True)


def body(
    skip_stream_entering,
    unfiltered_channel_feed,
    unfiltered_state_entry,
    unfiltered_state_exit,
    final_valve_preactivation,
    increment_preactivation,
    summed_attenuation_both_ways,
    channel_fading_speed,
    channel_feed_filter,
    state_entry_filter,
    state_exit_filter,
    clustered_rescale_factor,
    final_projection_weights,
    specialist_rescale_factor,
    item_specialist_couple,
    selected_cluster_likelihood,
    selected_twin_scores_raw,
    specialist_gating_weights,
    specialist_raising_weights,
    specialist_lowering_weights,
):
    f32, bf16 = jnp.float32, jnp.bfloat16
    length, width = unfiltered_channel_feed.shape
    blocks = lax.axis_size(SP)
    peers_x, peers_y, peers_z = (lax.axis_size(a) for a in ("x", "y", "z"))
    capacity = 4 * length // blocks
    slots = blocks * capacity
    axes = [lax.axis_index(a) for a in ("x", "z", "c")]
    place = jnp.stack([*axes, axes[0] % 2]).astype(jnp.int32)

    rim = CONV // 2
    even_rim, odd_rim, *feeds = call(
        rim_kernel,
        "rim",
        [((rim, 3 * width), f32)] * 2 + [((length, width), bf16)] * 3,
        (place, unfiltered_channel_feed, unfiltered_state_entry, unfiltered_state_exit),
        flops=100_000,
        scratch=[pltpu.SemaphoreType.DMA((3,))],
        smem=1,
        hbm=3,
    )
    pairs = [(i, i + 1) for i in range(blocks - 1)]
    even_rim = lax.ppermute(even_rim, SP, [p for a, b in pairs[0::2] for p in ((a, b), (b, a))])
    odd_rim = lax.ppermute(odd_rim, SP, [p for a, b in pairs[1::2] for p in ((a, b), (b, a))])
    filters = (channel_feed_filter, state_entry_filter, state_exit_filter)
    heads = increment_preactivation.shape[1]
    rows, cols, *filters = call(
        functools.partial(table_kernel, capacity),
        "table",
        [((16, length), f32), ((length, length), f32)] + [((CONV, width), f32)] * 3,
        (
            increment_preactivation,
            summed_attenuation_both_ways,
            channel_fading_speed,
            item_specialist_couple.T,
            selected_cluster_likelihood[None],
            selected_twin_scores_raw.T,
            *filters,
        ),
        flops=4_000_000,
        scratch=[
            pltpu.VMEM((2, heads, length), f32),
            pltpu.VMEM((2, heads, length), f32),
            pltpu.VMEM((2, heads), f32),
            pltpu.VMEM((2, length), jnp.int32),
            pltpu.VMEM((1, length), f32),
            pltpu.VMEM((2, length), f32),
            pltpu.SemaphoreType.DMA((9,)),
        ],
        hbm=9,
    )
    message, x_conv, b_conv, c_conv = call(
        conv_kernel,
        "conv",
        [((peers_x, 2 * width + 16, NS), bf16)] + [((length, width), bf16)] * 3,
        (place, *feeds, even_rim, odd_rim, *filters, cols),
        flops=4_000_000,
        scratch=[pltpu.VMEM((length + 16, width), f32)],
        smem=1,
    )
    seen = lax.all_to_all(message, "x", 0, 0, tiled=True)
    onward, near, ahead = call(
        row_kernel,
        "row",
        [((peers_z, width + 16, NS), bf16), ((2, width, NS), f32), ((8, NS), f32)],
        (place, seen),
        smem=1,
    )
    got = lax.all_to_all(onward, "z", 0, 0, tiled=True)
    (copies,) = call(
        mixed_kernel,
        "mixed",
        [((peers_y, length, width), bf16)],
        (
            place, got, near, ahead, x_conv, b_conv, c_conv, rows, cols,
            final_valve_preactivation, clustered_rescale_factor[None],
        ),
        smem=1,
    )
    gathered = lax.all_gather(
        lax.all_to_all(copies, "y", 0, 0, tiled=True), "c", axis=1, tiled=True
    )
    stream, outgoing = call(
        stream_kernel,
        "stream",
        [((length, width), bf16), ((slots, width), bf16)],
        (gathered, final_projection_weights, skip_stream_entering, rows),
    )
    arrived = lax.all_to_all(
        outgoing.reshape(blocks, capacity, width), SP, 0, 0, tiled=True
    ).reshape(slots, width)
    own = to_all(arrived, "y")
    theirs = swapped(own)
    chunk = 256
    wide = (peers_y, 2, 128)
    gain = specialist_rescale_factor.reshape(wide)
    weight_gate = specialist_gating_weights.reshape(*wide, -1)
    weight_up = specialist_raising_weights.reshape(*wide, -1)
    weight_down = specialist_lowering_weights[0]
    units = weight_down.shape[0]
    half = pltpu.VMEM((D // 2, units), bf16)
    down_half = pltpu.VMEM((units, D // 2), bf16)
    scaled = pltpu.VMEM((chunk, D // 2), bf16)
    squares, gate, upward = call(
        functools.partial(first_half_kernel, chunk),
        "first_half",
        [((slots, 128), f32), ((slots, units), f32), ((slots, units), f32)],
        (place, own, gain, weight_gate, weight_up),
        flops=4 * slots * units * D // 2,
        scratch=[scaled, half, half],
        smem=1,
        room=16,
    )
    hidden, sent = call(
        functools.partial(second_half_kernel, chunk),
        "second_half",
        [((slots, units), bf16), ((peers_y, slots, width), bf16)],
        (place, theirs, gain, weight_gate, weight_up, weight_down, squares, gate, upward),
        flops=6 * slots * units * D // 2,
        scratch=[scaled, half, half, down_half],
        smem=1,
        room=20,
    )
    partner = swapped(sent)
    (kept,) = call(
        functools.partial(own_half_kernel, chunk),
        "own_half",
        [((peers_y, slots, width), bf16)],
        (place, hidden, weight_down),
        flops=2 * slots * units * D // 2,
        scratch=[down_half],
        smem=1,
        room=12,
    )
    pair = (kept.astype(f32) + partner.astype(f32)).astype(bf16)
    whole = lax.all_to_all(pair, "y", 0, 0, tiled=True)
    answer = jnp.sum(whole.astype(f32), axis=0).astype(bf16)
    returned = lax.all_to_all(
        answer.reshape(blocks, capacity, width), SP, 0, 0, tiled=True
    ).reshape(slots, width)
    (out,) = call(final_kernel, "final", [((length, width), bf16)], (returned, stream, cols))
    return out


def solution(mesh):
    sizes = dict(mesh.shape)
    torus = Mesh(mesh.devices.reshape(8, 4, sizes["tp"] // 2, 2), ("z", "x", "y", "c"))
    return jax.shard_map(
        body,
        mesh=torus,
        in_specs=(
            P(SP, TP),
            P(SP, TP),
            P(SP, TP),
            P(SP, TP),
            P(SP, TP),
            P(None, TP, SP),
            P(None, TP, SP),
            P(None, TP),
            P(None, TP),
            P(None, TP),
            P(None, TP),
            P(TP),
            P(None, TP),
            P(),
            P(SP, None),
            P(SP),
            P(SP, None),
            P(SP, None, TP),
            P(SP, None, TP),
            P(SP, TP, None),
        ),
        out_specs=P(SP, TP),
        check_vma=False,
    )
```

```python
import functools

import jax
import jax.numpy as jnp
from jax import lax
from jax.experimental import pallas as pl
from jax.experimental.pallas import tpu as pltpu
from jax.sharding import Mesh
from jax.sharding import PartitionSpec as P

D = 2048
HD = 64
NS = 128
CONV = 5
SP = ("z", "x")
TP = ("y", "c")

HIGHEST = lax.Precision.HIGHEST
group_eps = 1e-05
stream_eps = 1e-06

VMEM = pl.BlockSpec(memory_space=pltpu.VMEM)
SMEM = pl.BlockSpec(memory_space=pltpu.SMEM)
HBM = pl.BlockSpec(memory_space=pltpu.HBM)
MIB = 1 << 20


def call(kernel, name, outs, args, flops=1000, scratch=(), room=8, smem=0, hbm=0):
    shapes = [jax.ShapeDtypeStruct(shape, dtype) for shape, dtype in outs]
    moved = sum(a.size * a.dtype.itemsize for a in args) + sum(
        o.size * o.dtype.itemsize for o in shapes
    )
    args = list(args)
    for n in range(smem, smem + hbm):
        args[n] = pltpu.with_memory_space_constraint(args[n], pltpu.HBM)
    return pl.pallas_call(
        kernel,
        out_shape=shapes,
        in_specs=[SMEM] * smem + [HBM] * hbm + [VMEM] * (len(args) - smem - hbm),
        out_specs=[VMEM] * len(shapes),
        scratch_shapes=list(scratch),
        compiler_params=pltpu.CompilerParams(vmem_limit_bytes=room * MIB),
        cost_estimate=pl.CostEstimate(flops=flops, bytes_accessed=moved, transcendentals=0),
        name=name,
    )(*args)


def exact_dot(a, b):
    return jnp.dot(a, b, precision=HIGHEST, preferred_element_type=jnp.float32)


def dot_rows(a, b, precision=None):
    return lax.dot_general(
        a,
        b,
        (((1,), (1,)), ((), ())),
        precision=precision,
        preferred_element_type=jnp.float32,
    )


def iota(shape, dim):
    return lax.broadcasted_iota(jnp.int32, shape, dim)


def fetch(pairs, done):
    copies = [pltpu.make_async_copy(a, b, done.at[n]) for n, (a, b) in enumerate(pairs)]
    for copy in copies:
        copy.start()
    for copy in copies:
        copy.wait()


def rim_kernel(place_ref, x_in, b_in, c_in, even_ref, odd_ref, x_ref, b_ref, c_ref, done):
    fetch(((x_in, x_ref), (b_in, b_ref), (c_in, c_ref)), done)
    even = place_ref[3] == 0
    length, width = x_ref.shape
    for n, ref in enumerate((x_ref, b_ref, c_ref)):
        lanes = slice(n * width, (n + 1) * width)
        top = ref[0:16, :].astype(jnp.float32)[0:2]
        tail = ref[length - 16 : length, :].astype(jnp.float32)[14:16]
        even_ref[:, lanes] = jnp.where(even, tail, top)
        odd_ref[:, lanes] = jnp.where(even, top, tail)


def table_kernel(
    capacity, step_in, fade_in, speed_in, named_in, like_in, score_in, kx_in, kb_in, kc_in,
    row_ref, col_ref, kx_ref, kb_ref, kc_ref,
    step_ref, fade_ref, speed_ref, named_ref, like_ref, score_ref, done,
):
    fetch(
        (
            (step_in, step_ref), (fade_in, fade_ref), (speed_in, speed_ref), (named_in, named_ref),
            (like_in, like_ref), (score_in, score_ref), (kx_in, kx_ref), (kb_in, kb_ref), (kc_in, kc_ref),
        ),
        done,
    )
    length = row_ref.shape[1]
    for d in range(2):
        raw = step_ref[d]
        step = jnp.maximum(raw, 0.0) + jnp.log1p(jnp.exp(-jnp.abs(raw)))
        row_ref[4 + 2 * d : 6 + 2 * d, :] = step
        for h in range(2):
            k = 2 * d + h
            row_ref[k : k + 1, :] = (
                -step[h : h + 1] * speed_ref[d : d + 1, h : h + 1] + fade_ref[d][h : h + 1]
            )
    whole = row_ref[0:8, :]
    lane, line = iota(whole.shape, 1), iota(whole.shape, 0)
    ahead = behind = whole
    reach = 1
    while reach < length:
        ahead = ahead + jnp.where(lane >= reach, pltpu.roll(ahead, reach, 1), 0.0)
        behind = behind + jnp.where(lane < length - reach, pltpu.roll(behind, length - reach, 1), 0.0)
        reach *= 2
    row_ref[0:8, :] = jnp.where(line < 2, ahead, jnp.where(line < 4, behind, whole))
    experts = 32
    expert = iota((experts, length), 0)
    hit = [named_ref[k : k + 1, :] == expert for k in range(2)]
    earlier = iota((length, length), 0) < iota((length, length), 1)
    ranking = jnp.dot(
        jnp.where(hit[0] | hit[1], 1.0, 0.0).astype(jnp.bfloat16),
        jnp.where(earlier, 1.0, 0.0).astype(jnp.bfloat16),
        preferred_element_type=jnp.float32,
    )
    place = ranking + expert.astype(jnp.float32) * capacity
    for k in range(2):
        row_ref[8 + k : 9 + k, :] = jnp.sum(jnp.where(hit[k], place, 0.0), axis=0, keepdims=True)
    first = jax.nn.sigmoid(score_ref[0:1, :] - score_ref[1:2, :])
    row_ref[10:11, :] = like_ref[...] * first
    row_ref[11:12, :] = like_ref[...] * (1.0 - first)
    row_ref[12:16, :] = jnp.zeros((4, length), jnp.float32)
    col_ref[...] = jnp.zeros_like(col_ref)
    col_ref[0:16, :] = row_ref[...]
    col_ref[...] = jnp.transpose(col_ref[...])


def conv_kernel(
    place_ref, x_ref, b_ref, c_ref, even_ref, odd_ref, kx_ref, kb_ref, kc_ref, col_ref,
    message_ref, xs_ref, bs_ref, cs_ref, padded,
):
    length, width = x_ref.shape
    even = place_ref[3] == 0
    before = jnp.where(even, odd_ref[...], even_ref[...])
    after = jnp.where(even, even_ref[...], odd_ref[...])
    parts = []
    for n, (ref, taps) in enumerate(((x_ref, kx_ref), (b_ref, kb_ref), (c_ref, kc_ref))):
        lanes = slice(n * width, (n + 1) * width)
        padded[8 : 8 + length, :] = ref[...].astype(jnp.float32)
        padded[6:8, :] = before[:, lanes]
        padded[8 + length : 10 + length, :] = after[:, lanes]
        total = jnp.zeros((length, width), jnp.float32)
        for k in range(CONV):
            total = total + taps[k : k + 1, :] * padded[6 + k : 6 + k + length, :]
        parts.append(jax.nn.silu(total).astype(jnp.bfloat16))
    xs_ref[...], bs_ref[...], cs_ref[...] = parts
    x_block = parts[0].astype(jnp.float32)
    b_block = parts[1].astype(jnp.float32)
    left = iota((length, width), 1) < HD
    logs = jnp.zeros((16, width), jnp.float32)
    line = iota((16, width), 0)
    for d, last in ((0, length - 1), (1, 0)):
        weight = []
        for h in range(2):
            k = 2 * d + h
            end = col_ref[last : last + 1, k : k + 1]
            weight.append(jnp.exp(end - col_ref[:, k : k + 1]) * col_ref[:, 4 + k : 5 + k])
            high = end.astype(jnp.bfloat16).astype(jnp.float32)
            logs = jnp.where(line == 4 * d + h, high, logs)
            logs = jnp.where(line == 4 * d + 2 + h, end - high, logs)
        scaled = x_block * jnp.where(left, weight[0], weight[1])
        state = exact_dot(jnp.transpose(scaled), b_block).astype(jnp.bfloat16)
        for peer in range(message_ref.shape[0]):
            message_ref[peer, d * width : (d + 1) * width, :] = state
    for peer in range(message_ref.shape[0]):
        message_ref[peer, 2 * width :, :] = logs.astype(jnp.bfloat16)


def within(xs_ref, bs_ref, cs_ref, row_ref, col_ref):
    length, width = xs_ref.shape
    scores = dot_rows(cs_ref[...], bs_ref[...])
    x_block = xs_ref[...].astype(jnp.float32)
    to, since = iota((length, length), 0), iota((length, length), 1)
    sides = []
    for h in range(2):
        both = jnp.zeros((length, length), jnp.float32)
        for d in range(2):
            k = 2 * d + h
            seen = since <= to if d == 0 else since >= to
            passed = col_ref[:, k : k + 1] - row_ref[k : k + 1, :]
            decay = jnp.where(seen, jnp.exp(jnp.minimum(passed, 0.0)), 0.0)
            both = both + decay * row_ref[4 + k : 5 + k, :]
        sides.append(exact_dot(scores * both, x_block))
    return jnp.where(iota((length, width), 1) < HD, sides[0], sides[1])


def log_pair(tile, d):
    return [tile[4 * d + h : 4 * d + h + 1, :] + tile[4 * d + 2 + h : 4 * d + 3 + h, :] for h in range(2)]


def by_head(pair, rows):
    return jnp.where(iota((rows, 128), 0) < HD, pair[0], pair[1])


def row_kernel(place_ref, seen_ref, message_ref, near_ref, ahead_ref):
    my_x, my_z = place_ref[0], place_ref[1]
    peers, rows = seen_ref.shape[0], near_ref.shape[1]
    line = iota((16, 128), 0)
    out = []
    ahead_ref[...] = jnp.zeros_like(ahead_ref)
    for d in range(2):
        total = near = jnp.zeros((rows, 128), jnp.float32)
        far = [jnp.zeros((1, 128), jnp.float32)] * 2
        ahead = list(far)
        for k in range(peers) if d == 0 else reversed(range(peers)):
            logs = log_pair(seen_ref[k, 2 * rows :, :].astype(jnp.float32), d)
            near = jnp.where(k == my_x, total, near)
            passed = k < my_x if d == 0 else k > my_x
            state = seen_ref[k, d * rows : (d + 1) * rows, :].astype(jnp.float32)
            total = total * jnp.exp(by_head(logs, rows)) + state
            for h in range(2):
                far[h] = far[h] + logs[h]
                ahead[h] = ahead[h] + jnp.where(passed, logs[h], 0.0)
        near_ref[d] = near
        tile = jnp.zeros((16, 128), jnp.float32)
        for h in range(2):
            ahead_ref[2 * d + h : 2 * d + h + 1, :] = ahead[h]
            high = far[h].astype(jnp.bfloat16).astype(jnp.float32)
            tile = jnp.where(line == h, high, tile)
            tile = jnp.where(line == 2 + h, far[h] - high, tile)
        out.append((total, tile))
    for k in range(message_ref.shape[0]):
        onward = k > my_z
        message_ref[k, :rows, :] = jnp.where(onward, out[0][0], out[1][0]).astype(jnp.bfloat16)
        message_ref[k, rows:, :] = jnp.where(onward, out[0][1], out[1][1]).astype(jnp.bfloat16)


def mixed_kernel(
    place_ref, got_ref, near_ref, ahead_ref, xs_ref, bs_ref, cs_ref, row_ref, col_ref, valve_ref, gain_ref,
    out_ref,
):
    my_z = place_ref[1]
    peers, rows = got_ref.shape[0], near_ref.shape[1]
    length = cs_ref.shape[0]
    c_block = cs_ref[...].astype(jnp.float32)
    left = iota((length, rows), 1) < HD
    mixer = within(xs_ref, bs_ref, cs_ref, row_ref, col_ref)
    for d in range(2):
        state = jnp.zeros((rows, 128), jnp.float32)
        for k in range(peers) if d == 0 else reversed(range(peers)):
            passed = k < my_z if d == 0 else k > my_z
            logs = log_pair(got_ref[k, rows:, :].astype(jnp.float32), 0)
            onto = state * jnp.exp(by_head(logs, rows)) + got_ref[k, :rows, :].astype(jnp.float32)
            state = jnp.where(passed, onto, state)
        ahead = [ahead_ref[2 * d + h : 2 * d + h + 1, :] for h in range(2)]
        state = state * jnp.exp(by_head(ahead, rows)) + near_ref[d]
        factor = jnp.exp(
            jnp.where(left, col_ref[:, 2 * d : 2 * d + 1], col_ref[:, 2 * d + 1 : 2 * d + 2])
        )
        mixer = mixer + dot_rows(c_block, state, HIGHEST) * factor
    gated = mixer * jax.nn.silu(valve_ref[...].astype(jnp.float32))
    gated = gated * lax.rsqrt(jnp.mean(gated * gated, axis=-1, keepdims=True) + group_eps)
    mixed = (gated * gain_ref[...]).astype(jnp.bfloat16)
    for k in range(out_ref.shape[0]):
        out_ref[k] = mixed


def stream_kernel(mixed_ref, weight_ref, skip_ref, row_ref, stream_ref, out_ref):
    length, width = skip_ref.shape
    places = mixed_ref.shape[0]
    total = skip_ref[...].astype(jnp.float32)
    product = jnp.zeros((length, width), jnp.float32)
    for y in range(places):
        both = jnp.concatenate([mixed_ref[y, :length, :], mixed_ref[y, length:, :]], axis=1)
        product = product + jnp.dot(
            both, weight_ref[2 * y * width : 2 * (y + 1) * width, :], preferred_element_type=jnp.float32
        )
    stream = (total + product).astype(jnp.bfloat16)
    stream_ref[...] = stream
    blocks, places, cores, half, _ = out_ref.shape
    slot = iota((blocks * cores * half, length), 0).astype(jnp.float32)
    chosen = (row_ref[8:9, :] == slot) | (row_ref[9:10, :] == slot)
    picked = jnp.dot(
        jnp.where(chosen, 1.0, 0.0).astype(jnp.bfloat16), stream, preferred_element_type=jnp.float32
    )
    picked = picked.reshape(blocks, cores, half, width).astype(jnp.bfloat16)
    for y in range(places):
        out_ref[:, y] = picked


def expert_kernel(
    rows_ref, gain_ref, gate_own, gate_other, up_own, up_other, down_own, down_other, out_ref, scaled
):
    blocks, features, half, lanes = rows_ref.shape
    count = blocks * half
    squares = jnp.zeros((count, lanes), jnp.float32)
    for k in range(features):
        part = rows_ref[:, k].astype(jnp.float32).reshape(count, lanes)
        squares = squares + part * part
        at = slice(k * lanes, (k + 1) * lanes)
        scaled[:, at] = (part * gain_ref[:, at]).astype(jnp.bfloat16)
    scale = lax.rsqrt(jnp.sum(squares, axis=1, keepdims=True) / D + stream_eps)
    whole = scaled[...]
    hidden = []
    for gate_ref, up_ref in ((gate_own, up_own), (gate_other, up_other)):
        gate = jnp.dot(whole, gate_ref[...], preferred_element_type=jnp.float32) * scale
        upward = jnp.dot(whole, up_ref[...], preferred_element_type=jnp.float32) * scale
        hidden.append((jax.nn.silu(gate) * upward).astype(jnp.bfloat16))
    step = 2 * lanes
    for j in range(features // 2):
        at = slice(j * step, (j + 1) * step)
        part = jnp.dot(hidden[0], down_own[:, at], preferred_element_type=jnp.float32)
        part = part + jnp.dot(hidden[1], down_other[:, at], preferred_element_type=jnp.float32)
        for n in range(2):
            tile = part[:, n * lanes : (n + 1) * lanes].reshape(blocks, half, lanes)
            out_ref[:, 2 * j + n] = tile.astype(jnp.bfloat16)


def final_kernel(returned_ref, stream_ref, col_ref, out_ref):
    length, width = stream_ref.shape
    blocks, places, cores, half, _ = returned_ref.shape
    slots = blocks * cores * half
    slot = iota((length, slots), 1).astype(jnp.float32)
    answer = returned_ref[:, 0].astype(jnp.float32)
    for y in range(1, places):
        answer = answer + returned_ref[:, y].astype(jnp.float32)
    returned = answer.reshape(slots, width).astype(jnp.bfloat16)
    total = stream_ref[...].astype(jnp.float32)
    for k in range(2):
        chosen = jnp.where(col_ref[:, 8 + k : 9 + k] == slot, 1.0, 0.0).astype(jnp.bfloat16)
        picked = jnp.dot(chosen, returned, preferred_element_type=jnp.float32)
        total = total + col_ref[:, 10 + k : 11 + k] * picked
    out_ref[...] = total.astype(jnp.bfloat16)


def swapped(value):
    return lax.ppermute(value, "c", [(0, 1), (1, 0)])


def body(
    skip_stream_entering,
    unfiltered_channel_feed,
    unfiltered_state_entry,
    unfiltered_state_exit,
    final_valve_preactivation,
    increment_preactivation,
    summed_attenuation_both_ways,
    channel_fading_speed,
    channel_feed_filter,
    state_entry_filter,
    state_exit_filter,
    clustered_rescale_factor,
    final_projection_weights,
    specialist_rescale_factor,
    item_specialist_couple,
    selected_cluster_likelihood,
    selected_twin_scores_raw,
    specialist_gating_weights,
    specialist_raising_weights,
    specialist_lowering_weights,
):
    f32, bf16 = jnp.float32, jnp.bfloat16
    length, width = unfiltered_channel_feed.shape
    blocks = lax.axis_size(SP)
    peers_x, peers_y, peers_z = (lax.axis_size(a) for a in ("x", "y", "z"))
    capacity = 4 * length // blocks
    slots = blocks * capacity
    axes = [lax.axis_index(a) for a in ("x", "z", "c")]
    place = jnp.stack([*axes, axes[0] % 2]).astype(jnp.int32)

    rim = CONV // 2
    even_rim, odd_rim, *feeds = call(
        rim_kernel,
        "rim",
        [((rim, 3 * width), f32)] * 2 + [((length, width), bf16)] * 3,
        (place, unfiltered_channel_feed, unfiltered_state_entry, unfiltered_state_exit),
        flops=100_000,
        scratch=[pltpu.SemaphoreType.DMA((3,))],
        smem=1,
        hbm=3,
    )
    pairs = [(i, i + 1) for i in range(blocks - 1)]
    even_rim = lax.ppermute(even_rim, SP, [p for a, b in pairs[0::2] for p in ((a, b), (b, a))])
    odd_rim = lax.ppermute(odd_rim, SP, [p for a, b in pairs[1::2] for p in ((a, b), (b, a))])
    filters = (channel_feed_filter, state_entry_filter, state_exit_filter)
    heads = increment_preactivation.shape[1]
    rows, cols, *filters = call(
        functools.partial(table_kernel, capacity),
        "table",
        [((16, length), f32), ((length, length), f32)] + [((CONV, width), f32)] * 3,
        (
            increment_preactivation,
            summed_attenuation_both_ways,
            channel_fading_speed,
            item_specialist_couple.T,
            selected_cluster_likelihood[None],
            selected_twin_scores_raw.T,
            *filters,
        ),
        flops=4_000_000,
        scratch=[
            pltpu.VMEM((2, heads, length), f32),
            pltpu.VMEM((2, heads, length), f32),
            pltpu.VMEM((2, heads), f32),
            pltpu.VMEM((2, length), jnp.int32),
            pltpu.VMEM((1, length), f32),
            pltpu.VMEM((2, length), f32),
            pltpu.SemaphoreType.DMA((9,)),
        ],
        hbm=9,
    )
    rows, gate_own, up_own, down_own = lax.optimization_barrier(
        (
            rows,
            specialist_gating_weights[0],
            specialist_raising_weights[0],
            specialist_lowering_weights[0],
        )
    )
    gate_other, up_other, down_other = swapped(gate_own), swapped(up_own), swapped(down_own)
    message, x_conv, b_conv, c_conv = call(
        conv_kernel,
        "conv",
        [((peers_x, 2 * width + 16, NS), bf16)] + [((length, width), bf16)] * 3,
        (place, *feeds, even_rim, odd_rim, *filters, cols),
        flops=4_000_000,
        scratch=[pltpu.VMEM((length + 16, width), f32)],
        smem=1,
    )
    seen = lax.all_to_all(message, "x", 0, 0, tiled=True)
    onward, near, ahead = call(
        row_kernel,
        "row",
        [((peers_z, width + 16, NS), bf16), ((2, width, NS), f32), ((8, NS), f32)],
        (place, seen),
        smem=1,
    )
    got = lax.all_to_all(onward, "z", 0, 0, tiled=True)
    (copies,) = call(
        mixed_kernel,
        "mixed",
        [((peers_y, length, width), bf16)],
        (
            place, got, near, ahead, x_conv, b_conv, c_conv, rows, cols,
            final_valve_preactivation, clustered_rescale_factor[None],
        ),
        smem=1,
    )
    gathered = lax.all_gather(
        lax.all_to_all(copies, "y", 0, 0, tiled=True), "c", axis=1, tiled=True
    )
    half = capacity // 2
    spread = (blocks, peers_y, 2, half, width)
    everyone = (*SP, *TP)
    stream, outgoing = call(
        stream_kernel,
        "stream",
        [((length, width), bf16), (spread, bf16)],
        (gathered, final_projection_weights, skip_stream_entering, rows),
    )
    arrived = lax.all_to_all(
        outgoing.reshape(-1, half, width), everyone, 0, 0, tiled=True
    ).reshape(blocks, 2 * peers_y, half, width)
    (partial_out,) = call(
        expert_kernel,
        "expert",
        [(arrived.shape, bf16)],
        (
            arrived, specialist_rescale_factor[None], gate_own, gate_other, up_own, up_other,
            down_own, down_other,
        ),
        flops=6 * slots * gate_own.shape[1] * D,
        scratch=[pltpu.VMEM((slots // 2, D), bf16)],
        room=24,
    )
    returned = lax.all_to_all(
        partial_out.reshape(-1, half, width), everyone, 0, 0, tiled=True
    ).reshape(spread)
    (out,) = call(final_kernel, "final", [((length, width), bf16)], (returned, stream, cols))
    return out


def solution(mesh):
    sizes = dict(mesh.shape)
    torus = Mesh(mesh.devices.reshape(8, 4, sizes["tp"] // 2, 2), ("z", "x", "y", "c"))
    return jax.shard_map(
        body,
        mesh=torus,
        in_specs=(
            P(SP, TP),
            P(SP, TP),
            P(SP, TP),
            P(SP, TP),
            P(SP, TP),
            P(None, TP, SP),
            P(None, TP, SP),
            P(None, TP),
            P(None, TP),
            P(None, TP),
            P(None, TP),
            P(TP),
            P(None, TP),
            P(),
            P(SP, None),
            P(SP),
            P(SP, None),
            P(SP, None, TP),
            P(SP, None, TP),
            P(SP, TP, None),
        ),
        out_specs=P(SP, TP),
        check_vma=False,
    )
```

```python
import functools

import jax
import jax.numpy as jnp
from jax import lax
from jax.experimental import pallas as pl
from jax.experimental.pallas import tpu as pltpu
from jax.sharding import Mesh
from jax.sharding import PartitionSpec as P


D = 2048
HD = 64
NS = 128
CONV = 5
SP = ("z", "x")
TP = ("y", "c")

HIGHEST = lax.Precision.HIGHEST
group_eps = 1e-05
stream_eps = 1e-06

VMEM = pl.BlockSpec(memory_space=pltpu.VMEM)
SMEM = pl.BlockSpec(memory_space=pltpu.SMEM)
HBM = pl.BlockSpec(memory_space=pltpu.HBM)
MIB = 1 << 20


def call(kernel, outs, args, flops=1000, scratch=(), room=8, smem=0, hbm=0):
    shapes = [jax.ShapeDtypeStruct(shape, dtype) for shape, dtype in outs]
    moved = sum(a.size * a.dtype.itemsize for a in args) + sum(
        o.size * o.dtype.itemsize for o in shapes
    )
    args = list(args)
    for n in range(smem, smem + hbm):
        args[n] = pltpu.with_memory_space_constraint(args[n], pltpu.HBM)
    return pl.pallas_call(
        kernel,
        out_shape=shapes,
        in_specs=[SMEM] * smem + [HBM] * hbm + [VMEM] * (len(args) - smem - hbm),
        out_specs=[VMEM] * len(shapes),
        scratch_shapes=list(scratch),
        compiler_params=pltpu.CompilerParams(vmem_limit_bytes=room * MIB),
        cost_estimate=pl.CostEstimate(flops=flops, bytes_accessed=moved, transcendentals=0),
    )(*args)


def exact_dot(a, b):
    return jnp.dot(a, b, precision=HIGHEST, preferred_element_type=jnp.float32)


def dot_rows(a, b, precision=None):
    return lax.dot_general(
        a,
        b,
        (((1,), (1,)), ((), ())),
        precision=precision,
        preferred_element_type=jnp.float32,
    )


def iota(shape, dim):
    return lax.broadcasted_iota(jnp.int32, shape, dim)


def fetch(pairs, done):
    copies = [pltpu.make_async_copy(a, b, done.at[n]) for n, (a, b) in enumerate(pairs)]
    for copy in copies:
        copy.start()
    for copy in copies:
        copy.wait()


def rim_kernel(place_ref, x_in, b_in, c_in, even_ref, odd_ref, x_ref, b_ref, c_ref, done):
    fetch(((x_in, x_ref), (b_in, b_ref), (c_in, c_ref)), done)
    even = place_ref[3] == 0
    length, width = x_ref.shape
    for n, ref in enumerate((x_ref, b_ref, c_ref)):
        lanes = slice(n * width, (n + 1) * width)
        top = ref[0:16, :].astype(jnp.float32)[0:2]
        tail = ref[length - 16 : length, :].astype(jnp.float32)[14:16]
        even_ref[:, lanes] = jnp.where(even, tail, top)
        odd_ref[:, lanes] = jnp.where(even, top, tail)


def table_kernel(
    capacity, step_in, fade_in, speed_in, named_in, like_in, score_in, kx_in, kb_in, kc_in,
    row_ref, col_ref, kx_ref, kb_ref, kc_ref,
    step_ref, fade_ref, speed_ref, named_ref, like_ref, score_ref, done,
):
    fetch(
        (
            (step_in, step_ref), (fade_in, fade_ref), (speed_in, speed_ref), (named_in, named_ref),
            (like_in, like_ref), (score_in, score_ref), (kx_in, kx_ref), (kb_in, kb_ref), (kc_in, kc_ref),
        ),
        done,
    )
    length = row_ref.shape[1]
    for d in range(2):
        raw = step_ref[d]
        step = jnp.maximum(raw, 0.0) + jnp.log1p(jnp.exp(-jnp.abs(raw)))
        row_ref[4 + 2 * d : 6 + 2 * d, :] = step
        for h in range(2):
            k = 2 * d + h
            row_ref[k : k + 1, :] = (
                -step[h : h + 1] * speed_ref[d : d + 1, h : h + 1] + fade_ref[d][h : h + 1]
            )
    whole = row_ref[0:8, :]
    lane, line = iota(whole.shape, 1), iota(whole.shape, 0)
    ahead = behind = whole
    reach = 1
    while reach < length:
        ahead = ahead + jnp.where(lane >= reach, pltpu.roll(ahead, reach, 1), 0.0)
        behind = behind + jnp.where(lane < length - reach, pltpu.roll(behind, length - reach, 1), 0.0)
        reach *= 2
    row_ref[0:8, :] = jnp.where(line < 2, ahead, jnp.where(line < 4, behind, whole))
    experts = 32
    expert = iota((experts, length), 0)
    hit = [named_ref[k : k + 1, :] == expert for k in range(2)]
    earlier = iota((length, length), 0) < iota((length, length), 1)
    ranking = jnp.dot(
        jnp.where(hit[0] | hit[1], 1.0, 0.0).astype(jnp.bfloat16),
        jnp.where(earlier, 1.0, 0.0).astype(jnp.bfloat16),
        preferred_element_type=jnp.float32,
    )
    place = ranking + expert.astype(jnp.float32) * capacity
    for k in range(2):
        row_ref[8 + k : 9 + k, :] = jnp.sum(jnp.where(hit[k], place, 0.0), axis=0, keepdims=True)
    first = jax.nn.sigmoid(score_ref[0:1, :] - score_ref[1:2, :])
    row_ref[10:11, :] = like_ref[...] * first
    row_ref[11:12, :] = like_ref[...] * (1.0 - first)
    row_ref[12:16, :] = jnp.zeros((4, length), jnp.float32)
    col_ref[...] = jnp.zeros_like(col_ref)
    col_ref[0:16, :] = row_ref[...]
    col_ref[...] = jnp.transpose(col_ref[...])


def conv_kernel(
    place_ref, x_ref, b_ref, c_ref, even_ref, odd_ref, kx_ref, kb_ref, kc_ref, col_ref,
    message_ref, xs_ref, bs_ref, cs_ref, padded,
):
    length, width = x_ref.shape
    even = place_ref[3] == 0
    before = jnp.where(even, odd_ref[...], even_ref[...])
    after = jnp.where(even, even_ref[...], odd_ref[...])
    parts = []
    for n, (ref, taps) in enumerate(((x_ref, kx_ref), (b_ref, kb_ref), (c_ref, kc_ref))):
        lanes = slice(n * width, (n + 1) * width)
        padded[8 : 8 + length, :] = ref[...].astype(jnp.float32)
        padded[6:8, :] = before[:, lanes]
        padded[8 + length : 10 + length, :] = after[:, lanes]
        total = jnp.zeros((length, width), jnp.float32)
        for k in range(CONV):
            total = total + taps[k : k + 1, :] * padded[6 + k : 6 + k + length, :]
        parts.append(jax.nn.silu(total).astype(jnp.bfloat16))
    xs_ref[...], bs_ref[...], cs_ref[...] = parts
    x_block = parts[0].astype(jnp.float32)
    b_block = parts[1].astype(jnp.float32)
    left = iota((length, width), 1) < HD
    logs = jnp.zeros((16, width), jnp.float32)
    line = iota((16, width), 0)
    for d, last in ((0, length - 1), (1, 0)):
        weight = []
        for h in range(2):
            k = 2 * d + h
            end = col_ref[last : last + 1, k : k + 1]
            weight.append(jnp.exp(end - col_ref[:, k : k + 1]) * col_ref[:, 4 + k : 5 + k])
            high = end.astype(jnp.bfloat16).astype(jnp.float32)
            logs = jnp.where(line == 4 * d + h, high, logs)
            logs = jnp.where(line == 4 * d + 2 + h, end - high, logs)
        scaled = x_block * jnp.where(left, weight[0], weight[1])
        state = exact_dot(jnp.transpose(scaled), b_block).astype(jnp.bfloat16)
        for peer in range(message_ref.shape[0]):
            message_ref[peer, d * width : (d + 1) * width, :] = state
    for peer in range(message_ref.shape[0]):
        message_ref[peer, 2 * width :, :] = logs.astype(jnp.bfloat16)


def within(xs_ref, bs_ref, cs_ref, row_ref, col_ref):
    length, width = xs_ref.shape
    scores = dot_rows(cs_ref[...], bs_ref[...])
    x_block = xs_ref[...].astype(jnp.float32)
    to, since = iota((length, length), 0), iota((length, length), 1)
    sides = []
    for h in range(2):
        both = jnp.zeros((length, length), jnp.float32)
        for d in range(2):
            k = 2 * d + h
            seen = since <= to if d == 0 else since >= to
            passed = col_ref[:, k : k + 1] - row_ref[k : k + 1, :]
            decay = jnp.where(seen, jnp.exp(jnp.minimum(passed, 0.0)), 0.0)
            both = both + decay * row_ref[4 + k : 5 + k, :]
        sides.append(exact_dot(scores * both, x_block))
    return jnp.where(iota((length, width), 1) < HD, sides[0], sides[1])


def log_pair(tile, d):
    return [tile[4 * d + h : 4 * d + h + 1, :] + tile[4 * d + 2 + h : 4 * d + 3 + h, :] for h in range(2)]


def by_head(pair, rows):
    return jnp.where(iota((rows, 128), 0) < HD, pair[0], pair[1])


def row_kernel(place_ref, seen_ref, message_ref, near_ref, ahead_ref):
    my_x, my_z = place_ref[0], place_ref[1]
    peers, rows = seen_ref.shape[0], near_ref.shape[1]
    line = iota((16, 128), 0)
    out = []
    ahead_ref[...] = jnp.zeros_like(ahead_ref)
    for d in range(2):
        total = near = jnp.zeros((rows, 128), jnp.float32)
        far = [jnp.zeros((1, 128), jnp.float32)] * 2
        ahead = list(far)
        for k in range(peers) if d == 0 else reversed(range(peers)):
            logs = log_pair(seen_ref[k, 2 * rows :, :].astype(jnp.float32), d)
            near = jnp.where(k == my_x, total, near)
            passed = k < my_x if d == 0 else k > my_x
            state = seen_ref[k, d * rows : (d + 1) * rows, :].astype(jnp.float32)
            total = total * jnp.exp(by_head(logs, rows)) + state
            for h in range(2):
                far[h] = far[h] + logs[h]
                ahead[h] = ahead[h] + jnp.where(passed, logs[h], 0.0)
        near_ref[d] = near
        tile = jnp.zeros((16, 128), jnp.float32)
        for h in range(2):
            ahead_ref[2 * d + h : 2 * d + h + 1, :] = ahead[h]
            high = far[h].astype(jnp.bfloat16).astype(jnp.float32)
            tile = jnp.where(line == h, high, tile)
            tile = jnp.where(line == 2 + h, far[h] - high, tile)
        out.append((total, tile))
    for k in range(message_ref.shape[0]):
        onward = k > my_z
        message_ref[k, :rows, :] = jnp.where(onward, out[0][0], out[1][0]).astype(jnp.bfloat16)
        message_ref[k, rows:, :] = jnp.where(onward, out[0][1], out[1][1]).astype(jnp.bfloat16)


def mixed_kernel(
    place_ref, got_ref, near_ref, ahead_ref, xs_ref, bs_ref, cs_ref, row_ref, col_ref, valve_ref, gain_ref,
    out_ref,
):
    my_z = place_ref[1]
    peers, rows = got_ref.shape[0], near_ref.shape[1]
    length = cs_ref.shape[0]
    c_block = cs_ref[...].astype(jnp.float32)
    left = iota((length, rows), 1) < HD
    mixer = within(xs_ref, bs_ref, cs_ref, row_ref, col_ref)
    for d in range(2):
        state = jnp.zeros((rows, 128), jnp.float32)
        for k in range(peers) if d == 0 else reversed(range(peers)):
            passed = k < my_z if d == 0 else k > my_z
            logs = log_pair(got_ref[k, rows:, :].astype(jnp.float32), 0)
            onto = state * jnp.exp(by_head(logs, rows)) + got_ref[k, :rows, :].astype(jnp.float32)
            state = jnp.where(passed, onto, state)
        ahead = [ahead_ref[2 * d + h : 2 * d + h + 1, :] for h in range(2)]
        state = state * jnp.exp(by_head(ahead, rows)) + near_ref[d]
        factor = jnp.exp(
            jnp.where(left, col_ref[:, 2 * d : 2 * d + 1], col_ref[:, 2 * d + 1 : 2 * d + 2])
        )
        mixer = mixer + dot_rows(c_block, state, HIGHEST) * factor
    gated = mixer * jax.nn.silu(valve_ref[...].astype(jnp.float32))
    gated = gated * lax.rsqrt(jnp.mean(gated * gated, axis=-1, keepdims=True) + group_eps)
    mixed = (gated * gain_ref[...]).astype(jnp.bfloat16)
    for k in range(out_ref.shape[0]):
        out_ref[k] = mixed


def stream_kernel(mixed_ref, weight_ref, skip_ref, row_ref, stream_ref, out_ref):
    length, width = skip_ref.shape
    places = mixed_ref.shape[0]
    total = skip_ref[...].astype(jnp.float32)
    product = jnp.zeros((length, width), jnp.float32)
    for y in range(places):
        both = jnp.concatenate([mixed_ref[y, :length, :], mixed_ref[y, length:, :]], axis=1)
        product = product + jnp.dot(
            both, weight_ref[2 * y * width : 2 * (y + 1) * width, :], preferred_element_type=jnp.float32
        )
    stream = (total + product).astype(jnp.bfloat16)
    stream_ref[...] = stream
    blocks, places, cores, half, _ = out_ref.shape
    slot = iota((blocks * cores * half, length), 0).astype(jnp.float32)
    chosen = (row_ref[8:9, :] == slot) | (row_ref[9:10, :] == slot)
    picked = jnp.dot(
        jnp.where(chosen, 1.0, 0.0).astype(jnp.bfloat16), stream, preferred_element_type=jnp.float32
    )
    picked = picked.reshape(blocks, cores, half, width).astype(jnp.bfloat16)
    for y in range(places):
        out_ref[:, y] = picked


def expert_kernel(
    rows_ref, gain_ref, gate_own, gate_other, up_own, up_other, down_own, down_other, out_ref, scaled
):
    blocks, features, half, lanes = rows_ref.shape
    count = blocks * half
    squares = jnp.zeros((count, lanes), jnp.float32)
    for k in range(features):
        part = rows_ref[:, k].astype(jnp.float32).reshape(count, lanes)
        squares = squares + part * part
        at = slice(k * lanes, (k + 1) * lanes)
        scaled[:, at] = (part * gain_ref[:, at]).astype(jnp.bfloat16)
    scale = lax.rsqrt(jnp.sum(squares, axis=1, keepdims=True) / D + stream_eps)
    whole = scaled[...]
    hidden = []
    for gate_ref, up_ref in ((gate_own, up_own), (gate_other, up_other)):
        gate = jnp.dot(whole, gate_ref[...], preferred_element_type=jnp.float32) * scale
        upward = jnp.dot(whole, up_ref[...], preferred_element_type=jnp.float32) * scale
        hidden.append((jax.nn.silu(gate) * upward).astype(jnp.bfloat16))
    step = 2 * lanes
    for j in range(features // 2):
        at = slice(j * step, (j + 1) * step)
        part = jnp.dot(hidden[0], down_own[:, at], preferred_element_type=jnp.float32)
        part = part + jnp.dot(hidden[1], down_other[:, at], preferred_element_type=jnp.float32)
        for n in range(2):
            tile = part[:, n * lanes : (n + 1) * lanes].reshape(blocks, half, lanes)
            out_ref[:, 2 * j + n] = tile.astype(jnp.bfloat16)


def final_kernel(returned_ref, stream_ref, col_ref, out_ref):
    length, width = stream_ref.shape
    blocks, places, cores, half, _ = returned_ref.shape
    slots = blocks * cores * half
    slot = iota((length, slots), 1).astype(jnp.float32)
    answer = returned_ref[:, 0].astype(jnp.float32)
    for y in range(1, places):
        answer = answer + returned_ref[:, y].astype(jnp.float32)
    returned = answer.reshape(slots, width).astype(jnp.bfloat16)
    total = stream_ref[...].astype(jnp.float32)
    for k in range(2):
        chosen = jnp.where(col_ref[:, 8 + k : 9 + k] == slot, 1.0, 0.0).astype(jnp.bfloat16)
        picked = jnp.dot(chosen, returned, preferred_element_type=jnp.float32)
        total = total + col_ref[:, 10 + k : 11 + k] * picked
    out_ref[...] = total.astype(jnp.bfloat16)


def swapped(value):
    return lax.ppermute(value, "c", [(0, 1), (1, 0)])


def body(
    skip_stream_entering,
    unfiltered_channel_feed,
    unfiltered_state_entry,
    unfiltered_state_exit,
    final_valve_preactivation,
    increment_preactivation,
    summed_attenuation_both_ways,
    channel_fading_speed,
    channel_feed_filter,
    state_entry_filter,
    state_exit_filter,
    clustered_rescale_factor,
    final_projection_weights,
    specialist_rescale_factor,
    item_specialist_couple,
    selected_cluster_likelihood,
    selected_twin_scores_raw,
    specialist_gating_weights,
    specialist_raising_weights,
    specialist_lowering_weights,
):
    f32, bf16 = jnp.float32, jnp.bfloat16
    length, width = unfiltered_channel_feed.shape
    blocks = lax.axis_size(SP)
    peers_x, peers_y, peers_z = (lax.axis_size(a) for a in ("x", "y", "z"))
    capacity = 4 * length // blocks
    slots = blocks * capacity
    axes = [lax.axis_index(a) for a in ("x", "z", "c")]
    place = jnp.stack([*axes, axes[0] % 2]).astype(jnp.int32)

    rim = CONV // 2
    even_rim, odd_rim, *feeds = call(
        rim_kernel,
        [((rim, 3 * width), f32)] * 2 + [((length, width), bf16)] * 3,
        (place, unfiltered_channel_feed, unfiltered_state_entry, unfiltered_state_exit),
        flops=100_000,
        scratch=[pltpu.SemaphoreType.DMA((3,))],
        smem=1,
        hbm=3,
    )
    pairs = [(i, i + 1) for i in range(blocks - 1)]
    even_rim = lax.ppermute(even_rim, SP, [p for a, b in pairs[0::2] for p in ((a, b), (b, a))])
    odd_rim = lax.ppermute(odd_rim, SP, [p for a, b in pairs[1::2] for p in ((a, b), (b, a))])
    filters = (channel_feed_filter, state_entry_filter, state_exit_filter)
    heads = increment_preactivation.shape[1]
    rows, cols, *filters = call(
        functools.partial(table_kernel, capacity),
        [((16, length), f32), ((length, length), f32)] + [((CONV, width), f32)] * 3,
        (
            increment_preactivation,
            summed_attenuation_both_ways,
            channel_fading_speed,
            item_specialist_couple.T,
            selected_cluster_likelihood[None],
            selected_twin_scores_raw.T,
            *filters,
        ),
        flops=4_000_000,
        scratch=[
            pltpu.VMEM((2, heads, length), f32),
            pltpu.VMEM((2, heads, length), f32),
            pltpu.VMEM((2, heads), f32),
            pltpu.VMEM((2, length), jnp.int32),
            pltpu.VMEM((1, length), f32),
            pltpu.VMEM((2, length), f32),
            pltpu.SemaphoreType.DMA((9,)),
        ],
        hbm=9,
    )
    message, x_conv, b_conv, c_conv = call(
        conv_kernel,
        [((peers_x, 2 * width + 16, NS), bf16)] + [((length, width), bf16)] * 3,
        (place, *feeds, even_rim, odd_rim, *filters, cols),
        flops=4_000_000,
        scratch=[pltpu.VMEM((length + 16, width), f32)],
        smem=1,
    )
    seen = lax.all_to_all(message, "x", 0, 0, tiled=True)
    onward, near, ahead = call(
        row_kernel,
        [((peers_z, width + 16, NS), bf16), ((2, width, NS), f32), ((8, NS), f32)],
        (place, seen),
        smem=1,
    )
    got = lax.all_to_all(onward, "z", 0, 0, tiled=True)
    (copies,) = call(
        mixed_kernel,
        [((peers_y, length, width), bf16)],
        (
            place, got, near, ahead, x_conv, b_conv, c_conv, rows, cols,
            final_valve_preactivation, clustered_rescale_factor[None],
        ),
        smem=1,
    )
    copies, gate_own, up_own, down_own = lax.optimization_barrier(
        (
            copies,
            specialist_gating_weights[0],
            specialist_raising_weights[0],
            specialist_lowering_weights[0],
        )
    )
    others = []
    for weight in (gate_own, up_own, down_own):
        others.append(swapped(weight))
    gate_other, up_other, down_other = others
    columns = lax.all_to_all(copies, "y", 0, 0, tiled=True)
    columns, gate_other, up_other, down_other = lax.optimization_barrier(
        (columns, gate_other, up_other, down_other)
    )
    gathered = lax.all_gather(columns, "c", axis=1, tiled=True)
    half = capacity // 2
    spread = (blocks, peers_y, 2, half, width)
    everyone = (*SP, *TP)
    stream, outgoing = call(
        stream_kernel,
        [((length, width), bf16), (spread, bf16)],
        (gathered, final_projection_weights, skip_stream_entering, rows),
    )
    arrived = lax.all_to_all(
        outgoing.reshape(-1, half, width), everyone, 0, 0, tiled=True
    ).reshape(blocks, 2 * peers_y, half, width)
    (partial_out,) = call(
        expert_kernel,
        [(arrived.shape, bf16)],
        (
            arrived, specialist_rescale_factor[None], gate_own, gate_other, up_own, up_other,
            down_own, down_other,
        ),
        flops=6 * slots * gate_own.shape[1] * D,
        scratch=[pltpu.VMEM((slots // 2, D), bf16)],
        room=24,
    )
    returned = lax.all_to_all(
        partial_out.reshape(-1, half, width), everyone, 0, 0, tiled=True
    ).reshape(spread)
    (out,) = call(final_kernel, [((length, width), bf16)], (returned, stream, cols))
    return out


def solution(mesh):
    sizes = dict(mesh.shape)
    torus = Mesh(mesh.devices.reshape(8, 4, sizes["tp"] // 2, 2), ("z", "x", "y", "c"))
    return jax.shard_map(
        body,
        mesh=torus,
        in_specs=(
            P(SP, TP),
            P(SP, TP),
            P(SP, TP),
            P(SP, TP),
            P(SP, TP),
            P(None, TP, SP),
            P(None, TP, SP),
            P(None, TP),
            P(None, TP),
            P(None, TP),
            P(None, TP),
            P(TP),
            P(None, TP),
            P(),
            P(SP, None),
            P(SP),
            P(SP, None),
            P(SP, None, TP),
            P(SP, None, TP),
            P(SP, TP, None),
        ),
        out_specs=P(SP, TP),
        check_vma=False,
    )
```

```python
import functools

import jax
import jax.numpy as jnp
from jax import lax
from jax.experimental import pallas as pl
from jax.experimental.pallas import tpu as pltpu
from jax.sharding import Mesh
from jax.sharding import PartitionSpec as P


D = 2048
HD = 64
NS = 128
CONV = 5
SP = ("z", "x")
ROW = ("yh", "p")
TP = (*ROW, "c")

HIGHEST = lax.Precision.HIGHEST
group_eps = 1e-05
stream_eps = 1e-06

VMEM = pl.BlockSpec(memory_space=pltpu.VMEM)
SMEM = pl.BlockSpec(memory_space=pltpu.SMEM)
HBM = pl.BlockSpec(memory_space=pltpu.HBM)
MIB = 1 << 20


def call(kernel, outs, args, flops=1000, scratch=(), room=8, smem=0, hbm=0):
    shapes = [jax.ShapeDtypeStruct(shape, dtype) for shape, dtype in outs]
    moved = sum(a.size * a.dtype.itemsize for a in args) + sum(
        o.size * o.dtype.itemsize for o in shapes
    )
    args = list(args)
    for n in range(smem, smem + hbm):
        args[n] = pltpu.with_memory_space_constraint(args[n], pltpu.HBM)
    return pl.pallas_call(
        kernel,
        out_shape=shapes,
        in_specs=[SMEM] * smem + [HBM] * hbm + [VMEM] * (len(args) - smem - hbm),
        out_specs=[VMEM] * len(shapes),
        scratch_shapes=list(scratch),
        compiler_params=pltpu.CompilerParams(vmem_limit_bytes=room * MIB),
        cost_estimate=pl.CostEstimate(flops=flops, bytes_accessed=moved, transcendentals=0),
    )(*args)


def exact_dot(a, b):
    return jnp.dot(a, b, precision=HIGHEST, preferred_element_type=jnp.float32)


def dot_rows(a, b, precision=None):
    return lax.dot_general(
        a,
        b,
        (((1,), (1,)), ((), ())),
        precision=precision,
        preferred_element_type=jnp.float32,
    )


def iota(shape, dim):
    return lax.broadcasted_iota(jnp.int32, shape, dim)


def fetch(pairs, done):
    copies = [pltpu.make_async_copy(a, b, done.at[n]) for n, (a, b) in enumerate(pairs)]
    for copy in copies:
        copy.start()
    for copy in copies:
        copy.wait()


def rim_kernel(place_ref, x_in, b_in, c_in, even_ref, odd_ref, x_ref, b_ref, c_ref, done):
    fetch(((x_in, x_ref), (b_in, b_ref), (c_in, c_ref)), done)
    even = place_ref[3] == 0
    length, width = x_ref.shape
    for n, ref in enumerate((x_ref, b_ref, c_ref)):
        lanes = slice(n * width, (n + 1) * width)
        top = ref[0:16, :].astype(jnp.float32)[0:2]
        tail = ref[length - 16 : length, :].astype(jnp.float32)[14:16]
        even_ref[:, lanes] = jnp.where(even, tail, top)
        odd_ref[:, lanes] = jnp.where(even, top, tail)


def table_kernel(
    capacity, step_in, fade_in, speed_in, named_in, like_in, score_in, kx_in, kb_in, kc_in,
    row_ref, col_ref, kx_ref, kb_ref, kc_ref,
    step_ref, fade_ref, speed_ref, named_ref, like_ref, score_ref, done,
):
    fetch(
        (
            (step_in, step_ref), (fade_in, fade_ref), (speed_in, speed_ref), (named_in, named_ref),
            (like_in, like_ref), (score_in, score_ref), (kx_in, kx_ref), (kb_in, kb_ref), (kc_in, kc_ref),
        ),
        done,
    )
    length = row_ref.shape[1]
    for d in range(2):
        raw = step_ref[d]
        step = jnp.maximum(raw, 0.0) + jnp.log1p(jnp.exp(-jnp.abs(raw)))
        row_ref[4 + 2 * d : 6 + 2 * d, :] = step
        for h in range(2):
            k = 2 * d + h
            row_ref[k : k + 1, :] = (
                -step[h : h + 1] * speed_ref[d : d + 1, h : h + 1] + fade_ref[d][h : h + 1]
            )
    whole = row_ref[0:8, :]
    lane, line = iota(whole.shape, 1), iota(whole.shape, 0)
    ahead = behind = whole
    reach = 1
    while reach < length:
        ahead = ahead + jnp.where(lane >= reach, pltpu.roll(ahead, reach, 1), 0.0)
        behind = behind + jnp.where(lane < length - reach, pltpu.roll(behind, length - reach, 1), 0.0)
        reach *= 2
    row_ref[0:8, :] = jnp.where(line < 2, ahead, jnp.where(line < 4, behind, whole))
    experts = 32
    expert = iota((experts, length), 0)
    hit = [named_ref[k : k + 1, :] == expert for k in range(2)]
    earlier = iota((length, length), 0) < iota((length, length), 1)
    ranking = jnp.dot(
        jnp.where(hit[0] | hit[1], 1.0, 0.0).astype(jnp.bfloat16),
        jnp.where(earlier, 1.0, 0.0).astype(jnp.bfloat16),
        preferred_element_type=jnp.float32,
    )
    place = ranking + expert.astype(jnp.float32) * capacity
    for k in range(2):
        row_ref[8 + k : 9 + k, :] = jnp.sum(jnp.where(hit[k], place, 0.0), axis=0, keepdims=True)
    first = jax.nn.sigmoid(score_ref[0:1, :] - score_ref[1:2, :])
    row_ref[10:11, :] = like_ref[...] * first
    row_ref[11:12, :] = like_ref[...] * (1.0 - first)
    row_ref[12:16, :] = jnp.zeros((4, length), jnp.float32)
    col_ref[...] = jnp.zeros_like(col_ref)
    col_ref[0:16, :] = row_ref[...]
    col_ref[...] = jnp.transpose(col_ref[...])


def conv_kernel(
    place_ref, x_ref, b_ref, c_ref, even_ref, odd_ref, kx_ref, kb_ref, kc_ref, col_ref,
    message_ref, xs_ref, bs_ref, cs_ref, padded,
):
    length, width = x_ref.shape
    even = place_ref[3] == 0
    before = jnp.where(even, odd_ref[...], even_ref[...])
    after = jnp.where(even, even_ref[...], odd_ref[...])
    parts = []
    for n, (ref, taps) in enumerate(((x_ref, kx_ref), (b_ref, kb_ref), (c_ref, kc_ref))):
        lanes = slice(n * width, (n + 1) * width)
        padded[8 : 8 + length, :] = ref[...].astype(jnp.float32)
        padded[6:8, :] = before[:, lanes]
        padded[8 + length : 10 + length, :] = after[:, lanes]
        total = jnp.zeros((length, width), jnp.float32)
        for k in range(CONV):
            total = total + taps[k : k + 1, :] * padded[6 + k : 6 + k + length, :]
        parts.append(jax.nn.silu(total).astype(jnp.bfloat16))
    xs_ref[...], bs_ref[...], cs_ref[...] = parts
    x_block = parts[0].astype(jnp.float32)
    b_block = parts[1].astype(jnp.float32)
    left = iota((length, width), 1) < HD
    logs = jnp.zeros((16, width), jnp.float32)
    line = iota((16, width), 0)
    for d, last in ((0, length - 1), (1, 0)):
        weight = []
        for h in range(2):
            k = 2 * d + h
            end = col_ref[last : last + 1, k : k + 1]
            weight.append(jnp.exp(end - col_ref[:, k : k + 1]) * col_ref[:, 4 + k : 5 + k])
            high = end.astype(jnp.bfloat16).astype(jnp.float32)
            logs = jnp.where(line == 4 * d + h, high, logs)
            logs = jnp.where(line == 4 * d + 2 + h, end - high, logs)
        scaled = x_block * jnp.where(left, weight[0], weight[1])
        state = exact_dot(jnp.transpose(scaled), b_block).astype(jnp.bfloat16)
        for peer in range(message_ref.shape[0]):
            message_ref[peer, d * width : (d + 1) * width, :] = state
    for peer in range(message_ref.shape[0]):
        message_ref[peer, 2 * width :, :] = logs.astype(jnp.bfloat16)


def within(xs_ref, bs_ref, cs_ref, row_ref, col_ref):
    length, width = xs_ref.shape
    scores = dot_rows(cs_ref[...], bs_ref[...])
    x_block = xs_ref[...].astype(jnp.float32)
    to, since = iota((length, length), 0), iota((length, length), 1)
    sides = []
    for h in range(2):
        both = jnp.zeros((length, length), jnp.float32)
        for d in range(2):
            k = 2 * d + h
            seen = since <= to if d == 0 else since >= to
            passed = col_ref[:, k : k + 1] - row_ref[k : k + 1, :]
            decay = jnp.where(seen, jnp.exp(jnp.minimum(passed, 0.0)), 0.0)
            both = both + decay * row_ref[4 + k : 5 + k, :]
        sides.append(exact_dot(scores * both, x_block))
    return jnp.where(iota((length, width), 1) < HD, sides[0], sides[1])


def log_pair(tile, d):
    return [tile[4 * d + h : 4 * d + h + 1, :] + tile[4 * d + 2 + h : 4 * d + 3 + h, :] for h in range(2)]


def by_head(pair, rows):
    return jnp.where(iota((rows, 128), 0) < HD, pair[0], pair[1])


def row_kernel(place_ref, seen_ref, message_ref, near_ref, ahead_ref):
    my_x, my_z = place_ref[0], place_ref[1]
    peers, rows = seen_ref.shape[0], near_ref.shape[1]
    line = iota((16, 128), 0)
    out = []
    ahead_ref[...] = jnp.zeros_like(ahead_ref)
    for d in range(2):
        total = near = jnp.zeros((rows, 128), jnp.float32)
        far = [jnp.zeros((1, 128), jnp.float32)] * 2
        ahead = list(far)
        for k in range(peers) if d == 0 else reversed(range(peers)):
            logs = log_pair(seen_ref[k, 2 * rows :, :].astype(jnp.float32), d)
            near = jnp.where(k == my_x, total, near)
            passed = k < my_x if d == 0 else k > my_x
            state = seen_ref[k, d * rows : (d + 1) * rows, :].astype(jnp.float32)
            total = total * jnp.exp(by_head(logs, rows)) + state
            for h in range(2):
                far[h] = far[h] + logs[h]
                ahead[h] = ahead[h] + jnp.where(passed, logs[h], 0.0)
        near_ref[d] = near
        tile = jnp.zeros((16, 128), jnp.float32)
        for h in range(2):
            ahead_ref[2 * d + h : 2 * d + h + 1, :] = ahead[h]
            high = far[h].astype(jnp.bfloat16).astype(jnp.float32)
            tile = jnp.where(line == h, high, tile)
            tile = jnp.where(line == 2 + h, far[h] - high, tile)
        out.append((total, tile))
    for k in range(message_ref.shape[0]):
        onward = k > my_z
        message_ref[k, :rows, :] = jnp.where(onward, out[0][0], out[1][0]).astype(jnp.bfloat16)
        message_ref[k, rows:, :] = jnp.where(onward, out[0][1], out[1][1]).astype(jnp.bfloat16)


def mixed_kernel(
    place_ref, got_ref, near_ref, ahead_ref, xs_ref, bs_ref, cs_ref, row_ref, col_ref, valve_ref, gain_ref,
    out_ref,
):
    my_z = place_ref[1]
    peers, rows = got_ref.shape[0], near_ref.shape[1]
    length = cs_ref.shape[0]
    c_block = cs_ref[...].astype(jnp.float32)
    left = iota((length, rows), 1) < HD
    mixer = within(xs_ref, bs_ref, cs_ref, row_ref, col_ref)
    for d in range(2):
        state = jnp.zeros((rows, 128), jnp.float32)
        for k in range(peers) if d == 0 else reversed(range(peers)):
            passed = k < my_z if d == 0 else k > my_z
            logs = log_pair(got_ref[k, rows:, :].astype(jnp.float32), 0)
            onto = state * jnp.exp(by_head(logs, rows)) + got_ref[k, :rows, :].astype(jnp.float32)
            state = jnp.where(passed, onto, state)
        ahead = [ahead_ref[2 * d + h : 2 * d + h + 1, :] for h in range(2)]
        state = state * jnp.exp(by_head(ahead, rows)) + near_ref[d]
        factor = jnp.exp(
            jnp.where(left, col_ref[:, 2 * d : 2 * d + 1], col_ref[:, 2 * d + 1 : 2 * d + 2])
        )
        mixer = mixer + dot_rows(c_block, state, HIGHEST) * factor
    gated = mixer * jax.nn.silu(valve_ref[...].astype(jnp.float32))
    gated = gated * lax.rsqrt(jnp.mean(gated * gated, axis=-1, keepdims=True) + group_eps)
    mixed = (gated * gain_ref[...]).astype(jnp.bfloat16)
    for k in range(out_ref.shape[0]):
        out_ref[k] = mixed


def stream_kernel(mixed_ref, weight_ref, skip_ref, row_ref, stream_ref, out_ref):
    length, width = skip_ref.shape
    places = mixed_ref.shape[0]
    total = skip_ref[...].astype(jnp.float32)
    product = jnp.zeros((length, width), jnp.float32)
    for y in range(places):
        both = jnp.concatenate([mixed_ref[y, :length, :], mixed_ref[y, length:, :]], axis=1)
        product = product + jnp.dot(
            both, weight_ref[2 * y * width : 2 * (y + 1) * width, :], preferred_element_type=jnp.float32
        )
    stream = (total + product).astype(jnp.bfloat16)
    stream_ref[...] = stream
    blocks, places, cores, half, _ = out_ref.shape
    slot = iota((blocks * cores * half, length), 0).astype(jnp.float32)
    chosen = (row_ref[8:9, :] == slot) | (row_ref[9:10, :] == slot)
    picked = jnp.dot(
        jnp.where(chosen, 1.0, 0.0).astype(jnp.bfloat16), stream, preferred_element_type=jnp.float32
    )
    picked = picked.reshape(blocks, cores, half, width).astype(jnp.bfloat16)
    for y in range(places):
        out_ref[:, y] = picked


def expert_kernel(
    place_ref, gate_in, up_in, down_in, own_ref, first_ref, second_ref, gain_ref, gate_own, up_own, down_own,
    hidden_ref, first_out, second_out, scaled, gate_other, up_other, down_other, done,
):
    copies = [
        pltpu.make_async_copy(a, b, done.at[n])
        for n, (a, b) in enumerate(((gate_in, gate_other), (up_in, up_other), (down_in, down_other)))
    ]
    for copy in copies:
        copy.start()
    parity = place_ref[4]
    blocks, features, half, lanes = own_ref.shape
    count = blocks * half
    squares = jnp.zeros((count, lanes), jnp.float32)
    for role, q in ((0, parity), (1, 1 - parity)):
        for j in range(features):
            if role == 0:
                part = own_ref[:, j].astype(jnp.float32).reshape(count, lanes)
            else:
                part = jnp.concatenate([first_ref[:, j], second_ref[:, j]], axis=0)
                part = part.astype(jnp.float32).reshape(count, lanes)
            squares = squares + part * part
            gain = gain_ref[j // 2, q][:, (j % 2) * lanes : (j % 2 + 1) * lanes]
            scaled[role, :, j * lanes : (j + 1) * lanes] = (part * gain).astype(jnp.bfloat16)
    scale = lax.rsqrt(jnp.sum(squares, axis=1, keepdims=True) / D + stream_eps)

    def product(weight_ref):
        total = jnp.zeros((count, weight_ref.shape[-1]), jnp.float32)
        for role, q in ((0, parity), (1, 1 - parity)):
            for y in range(features // 2):
                at = slice(2 * y * lanes, 2 * (y + 1) * lanes)
                total = total + jnp.dot(
                    scaled[role, :, at], weight_ref[y, q], preferred_element_type=jnp.float32
                )
        return total * scale

    for n, (gate_ref, up_ref) in enumerate(((gate_own, up_own), (gate_other, up_other))):
        if n == 1:
            copies[0].wait()
            copies[1].wait()
        hidden_ref[n] = (jax.nn.silu(product(gate_ref)) * product(up_ref)).astype(jnp.bfloat16)
    copies[2].wait()
    for y in range(features // 2):
        part = lowered(hidden_ref, down_own, down_other, y, 1 - parity).reshape(blocks, half, 2 * lanes)
        for n in range(2):
            tile = part[:, :, n * lanes : (n + 1) * lanes].astype(jnp.bfloat16)
            first_out[:, 2 * y + n] = tile[: blocks // 2]
            second_out[:, 2 * y + n] = tile[blocks // 2 :]


def lowered(hidden_ref, down_own, down_other, y, q):
    at = pl.ds(pl.multiple_of((4 * y + 2 * q) * 128, 256), 256)
    return jnp.dot(hidden_ref[0], down_own[:, at], preferred_element_type=jnp.float32) + jnp.dot(
        hidden_ref[1], down_other[:, at], preferred_element_type=jnp.float32
    )


def own_columns_kernel(place_ref, hidden_ref, down_own, down_other, out_ref):
    parity = place_ref[4]
    blocks, features, half, lanes = out_ref.shape
    for y in range(features // 2):
        part = lowered(hidden_ref, down_own, down_other, y, parity).reshape(blocks, half, 2 * lanes)
        for n in range(2):
            out_ref[:, 2 * y + n] = part[:, :, n * lanes : (n + 1) * lanes].astype(jnp.bfloat16)


def final_kernel(returned_ref, stream_ref, col_ref, out_ref):
    length, width = stream_ref.shape
    blocks, places, cores, half, _ = returned_ref.shape
    slots = blocks * cores * half
    slot = iota((length, slots), 1).astype(jnp.float32)
    answer = returned_ref[:, 0].astype(jnp.float32)
    for y in range(1, places):
        answer = answer + returned_ref[:, y].astype(jnp.float32)
    returned = answer.reshape(slots, width).astype(jnp.bfloat16)
    total = stream_ref[...].astype(jnp.float32)
    for k in range(2):
        chosen = jnp.where(col_ref[:, 8 + k : 9 + k] == slot, 1.0, 0.0).astype(jnp.bfloat16)
        picked = jnp.dot(chosen, returned, preferred_element_type=jnp.float32)
        total = total + col_ref[:, 10 + k : 11 + k] * picked
    out_ref[...] = total.astype(jnp.bfloat16)


def swapped(value):
    return lax.ppermute(value, "c", [(0, 1), (1, 0)])


def from_both_sides(first, second):
    count = lax.axis_size(ROW)
    return (
        lax.ppermute(first, ROW, [((i + 1) % count, i) for i in range(count)]),
        lax.ppermute(second, ROW, [(i, (i + 1) % count) for i in range(count)]),
    )


def body(
    skip_stream_entering,
    unfiltered_channel_feed,
    unfiltered_state_entry,
    unfiltered_state_exit,
    final_valve_preactivation,
    increment_preactivation,
    summed_attenuation_both_ways,
    channel_fading_speed,
    channel_feed_filter,
    state_entry_filter,
    state_exit_filter,
    clustered_rescale_factor,
    final_projection_weights,
    specialist_rescale_factor,
    item_specialist_couple,
    selected_cluster_likelihood,
    selected_twin_scores_raw,
    specialist_gating_weights,
    specialist_raising_weights,
    specialist_lowering_weights,
):
    f32, bf16 = jnp.float32, jnp.bfloat16
    length, width = unfiltered_channel_feed.shape
    blocks = lax.axis_size(SP)
    peers_x, peers_y, peers_z = (lax.axis_size(a) for a in ("x", ROW, "z"))
    capacity = 4 * length // blocks
    slots = blocks * capacity
    axes = [lax.axis_index(a) for a in ("x", "z", "c")]
    place = jnp.stack([*axes, axes[0] % 2, lax.axis_index("p")]).astype(jnp.int32)

    rim = CONV // 2
    even_rim, odd_rim, *feeds = call(
        rim_kernel,
        [((rim, 3 * width), f32)] * 2 + [((length, width), bf16)] * 3,
        (place, unfiltered_channel_feed, unfiltered_state_entry, unfiltered_state_exit),
        flops=100_000,
        scratch=[pltpu.SemaphoreType.DMA((3,))],
        smem=1,
        hbm=3,
    )
    pairs = [(i, i + 1) for i in range(blocks - 1)]
    even_rim = lax.ppermute(even_rim, SP, [p for a, b in pairs[0::2] for p in ((a, b), (b, a))])
    odd_rim = lax.ppermute(odd_rim, SP, [p for a, b in pairs[1::2] for p in ((a, b), (b, a))])
    filters = (channel_feed_filter, state_entry_filter, state_exit_filter)
    heads = increment_preactivation.shape[1]
    rows, cols, *filters = call(
        functools.partial(table_kernel, capacity),
        [((16, length), f32), ((length, length), f32)] + [((CONV, width), f32)] * 3,
        (
            increment_preactivation,
            summed_attenuation_both_ways,
            channel_fading_speed,
            item_specialist_couple.T,
            selected_cluster_likelihood[None],
            selected_twin_scores_raw.T,
            *filters,
        ),
        flops=4_000_000,
        scratch=[
            pltpu.VMEM((2, heads, length), f32),
            pltpu.VMEM((2, heads, length), f32),
            pltpu.VMEM((2, heads), f32),
            pltpu.VMEM((2, length), jnp.int32),
            pltpu.VMEM((1, length), f32),
            pltpu.VMEM((2, length), f32),
            pltpu.SemaphoreType.DMA((9,)),
        ],
        hbm=9,
    )
    message, x_conv, b_conv, c_conv = call(
        conv_kernel,
        [((peers_x, 2 * width + 16, NS), bf16)] + [((length, width), bf16)] * 3,
        (place, *feeds, even_rim, odd_rim, *filters, cols),
        flops=4_000_000,
        scratch=[pltpu.VMEM((length + 16, width), f32)],
        smem=1,
    )
    seen = lax.all_to_all(message, "x", 0, 0, tiled=True)
    onward, near, ahead = call(
        row_kernel,
        [((peers_z, width + 16, NS), bf16), ((2, width, NS), f32), ((8, NS), f32)],
        (place, seen),
        smem=1,
    )
    got = lax.all_to_all(onward, "z", 0, 0, tiled=True)
    (copies,) = call(
        mixed_kernel,
        [((peers_y, length, width), bf16)],
        (
            place, got, near, ahead, x_conv, b_conv, c_conv, rows, cols,
            final_valve_preactivation, clustered_rescale_factor[None],
        ),
        smem=1,
    )
    copies, gate_own, up_own, down_own = lax.optimization_barrier(
        (
            copies,
            specialist_gating_weights[0],
            specialist_raising_weights[0],
            specialist_lowering_weights[0],
        )
    )
    others = []
    for weight in (gate_own, up_own, down_own):
        others.append(swapped(weight))
    gate_other, up_other, down_other = others
    columns = lax.all_to_all(copies, ROW, 0, 0, tiled=True)
    columns, gate_other, up_other, down_other = lax.optimization_barrier(
        (columns, gate_other, up_other, down_other)
    )
    gathered = lax.all_gather(columns, "c", axis=1, tiled=True)
    half = capacity // 2
    sides = peers_y // 2
    spread = (blocks, sides, 2, half, width)
    members = (*SP, "yh", "c")
    stream, outgoing = call(
        stream_kernel,
        [((length, width), bf16), (spread, bf16)],
        (gathered, final_projection_weights, skip_stream_entering, rows),
    )
    arrived = lax.all_to_all(
        outgoing.reshape(-1, half, width), members, 0, 0, tiled=True
    ).reshape(blocks, 2 * sides, half, width)
    first, second = from_both_sides(arrived[: blocks // 2], arrived[blocks // 2 :])
    units = gate_own.shape[1]
    wide = (sides, 2, 2 * width, units)
    hidden, first_sent, second_sent = call(
        expert_kernel,
        [((2, slots // 2, units), bf16), (first.shape, bf16), (second.shape, bf16)],
        (
            place, gate_other.reshape(wide), up_other.reshape(wide), down_other,
            arrived, first, second, specialist_rescale_factor.reshape(sides, 2, 1, 2 * width),
            gate_own.reshape(wide), up_own.reshape(wide), down_own,
        ),
        flops=5 * slots * units * D,
        scratch=[
            pltpu.VMEM((2, slots // 2, D // 2), bf16),
            pltpu.VMEM(wide, bf16),
            pltpu.VMEM(wide, bf16),
            pltpu.VMEM(down_own.shape, bf16),
            pltpu.SemaphoreType.DMA((3,)),
        ],
        smem=1,
        hbm=3,
        room=24,
    )
    first_partner, second_partner = from_both_sides(first_sent, second_sent)
    (kept,) = call(
        own_columns_kernel,
        [(arrived.shape, bf16)],
        (place, hidden, down_own, down_other),
        flops=slots * units * D,
        smem=1,
        room=12,
    )
    partner = jnp.concatenate([first_partner, second_partner], axis=0)
    partial_out = (kept.astype(f32) + partner.astype(f32)).astype(bf16)
    returned = lax.all_to_all(
        partial_out.reshape(-1, half, width), members, 0, 0, tiled=True
    ).reshape(spread)
    (out,) = call(final_kernel, [((length, width), bf16)], (returned, stream, cols))
    return out


def solution(mesh):
    sizes = dict(mesh.shape)
    torus = Mesh(
        mesh.devices.reshape(8, 4, sizes["tp"] // 4, 2, 2), ("z", "x", "yh", "p", "c")
    )
    return jax.shard_map(
        body,
        mesh=torus,
        in_specs=(
            P(SP, TP),
            P(SP, TP),
            P(SP, TP),
            P(SP, TP),
            P(SP, TP),
            P(None, TP, SP),
            P(None, TP, SP),
            P(None, TP),
            P(None, TP),
            P(None, TP),
            P(None, TP),
            P(TP),
            P(None, TP),
            P(),
            P(SP, None),
            P(SP),
            P(SP, None),
            P(SP, None, TP),
            P(SP, None, TP),
            P(SP, TP, None),
        ),
        out_specs=P(SP, TP),
        check_vma=False,
    )
```

```python
import functools

import jax
import jax.numpy as jnp
from jax import lax
from jax.experimental import pallas as pl
from jax.experimental.pallas import tpu as pltpu
from jax.sharding import Mesh
from jax.sharding import PartitionSpec as P


D = 2048
HD = 64
NS = 128
CONV = 5
SP = ("z", "x")
TP = ("y", "c")

HIGHEST = lax.Precision.HIGHEST
group_eps = 1e-05
stream_eps = 1e-06

VMEM = pl.BlockSpec(memory_space=pltpu.VMEM)
SMEM = pl.BlockSpec(memory_space=pltpu.SMEM)
HBM = pl.BlockSpec(memory_space=pltpu.HBM)
MIB = 1 << 20


def call(kernel, outs, args, flops=1000, scratch=(), room=8, smem=0, hbm=0):
    shapes = [jax.ShapeDtypeStruct(shape, dtype) for shape, dtype in outs]
    moved = sum(a.size * a.dtype.itemsize for a in args) + sum(
        o.size * o.dtype.itemsize for o in shapes
    )
    args = list(args)
    for n in range(smem, smem + hbm):
        args[n] = pltpu.with_memory_space_constraint(args[n], pltpu.HBM)
    return pl.pallas_call(
        kernel,
        out_shape=shapes,
        in_specs=[SMEM] * smem + [HBM] * hbm + [VMEM] * (len(args) - smem - hbm),
        out_specs=[VMEM] * len(shapes),
        scratch_shapes=list(scratch),
        compiler_params=pltpu.CompilerParams(vmem_limit_bytes=room * MIB),
        cost_estimate=pl.CostEstimate(flops=flops, bytes_accessed=moved, transcendentals=0),
    )(*args)


def exact_dot(a, b):
    return jnp.dot(a, b, precision=HIGHEST, preferred_element_type=jnp.float32)


def dot_rows(a, b, precision=None):
    return lax.dot_general(
        a,
        b,
        (((1,), (1,)), ((), ())),
        precision=precision,
        preferred_element_type=jnp.float32,
    )


def iota(shape, dim):
    return lax.broadcasted_iota(jnp.int32, shape, dim)


def fetch(pairs, done):
    copies = [pltpu.make_async_copy(a, b, done.at[n]) for n, (a, b) in enumerate(pairs)]
    for copy in copies:
        copy.start()
    for copy in copies:
        copy.wait()


def rim_kernel(place_ref, x_in, b_in, c_in, even_ref, odd_ref, x_ref, b_ref, c_ref, done):
    fetch(((x_in, x_ref), (b_in, b_ref), (c_in, c_ref)), done)
    even = place_ref[3] == 0
    length, width = x_ref.shape
    for n, ref in enumerate((x_ref, b_ref, c_ref)):
        lanes = slice(n * width, (n + 1) * width)
        top = ref[0:16, :].astype(jnp.float32)[0:2]
        tail = ref[length - 16 : length, :].astype(jnp.float32)[14:16]
        even_ref[:, lanes] = jnp.where(even, tail, top)
        odd_ref[:, lanes] = jnp.where(even, top, tail)


def table_kernel(
    capacity, step_in, fade_in, speed_in, named_in, like_in, score_in, kx_in, kb_in, kc_in,
    row_ref, col_ref, kx_ref, kb_ref, kc_ref,
    step_ref, fade_ref, speed_ref, named_ref, like_ref, score_ref, done,
):
    fetch(
        (
            (step_in, step_ref), (fade_in, fade_ref), (speed_in, speed_ref), (named_in, named_ref),
            (like_in, like_ref), (score_in, score_ref), (kx_in, kx_ref), (kb_in, kb_ref), (kc_in, kc_ref),
        ),
        done,
    )
    length = row_ref.shape[1]
    for d in range(2):
        raw = step_ref[d]
        step = jnp.maximum(raw, 0.0) + jnp.log1p(jnp.exp(-jnp.abs(raw)))
        row_ref[4 + 2 * d : 6 + 2 * d, :] = step
        for h in range(2):
            k = 2 * d + h
            row_ref[k : k + 1, :] = (
                -step[h : h + 1] * speed_ref[d : d + 1, h : h + 1] + fade_ref[d][h : h + 1]
            )
    whole = row_ref[0:8, :]
    lane, line = iota(whole.shape, 1), iota(whole.shape, 0)
    ahead = behind = whole
    reach = 1
    while reach < length:
        ahead = ahead + jnp.where(lane >= reach, pltpu.roll(ahead, reach, 1), 0.0)
        behind = behind + jnp.where(lane < length - reach, pltpu.roll(behind, length - reach, 1), 0.0)
        reach *= 2
    row_ref[0:8, :] = jnp.where(line < 2, ahead, jnp.where(line < 4, behind, whole))
    experts = 32
    expert = iota((experts, length), 0)
    hit = [named_ref[k : k + 1, :] == expert for k in range(2)]
    earlier = iota((length, length), 0) < iota((length, length), 1)
    ranking = jnp.dot(
        jnp.where(hit[0] | hit[1], 1.0, 0.0).astype(jnp.bfloat16),
        jnp.where(earlier, 1.0, 0.0).astype(jnp.bfloat16),
        preferred_element_type=jnp.float32,
    )
    place = ranking + expert.astype(jnp.float32) * capacity
    for k in range(2):
        row_ref[8 + k : 9 + k, :] = jnp.sum(jnp.where(hit[k], place, 0.0), axis=0, keepdims=True)
    first = jax.nn.sigmoid(score_ref[0:1, :] - score_ref[1:2, :])
    row_ref[10:11, :] = like_ref[...] * first
    row_ref[11:12, :] = like_ref[...] * (1.0 - first)
    row_ref[12:16, :] = jnp.zeros((4, length), jnp.float32)
    col_ref[...] = jnp.zeros_like(col_ref)
    col_ref[0:16, :] = row_ref[...]
    col_ref[...] = jnp.transpose(col_ref[...])


def conv_kernel(
    place_ref, x_ref, b_ref, c_ref, even_ref, odd_ref, kx_ref, kb_ref, kc_ref, col_ref,
    message_ref, xs_ref, bs_ref, cs_ref, padded,
):
    length, width = x_ref.shape
    even = place_ref[3] == 0
    before = jnp.where(even, odd_ref[...], even_ref[...])
    after = jnp.where(even, even_ref[...], odd_ref[...])
    parts = []
    for n, (ref, taps) in enumerate(((x_ref, kx_ref), (b_ref, kb_ref), (c_ref, kc_ref))):
        lanes = slice(n * width, (n + 1) * width)
        padded[8 : 8 + length, :] = ref[...].astype(jnp.float32)
        padded[6:8, :] = before[:, lanes]
        padded[8 + length : 10 + length, :] = after[:, lanes]
        total = jnp.zeros((length, width), jnp.float32)
        for k in range(CONV):
            total = total + taps[k : k + 1, :] * padded[6 + k : 6 + k + length, :]
        parts.append(jax.nn.silu(total).astype(jnp.bfloat16))
    xs_ref[...], bs_ref[...], cs_ref[...] = parts
    x_block = parts[0].astype(jnp.float32)
    b_block = parts[1].astype(jnp.float32)
    left = iota((length, width), 1) < HD
    logs = jnp.zeros((16, width), jnp.float32)
    line = iota((16, width), 0)
    for d, last in ((0, length - 1), (1, 0)):
        weight = []
        for h in range(2):
            k = 2 * d + h
            end = col_ref[last : last + 1, k : k + 1]
            weight.append(jnp.exp(end - col_ref[:, k : k + 1]) * col_ref[:, 4 + k : 5 + k])
            high = end.astype(jnp.bfloat16).astype(jnp.float32)
            logs = jnp.where(line == 4 * d + h, high, logs)
            logs = jnp.where(line == 4 * d + 2 + h, end - high, logs)
        scaled = x_block * jnp.where(left, weight[0], weight[1])
        state = exact_dot(jnp.transpose(scaled), b_block).astype(jnp.bfloat16)
        for peer in range(message_ref.shape[0]):
            message_ref[peer, d * width : (d + 1) * width, :] = state
    for peer in range(message_ref.shape[0]):
        message_ref[peer, 2 * width :, :] = logs.astype(jnp.bfloat16)


def within(xs_ref, bs_ref, cs_ref, row_ref, col_ref):
    length, width = xs_ref.shape
    scores = dot_rows(cs_ref[...], bs_ref[...])
    x_block = xs_ref[...].astype(jnp.float32)
    to, since = iota((length, length), 0), iota((length, length), 1)
    sides = []
    for h in range(2):
        both = jnp.zeros((length, length), jnp.float32)
        for d in range(2):
            k = 2 * d + h
            seen = since <= to if d == 0 else since >= to
            passed = col_ref[:, k : k + 1] - row_ref[k : k + 1, :]
            decay = jnp.where(seen, jnp.exp(jnp.minimum(passed, 0.0)), 0.0)
            both = both + decay * row_ref[4 + k : 5 + k, :]
        sides.append(exact_dot(scores * both, x_block))
    return jnp.where(iota((length, width), 1) < HD, sides[0], sides[1])


def log_pair(tile, d):
    return [tile[4 * d + h : 4 * d + h + 1, :] + tile[4 * d + 2 + h : 4 * d + 3 + h, :] for h in range(2)]


def by_head(pair, rows):
    return jnp.where(iota((rows, 128), 0) < HD, pair[0], pair[1])


def row_kernel(place_ref, seen_ref, message_ref, near_ref, ahead_ref):
    my_x, my_z = place_ref[0], place_ref[1]
    peers, rows = seen_ref.shape[0], near_ref.shape[1]
    line = iota((16, 128), 0)
    out = []
    ahead_ref[...] = jnp.zeros_like(ahead_ref)
    for d in range(2):
        total = near = jnp.zeros((rows, 128), jnp.float32)
        far = [jnp.zeros((1, 128), jnp.float32)] * 2
        ahead = list(far)
        for k in range(peers) if d == 0 else reversed(range(peers)):
            logs = log_pair(seen_ref[k, 2 * rows :, :].astype(jnp.float32), d)
            near = jnp.where(k == my_x, total, near)
            passed = k < my_x if d == 0 else k > my_x
            state = seen_ref[k, d * rows : (d + 1) * rows, :].astype(jnp.float32)
            total = total * jnp.exp(by_head(logs, rows)) + state
            for h in range(2):
                far[h] = far[h] + logs[h]
                ahead[h] = ahead[h] + jnp.where(passed, logs[h], 0.0)
        near_ref[d] = near
        tile = jnp.zeros((16, 128), jnp.float32)
        for h in range(2):
            ahead_ref[2 * d + h : 2 * d + h + 1, :] = ahead[h]
            high = far[h].astype(jnp.bfloat16).astype(jnp.float32)
            tile = jnp.where(line == h, high, tile)
            tile = jnp.where(line == 2 + h, far[h] - high, tile)
        out.append((total, tile))
    for k in range(message_ref.shape[0]):
        onward = k > my_z
        message_ref[k, :rows, :] = jnp.where(onward, out[0][0], out[1][0]).astype(jnp.bfloat16)
        message_ref[k, rows:, :] = jnp.where(onward, out[0][1], out[1][1]).astype(jnp.bfloat16)


def mixed_kernel(
    place_ref, got_ref, near_ref, ahead_ref, xs_ref, bs_ref, cs_ref, row_ref, col_ref, valve_ref, gain_ref,
    out_ref,
):
    my_z = place_ref[1]
    peers, rows = got_ref.shape[0], near_ref.shape[1]
    length = cs_ref.shape[0]
    c_block = cs_ref[...].astype(jnp.float32)
    left = iota((length, rows), 1) < HD
    mixer = within(xs_ref, bs_ref, cs_ref, row_ref, col_ref)
    for d in range(2):
        state = jnp.zeros((rows, 128), jnp.float32)
        for k in range(peers) if d == 0 else reversed(range(peers)):
            passed = k < my_z if d == 0 else k > my_z
            logs = log_pair(got_ref[k, rows:, :].astype(jnp.float32), 0)
            onto = state * jnp.exp(by_head(logs, rows)) + got_ref[k, :rows, :].astype(jnp.float32)
            state = jnp.where(passed, onto, state)
        ahead = [ahead_ref[2 * d + h : 2 * d + h + 1, :] for h in range(2)]
        state = state * jnp.exp(by_head(ahead, rows)) + near_ref[d]
        factor = jnp.exp(
            jnp.where(left, col_ref[:, 2 * d : 2 * d + 1], col_ref[:, 2 * d + 1 : 2 * d + 2])
        )
        mixer = mixer + dot_rows(c_block, state, HIGHEST) * factor
    gated = mixer * jax.nn.silu(valve_ref[...].astype(jnp.float32))
    gated = gated * lax.rsqrt(jnp.mean(gated * gated, axis=-1, keepdims=True) + group_eps)
    mixed = (gated * gain_ref[...]).astype(jnp.bfloat16)
    for k in range(out_ref.shape[0]):
        out_ref[k] = mixed


def stream_kernel(mixed_ref, weight_ref, skip_ref, row_ref, stream_ref, out_ref):
    length, width = skip_ref.shape
    places = mixed_ref.shape[0]
    total = skip_ref[...].astype(jnp.float32)
    product = jnp.zeros((length, width), jnp.float32)
    for y in range(places):
        both = jnp.concatenate([mixed_ref[y, :length, :], mixed_ref[y, length:, :]], axis=1)
        product = product + jnp.dot(
            both, weight_ref[2 * y * width : 2 * (y + 1) * width, :], preferred_element_type=jnp.float32
        )
    stream = (total + product).astype(jnp.bfloat16)
    stream_ref[...] = stream
    blocks, places, cores, half, _ = out_ref.shape
    slot = iota((blocks * cores * half, length), 0).astype(jnp.float32)
    chosen = (row_ref[8:9, :] == slot) | (row_ref[9:10, :] == slot)
    picked = jnp.dot(
        jnp.where(chosen, 1.0, 0.0).astype(jnp.bfloat16), stream, preferred_element_type=jnp.float32
    )
    picked = picked.reshape(blocks, cores, half, width).astype(jnp.bfloat16)
    for y in range(places):
        out_ref[:, y] = picked


def expert_kernel(
    gate_in, up_in, down_in, rows_ref, gain_ref, gate_own, up_own, down_own, out_ref,
    scaled, gate_other, up_other, down_other, done,
):
    copies = [
        pltpu.make_async_copy(a, b, done.at[n])
        for n, (a, b) in enumerate(((gate_in, gate_other), (up_in, up_other), (down_in, down_other)))
    ]
    for copy in copies:
        copy.start()
    blocks, features, half, lanes = rows_ref.shape
    count = blocks * half
    squares = jnp.zeros((count, lanes), jnp.float32)
    for k in range(features):
        part = rows_ref[:, k].astype(jnp.float32).reshape(count, lanes)
        squares = squares + part * part
        at = slice(k * lanes, (k + 1) * lanes)
        scaled[:, at] = (part * gain_ref[:, at]).astype(jnp.bfloat16)
    scale = lax.rsqrt(jnp.sum(squares, axis=1, keepdims=True) / D + stream_eps)
    whole = scaled[...]
    hidden = []
    for n, (gate_ref, up_ref) in enumerate(((gate_own, up_own), (gate_other, up_other))):
        if n == 1:
            copies[0].wait()
            copies[1].wait()
        gate = jnp.dot(whole, gate_ref[...], preferred_element_type=jnp.float32) * scale
        upward = jnp.dot(whole, up_ref[...], preferred_element_type=jnp.float32) * scale
        hidden.append((jax.nn.silu(gate) * upward).astype(jnp.bfloat16))
    copies[2].wait()
    step = 2 * lanes
    for j in range(features // 2):
        at = slice(j * step, (j + 1) * step)
        part = jnp.dot(hidden[0], down_own[:, at], preferred_element_type=jnp.float32)
        part = part + jnp.dot(hidden[1], down_other[:, at], preferred_element_type=jnp.float32)
        for n in range(2):
            tile = part[:, n * lanes : (n + 1) * lanes].reshape(blocks, half, lanes)
            out_ref[:, 2 * j + n] = tile.astype(jnp.bfloat16)


def final_kernel(returned_ref, stream_ref, col_ref, out_ref):
    length, width = stream_ref.shape
    blocks, places, cores, half, _ = returned_ref.shape
    slots = blocks * cores * half
    slot = iota((length, slots), 1).astype(jnp.float32)
    answer = returned_ref[:, 0].astype(jnp.float32)
    for y in range(1, places):
        answer = answer + returned_ref[:, y].astype(jnp.float32)
    returned = answer.reshape(slots, width).astype(jnp.bfloat16)
    total = stream_ref[...].astype(jnp.float32)
    for k in range(2):
        chosen = jnp.where(col_ref[:, 8 + k : 9 + k] == slot, 1.0, 0.0).astype(jnp.bfloat16)
        picked = jnp.dot(chosen, returned, preferred_element_type=jnp.float32)
        total = total + col_ref[:, 10 + k : 11 + k] * picked
    out_ref[...] = total.astype(jnp.bfloat16)


def swapped(value):
    return lax.ppermute(value, "c", [(0, 1), (1, 0)])


def body(
    skip_stream_entering,
    unfiltered_channel_feed,
    unfiltered_state_entry,
    unfiltered_state_exit,
    final_valve_preactivation,
    increment_preactivation,
    summed_attenuation_both_ways,
    channel_fading_speed,
    channel_feed_filter,
    state_entry_filter,
    state_exit_filter,
    clustered_rescale_factor,
    final_projection_weights,
    specialist_rescale_factor,
    item_specialist_couple,
    selected_cluster_likelihood,
    selected_twin_scores_raw,
    specialist_gating_weights,
    specialist_raising_weights,
    specialist_lowering_weights,
):
    f32, bf16 = jnp.float32, jnp.bfloat16
    length, width = unfiltered_channel_feed.shape
    blocks = lax.axis_size(SP)
    peers_x, peers_y, peers_z = (lax.axis_size(a) for a in ("x", "y", "z"))
    capacity = 4 * length // blocks
    slots = blocks * capacity
    axes = [lax.axis_index(a) for a in ("x", "z", "c")]
    place = jnp.stack([*axes, axes[0] % 2]).astype(jnp.int32)

    rim = CONV // 2
    even_rim, odd_rim, *feeds = call(
        rim_kernel,
        [((rim, 3 * width), f32)] * 2 + [((length, width), bf16)] * 3,
        (place, unfiltered_channel_feed, unfiltered_state_entry, unfiltered_state_exit),
        flops=100_000,
        scratch=[pltpu.SemaphoreType.DMA((3,))],
        smem=1,
        hbm=3,
    )
    pairs = [(i, i + 1) for i in range(blocks - 1)]
    even_rim = lax.ppermute(even_rim, SP, [p for a, b in pairs[0::2] for p in ((a, b), (b, a))])
    odd_rim = lax.ppermute(odd_rim, SP, [p for a, b in pairs[1::2] for p in ((a, b), (b, a))])
    filters = (channel_feed_filter, state_entry_filter, state_exit_filter)
    heads = increment_preactivation.shape[1]
    rows, cols, *filters = call(
        functools.partial(table_kernel, capacity),
        [((16, length), f32), ((length, length), f32)] + [((CONV, width), f32)] * 3,
        (
            increment_preactivation,
            summed_attenuation_both_ways,
            channel_fading_speed,
            item_specialist_couple.T,
            selected_cluster_likelihood[None],
            selected_twin_scores_raw.T,
            *filters,
        ),
        flops=4_000_000,
        scratch=[
            pltpu.VMEM((2, heads, length), f32),
            pltpu.VMEM((2, heads, length), f32),
            pltpu.VMEM((2, heads), f32),
            pltpu.VMEM((2, length), jnp.int32),
            pltpu.VMEM((1, length), f32),
            pltpu.VMEM((2, length), f32),
            pltpu.SemaphoreType.DMA((9,)),
        ],
        hbm=9,
    )
    message, x_conv, b_conv, c_conv = call(
        conv_kernel,
        [((peers_x, 2 * width + 16, NS), bf16)] + [((length, width), bf16)] * 3,
        (place, *feeds, even_rim, odd_rim, *filters, cols),
        flops=4_000_000,
        scratch=[pltpu.VMEM((length + 16, width), f32)],
        smem=1,
    )
    seen = lax.all_to_all(message, "x", 0, 0, tiled=True)
    onward, near, ahead = call(
        row_kernel,
        [((peers_z, width + 16, NS), bf16), ((2, width, NS), f32), ((8, NS), f32)],
        (place, seen),
        smem=1,
    )
    got = lax.all_to_all(onward, "z", 0, 0, tiled=True)
    (copies,) = call(
        mixed_kernel,
        [((peers_y, length, width), bf16)],
        (
            place, got, near, ahead, x_conv, b_conv, c_conv, rows, cols,
            final_valve_preactivation, clustered_rescale_factor[None],
        ),
        smem=1,
    )
    copies, gate_own, up_own, down_own = lax.optimization_barrier(
        (
            copies,
            specialist_gating_weights[0],
            specialist_raising_weights[0],
            specialist_lowering_weights[0],
        )
    )
    others = []
    for weight in (gate_own, up_own, down_own):
        others.append(swapped(weight))
    gate_other, up_other, down_other = others
    columns = lax.all_to_all(copies, "y", 0, 0, tiled=True)
    columns, gate_other, up_other, down_other = lax.optimization_barrier(
        (columns, gate_other, up_other, down_other)
    )
    gathered = lax.all_gather(columns, "c", axis=1, tiled=True)
    half = capacity // 2
    spread = (blocks, peers_y, 2, half, width)
    everyone = (*SP, *TP)
    stream, outgoing = call(
        stream_kernel,
        [((length, width), bf16), (spread, bf16)],
        (gathered, final_projection_weights, skip_stream_entering, rows),
    )
    arrived = lax.all_to_all(
        outgoing.reshape(-1, half, width), everyone, 0, 0, tiled=True
    ).reshape(blocks, 2 * peers_y, half, width)
    (partial_out,) = call(
        expert_kernel,
        [(arrived.shape, bf16)],
        (
            gate_other, up_other, down_other, arrived, specialist_rescale_factor[None],
            gate_own, up_own, down_own,
        ),
        flops=6 * slots * gate_own.shape[1] * D,
        scratch=[
            pltpu.VMEM((slots // 2, D), bf16),
            pltpu.VMEM(gate_own.shape, bf16),
            pltpu.VMEM(up_own.shape, bf16),
            pltpu.VMEM(down_own.shape, bf16),
            pltpu.SemaphoreType.DMA((3,)),
        ],
        hbm=3,
        room=24,
    )
    returned = lax.all_to_all(
        partial_out.reshape(-1, half, width), everyone, 0, 0, tiled=True
    ).reshape(spread)
    (out,) = call(final_kernel, [((length, width), bf16)], (returned, stream, cols))
    return out


def solution(mesh):
    sizes = dict(mesh.shape)
    torus = Mesh(mesh.devices.reshape(8, 4, sizes["tp"] // 2, 2), ("z", "x", "y", "c"))
    return jax.shard_map(
        body,
        mesh=torus,
        in_specs=(
            P(SP, TP),
            P(SP, TP),
            P(SP, TP),
            P(SP, TP),
            P(SP, TP),
            P(None, TP, SP),
            P(None, TP, SP),
            P(None, TP),
            P(None, TP),
            P(None, TP),
            P(None, TP),
            P(TP),
            P(None, TP),
            P(),
            P(SP, None),
            P(SP),
            P(SP, None),
            P(SP, None, TP),
            P(SP, None, TP),
            P(SP, TP, None),
        ),
        out_specs=P(SP, TP),
        check_vma=False,
    )
```

```python
import functools

import jax
import jax.numpy as jnp
from jax import lax
from jax.experimental import pallas as pl
from jax.experimental.pallas import tpu as pltpu
from jax.sharding import Mesh
from jax.sharding import PartitionSpec as P


D = 2048
HD = 64
NS = 128
CONV = 5
SP = ("z", "x")
TP = ("y", "c")

HIGHEST = lax.Precision.HIGHEST
group_eps = 1e-05
stream_eps = 1e-06

VMEM = pl.BlockSpec(memory_space=pltpu.VMEM)
SMEM = pl.BlockSpec(memory_space=pltpu.SMEM)
HBM = pl.BlockSpec(memory_space=pltpu.HBM)
MIB = 1 << 20


def call(kernel, outs, args, flops=1000, scratch=(), room=8, smem=0, hbm=0):
    shapes = [jax.ShapeDtypeStruct(shape, dtype) for shape, dtype in outs]
    moved = sum(a.size * a.dtype.itemsize for a in args) + sum(
        o.size * o.dtype.itemsize for o in shapes
    )
    args = list(args)
    for n in range(smem, smem + hbm):
        args[n] = pltpu.with_memory_space_constraint(args[n], pltpu.HBM)
    return pl.pallas_call(
        kernel,
        out_shape=shapes,
        in_specs=[SMEM] * smem + [HBM] * hbm + [VMEM] * (len(args) - smem - hbm),
        out_specs=[VMEM] * len(shapes),
        scratch_shapes=list(scratch),
        compiler_params=pltpu.CompilerParams(vmem_limit_bytes=room * MIB),
        cost_estimate=pl.CostEstimate(flops=flops, bytes_accessed=moved, transcendentals=0),
    )(*args)


def exact_dot(a, b):
    return jnp.dot(a, b, precision=HIGHEST, preferred_element_type=jnp.float32)


def dot_rows(a, b, precision=None):
    return lax.dot_general(
        a,
        b,
        (((1,), (1,)), ((), ())),
        precision=precision,
        preferred_element_type=jnp.float32,
    )


def iota(shape, dim):
    return lax.broadcasted_iota(jnp.int32, shape, dim)


def fetch(pairs, done):
    copies = [pltpu.make_async_copy(a, b, done.at[n]) for n, (a, b) in enumerate(pairs)]
    for copy in copies:
        copy.start()
    for copy in copies:
        copy.wait()


def rim_kernel(place_ref, x_in, b_in, c_in, even_ref, odd_ref, x_ref, b_ref, c_ref, done):
    fetch(((x_in, x_ref), (b_in, b_ref), (c_in, c_ref)), done)
    even = place_ref[3] == 0
    length, width = x_ref.shape
    for n, ref in enumerate((x_ref, b_ref, c_ref)):
        lanes = slice(n * width, (n + 1) * width)
        top = ref[0:16, :].astype(jnp.float32)[0:2]
        tail = ref[length - 16 : length, :].astype(jnp.float32)[14:16]
        even_ref[:, lanes] = jnp.where(even, tail, top)
        odd_ref[:, lanes] = jnp.where(even, top, tail)


def table_kernel(
    capacity, step_in, fade_in, speed_in, named_in, like_in, score_in, kx_in, kb_in, kc_in,
    row_ref, col_ref, kx_ref, kb_ref, kc_ref,
    step_ref, fade_ref, speed_ref, named_ref, like_ref, score_ref, done,
):
    fetch(
        (
            (step_in, step_ref), (fade_in, fade_ref), (speed_in, speed_ref), (named_in, named_ref),
            (like_in, like_ref), (score_in, score_ref), (kx_in, kx_ref), (kb_in, kb_ref), (kc_in, kc_ref),
        ),
        done,
    )
    length = row_ref.shape[1]
    for d in range(2):
        raw = step_ref[d]
        step = jnp.maximum(raw, 0.0) + jnp.log1p(jnp.exp(-jnp.abs(raw)))
        row_ref[4 + 2 * d : 6 + 2 * d, :] = step
        for h in range(2):
            k = 2 * d + h
            row_ref[k : k + 1, :] = (
                -step[h : h + 1] * speed_ref[d : d + 1, h : h + 1] + fade_ref[d][h : h + 1]
            )
    whole = row_ref[0:8, :]
    lane, line = iota(whole.shape, 1), iota(whole.shape, 0)
    ahead = behind = whole
    reach = 1
    while reach < length:
        ahead = ahead + jnp.where(lane >= reach, pltpu.roll(ahead, reach, 1), 0.0)
        behind = behind + jnp.where(lane < length - reach, pltpu.roll(behind, length - reach, 1), 0.0)
        reach *= 2
    row_ref[0:8, :] = jnp.where(line < 2, ahead, jnp.where(line < 4, behind, whole))
    experts = 32
    expert = iota((experts, length), 0)
    hit = [named_ref[k : k + 1, :] == expert for k in range(2)]
    earlier = iota((length, length), 0) < iota((length, length), 1)
    ranking = jnp.dot(
        jnp.where(hit[0] | hit[1], 1.0, 0.0).astype(jnp.bfloat16),
        jnp.where(earlier, 1.0, 0.0).astype(jnp.bfloat16),
        preferred_element_type=jnp.float32,
    )
    place = ranking + expert.astype(jnp.float32) * capacity
    for k in range(2):
        row_ref[8 + k : 9 + k, :] = jnp.sum(jnp.where(hit[k], place, 0.0), axis=0, keepdims=True)
    first = jax.nn.sigmoid(score_ref[0:1, :] - score_ref[1:2, :])
    row_ref[10:11, :] = like_ref[...] * first
    row_ref[11:12, :] = like_ref[...] * (1.0 - first)
    row_ref[12:16, :] = jnp.zeros((4, length), jnp.float32)
    col_ref[...] = jnp.zeros_like(col_ref)
    col_ref[0:16, :] = row_ref[...]
    col_ref[...] = jnp.transpose(col_ref[...])


def conv_kernel(
    place_ref, x_ref, b_ref, c_ref, even_ref, odd_ref, kx_ref, kb_ref, kc_ref, col_ref,
    message_ref, xs_ref, bs_ref, cs_ref, padded,
):
    length, width = x_ref.shape
    even = place_ref[3] == 0
    before = jnp.where(even, odd_ref[...], even_ref[...])
    after = jnp.where(even, even_ref[...], odd_ref[...])
    parts = []
    for n, (ref, taps) in enumerate(((x_ref, kx_ref), (b_ref, kb_ref), (c_ref, kc_ref))):
        lanes = slice(n * width, (n + 1) * width)
        padded[8 : 8 + length, :] = ref[...].astype(jnp.float32)
        padded[6:8, :] = before[:, lanes]
        padded[8 + length : 10 + length, :] = after[:, lanes]
        total = jnp.zeros((length, width), jnp.float32)
        for k in range(CONV):
            total = total + taps[k : k + 1, :] * padded[6 + k : 6 + k + length, :]
        parts.append(jax.nn.silu(total).astype(jnp.bfloat16))
    xs_ref[...], bs_ref[...], cs_ref[...] = parts
    x_block = parts[0].astype(jnp.float32)
    b_block = parts[1].astype(jnp.float32)
    left = iota((length, width), 1) < HD
    logs = jnp.zeros((8, width), jnp.float32)
    line = iota((8, width), 0)
    for d, last in ((0, length - 1), (1, 0)):
        weight = []
        for h in range(2):
            k = 2 * d + h
            end = col_ref[last : last + 1, k : k + 1]
            weight.append(jnp.exp(end - col_ref[:, k : k + 1]) * col_ref[:, 4 + k : 5 + k])
            high = end.astype(jnp.bfloat16).astype(jnp.float32)
            logs = jnp.where(line == 4 * d + h, high, logs)
            logs = jnp.where(line == 4 * d + 2 + h, end - high, logs)
        scaled = x_block * jnp.where(left, weight[0], weight[1])
        state = exact_dot(jnp.transpose(scaled), b_block).astype(jnp.bfloat16)
        for peer in range(message_ref.shape[0]):
            message_ref[peer, d * width : (d + 1) * width, :] = state
    for peer in range(message_ref.shape[0]):
        message_ref[peer, 2 * width :, :] = logs.astype(jnp.bfloat16)


def within(xs_ref, bs_ref, cs_ref, row_ref, col_ref):
    length, width = xs_ref.shape
    scores = dot_rows(cs_ref[...], bs_ref[...])
    x_block = xs_ref[...].astype(jnp.float32)
    to, since = iota((length, length), 0), iota((length, length), 1)
    sides = []
    for h in range(2):
        both = jnp.zeros((length, length), jnp.float32)
        for d in range(2):
            k = 2 * d + h
            seen = since <= to if d == 0 else since >= to
            passed = col_ref[:, k : k + 1] - row_ref[k : k + 1, :]
            decay = jnp.where(seen, jnp.exp(jnp.minimum(passed, 0.0)), 0.0)
            both = both + decay * row_ref[4 + k : 5 + k, :]
        sides.append(exact_dot(scores * both, x_block))
    return jnp.where(iota((length, width), 1) < HD, sides[0], sides[1])


def log_pair(tile, d):
    return [tile[4 * d + h : 4 * d + h + 1, :] + tile[4 * d + 2 + h : 4 * d + 3 + h, :] for h in range(2)]


def by_head(pair, rows):
    return jnp.where(iota((rows, 128), 0) < HD, pair[0], pair[1])


def row_kernel(place_ref, seen_ref, message_ref, near_ref, ahead_ref):
    my_x, my_z = place_ref[0], place_ref[1]
    peers, rows = seen_ref.shape[0], near_ref.shape[1]
    line = iota((8, 128), 0)
    out = []
    ahead_ref[...] = jnp.zeros_like(ahead_ref)
    for d in range(2):
        total = near = jnp.zeros((rows, 128), jnp.float32)
        far = [jnp.zeros((1, 128), jnp.float32)] * 2
        ahead = list(far)
        for k in range(peers) if d == 0 else reversed(range(peers)):
            logs = log_pair(seen_ref[k, 2 * rows :, :].astype(jnp.float32), d)
            near = jnp.where(k == my_x, total, near)
            passed = k < my_x if d == 0 else k > my_x
            state = seen_ref[k, d * rows : (d + 1) * rows, :].astype(jnp.float32)
            total = total * jnp.exp(by_head(logs, rows)) + state
            for h in range(2):
                far[h] = far[h] + logs[h]
                ahead[h] = ahead[h] + jnp.where(passed, logs[h], 0.0)
        near_ref[d] = near
        tile = jnp.zeros((8, 128), jnp.float32)
        for h in range(2):
            ahead_ref[2 * d + h : 2 * d + h + 1, :] = ahead[h]
            high = far[h].astype(jnp.bfloat16).astype(jnp.float32)
            tile = jnp.where(line == h, high, tile)
            tile = jnp.where(line == 2 + h, far[h] - high, tile)
        out.append((total, tile))
    for k in range(message_ref.shape[0]):
        onward = k > my_z
        message_ref[k, :rows, :] = jnp.where(onward, out[0][0], out[1][0]).astype(jnp.bfloat16)
        message_ref[k, rows:, :] = jnp.where(onward, out[0][1], out[1][1]).astype(jnp.bfloat16)


def mixed_kernel(
    place_ref, got_ref, near_ref, ahead_ref, xs_ref, bs_ref, cs_ref, row_ref, col_ref, valve_ref, gain_ref,
    out_ref,
):
    my_z = place_ref[1]
    peers, rows = got_ref.shape[0], near_ref.shape[1]
    length = cs_ref.shape[0]
    c_block = cs_ref[...].astype(jnp.float32)
    left = iota((length, rows), 1) < HD
    mixer = within(xs_ref, bs_ref, cs_ref, row_ref, col_ref)
    for d in range(2):
        state = jnp.zeros((rows, 128), jnp.float32)
        for k in range(peers) if d == 0 else reversed(range(peers)):
            passed = k < my_z if d == 0 else k > my_z
            logs = log_pair(got_ref[k, rows:, :].astype(jnp.float32), 0)
            onto = state * jnp.exp(by_head(logs, rows)) + got_ref[k, :rows, :].astype(jnp.float32)
            state = jnp.where(passed, onto, state)
        ahead = [ahead_ref[2 * d + h : 2 * d + h + 1, :] for h in range(2)]
        state = state * jnp.exp(by_head(ahead, rows)) + near_ref[d]
        factor = jnp.exp(
            jnp.where(left, col_ref[:, 2 * d : 2 * d + 1], col_ref[:, 2 * d + 1 : 2 * d + 2])
        )
        mixer = mixer + dot_rows(c_block, state, HIGHEST) * factor
    gated = mixer * jax.nn.silu(valve_ref[...].astype(jnp.float32))
    gated = gated * lax.rsqrt(jnp.mean(gated * gated, axis=-1, keepdims=True) + group_eps)
    mixed = (gated * gain_ref[...]).astype(jnp.bfloat16)
    for k in range(out_ref.shape[0]):
        out_ref[k] = mixed


def stream_kernel(mixed_ref, weight_ref, skip_ref, row_ref, stream_ref, out_ref):
    length, width = skip_ref.shape
    places = mixed_ref.shape[0]
    total = skip_ref[...].astype(jnp.float32)
    product = jnp.zeros((length, width), jnp.float32)
    for y in range(places):
        both = jnp.concatenate([mixed_ref[y, :length, :], mixed_ref[y, length:, :]], axis=1)
        product = product + jnp.dot(
            both, weight_ref[2 * y * width : 2 * (y + 1) * width, :], preferred_element_type=jnp.float32
        )
    stream = (total + product).astype(jnp.bfloat16)
    stream_ref[...] = stream
    blocks, places, cores, half, _ = out_ref.shape
    slot = iota((blocks * cores * half, length), 0).astype(jnp.float32)
    chosen = (row_ref[8:9, :] == slot) | (row_ref[9:10, :] == slot)
    picked = jnp.dot(
        jnp.where(chosen, 1.0, 0.0).astype(jnp.bfloat16), stream, preferred_element_type=jnp.float32
    )
    picked = picked.reshape(blocks, cores, half, width).astype(jnp.bfloat16)
    for y in range(places):
        out_ref[:, y] = picked


def expert_kernel(
    gate_in, up_in, down_in, rows_ref, gain_ref, gate_own, up_own, down_own, out_ref,
    scaled, gate_other, up_other, down_other, done,
):
    copies = [
        pltpu.make_async_copy(a, b, done.at[n])
        for n, (a, b) in enumerate(((gate_in, gate_other), (up_in, up_other), (down_in, down_other)))
    ]
    for copy in copies:
        copy.start()
    blocks, features, half, lanes = rows_ref.shape
    count = blocks * half
    squares = jnp.zeros((count, lanes), jnp.float32)
    for k in range(features):
        part = rows_ref[:, k].astype(jnp.float32).reshape(count, lanes)
        squares = squares + part * part
        at = slice(k * lanes, (k + 1) * lanes)
        scaled[:, at] = (part * gain_ref[:, at]).astype(jnp.bfloat16)
    scale = lax.rsqrt(jnp.sum(squares, axis=1, keepdims=True) / D + stream_eps)
    whole = scaled[...]
    hidden = []
    for n, (gate_ref, up_ref) in enumerate(((gate_own, up_own), (gate_other, up_other))):
        if n == 1:
            copies[0].wait()
        gate = jnp.dot(whole, gate_ref[...], preferred_element_type=jnp.float32) * scale
        if n == 1:
            copies[1].wait()
        upward = jnp.dot(whole, up_ref[...], preferred_element_type=jnp.float32) * scale
        hidden.append((jax.nn.silu(gate) * upward).astype(jnp.bfloat16))
    copies[2].wait()
    step = 2 * lanes
    for j in range(features // 2):
        at = slice(j * step, (j + 1) * step)
        part = jnp.dot(hidden[0], down_own[:, at], preferred_element_type=jnp.float32)
        part = part + jnp.dot(hidden[1], down_other[:, at], preferred_element_type=jnp.float32)
        for n in range(2):
            tile = part[:, n * lanes : (n + 1) * lanes].reshape(blocks, half, lanes)
            out_ref[:, 2 * j + n] = tile.astype(jnp.bfloat16)


def final_kernel(returned_ref, stream_ref, col_ref, out_ref):
    length, width = stream_ref.shape
    blocks, places, cores, half, _ = returned_ref.shape
    slots = blocks * cores * half
    slot = iota((length, slots), 1).astype(jnp.float32)
    answer = returned_ref[:, 0].astype(jnp.float32)
    for y in range(1, places):
        answer = answer + returned_ref[:, y].astype(jnp.float32)
    returned = answer.reshape(slots, width).astype(jnp.bfloat16)
    total = stream_ref[...].astype(jnp.float32)
    for k in range(2):
        chosen = jnp.where(col_ref[:, 8 + k : 9 + k] == slot, 1.0, 0.0).astype(jnp.bfloat16)
        picked = jnp.dot(chosen, returned, preferred_element_type=jnp.float32)
        total = total + col_ref[:, 10 + k : 11 + k] * picked
    out_ref[...] = total.astype(jnp.bfloat16)


def swapped(value):
    return lax.ppermute(value, "c", [(0, 1), (1, 0)])


def body(
    skip_stream_entering,
    unfiltered_channel_feed,
    unfiltered_state_entry,
    unfiltered_state_exit,
    final_valve_preactivation,
    increment_preactivation,
    summed_attenuation_both_ways,
    channel_fading_speed,
    channel_feed_filter,
    state_entry_filter,
    state_exit_filter,
    clustered_rescale_factor,
    final_projection_weights,
    specialist_rescale_factor,
    item_specialist_couple,
    selected_cluster_likelihood,
    selected_twin_scores_raw,
    specialist_gating_weights,
    specialist_raising_weights,
    specialist_lowering_weights,
):
    f32, bf16 = jnp.float32, jnp.bfloat16
    length, width = unfiltered_channel_feed.shape
    blocks = lax.axis_size(SP)
    peers_x, peers_y, peers_z = (lax.axis_size(a) for a in ("x", "y", "z"))
    capacity = 4 * length // blocks
    slots = blocks * capacity
    axes = [lax.axis_index(a) for a in ("x", "z", "c")]
    place = jnp.stack([*axes, axes[0] % 2]).astype(jnp.int32)

    rim = CONV // 2
    even_rim, odd_rim, *feeds = call(
        rim_kernel,
        [((rim, 3 * width), f32)] * 2 + [((length, width), bf16)] * 3,
        (place, unfiltered_channel_feed, unfiltered_state_entry, unfiltered_state_exit),
        flops=100_000,
        scratch=[pltpu.SemaphoreType.DMA((3,))],
        smem=1,
        hbm=3,
    )
    pairs = [(i, i + 1) for i in range(blocks - 1)]
    even_rim = lax.ppermute(even_rim, SP, [p for a, b in pairs[0::2] for p in ((a, b), (b, a))])
    odd_rim = lax.ppermute(odd_rim, SP, [p for a, b in pairs[1::2] for p in ((a, b), (b, a))])
    filters = (channel_feed_filter, state_entry_filter, state_exit_filter)
    heads = increment_preactivation.shape[1]
    rows, cols, *filters = call(
        functools.partial(table_kernel, capacity),
        [((16, length), f32), ((length, length), f32)] + [((CONV, width), f32)] * 3,
        (
            increment_preactivation,
            summed_attenuation_both_ways,
            channel_fading_speed,
            item_specialist_couple.T,
            selected_cluster_likelihood[None],
            selected_twin_scores_raw.T,
            *filters,
        ),
        flops=4_000_000,
        scratch=[
            pltpu.VMEM((2, heads, length), f32),
            pltpu.VMEM((2, heads, length), f32),
            pltpu.VMEM((2, heads), f32),
            pltpu.VMEM((2, length), jnp.int32),
            pltpu.VMEM((1, length), f32),
            pltpu.VMEM((2, length), f32),
            pltpu.SemaphoreType.DMA((9,)),
        ],
        hbm=9,
    )
    message, x_conv, b_conv, c_conv = call(
        conv_kernel,
        [((peers_x, 2 * width + 8, NS), bf16)] + [((length, width), bf16)] * 3,
        (place, *feeds, even_rim, odd_rim, *filters, cols),
        flops=4_000_000,
        scratch=[pltpu.VMEM((length + 16, width), f32)],
        smem=1,
    )
    seen = lax.all_to_all(message, "x", 0, 0, tiled=True)
    onward, near, ahead = call(
        row_kernel,
        [((peers_z, width + 8, NS), bf16), ((2, width, NS), f32), ((8, NS), f32)],
        (place, seen),
        smem=1,
    )
    got = lax.all_to_all(onward, "z", 0, 0, tiled=True)
    (copies,) = call(
        mixed_kernel,
        [((peers_y, length, width), bf16)],
        (
            place, got, near, ahead, x_conv, b_conv, c_conv, rows, cols,
            final_valve_preactivation, clustered_rescale_factor[None],
        ),
        smem=1,
    )
    copies, gate_own, up_own, down_own = lax.optimization_barrier(
        (
            copies,
            specialist_gating_weights[0],
            specialist_raising_weights[0],
            specialist_lowering_weights[0],
        )
    )
    others = []
    for weight in (gate_own, up_own, down_own):
        others.append(swapped(weight))
    gate_other, up_other, down_other = others
    columns = lax.all_to_all(copies, "y", 0, 0, tiled=True)
    columns, gate_other, up_other, down_other = lax.optimization_barrier(
        (columns, gate_other, up_other, down_other)
    )
    gathered = lax.all_gather(columns, "c", axis=1, tiled=True)
    half = capacity // 2
    spread = (blocks, peers_y, 2, half, width)
    everyone = (*SP, *TP)
    stream, outgoing = call(
        stream_kernel,
        [((length, width), bf16), (spread, bf16)],
        (gathered, final_projection_weights, skip_stream_entering, rows),
    )
    arrived = lax.all_to_all(
        outgoing.reshape(-1, half, width), everyone, 0, 0, tiled=True
    ).reshape(blocks, 2 * peers_y, half, width)
    (partial_out,) = call(
        expert_kernel,
        [(arrived.shape, bf16)],
        (
            gate_other, up_other, down_other, arrived, specialist_rescale_factor[None],
            gate_own, up_own, down_own,
        ),
        flops=6 * slots * gate_own.shape[1] * D,
        scratch=[
            pltpu.VMEM((slots // 2, D), bf16),
            pltpu.VMEM(gate_own.shape, bf16),
            pltpu.VMEM(up_own.shape, bf16),
            pltpu.VMEM(down_own.shape, bf16),
            pltpu.SemaphoreType.DMA((3,)),
        ],
        hbm=3,
        room=24,
    )
    returned = lax.all_to_all(
        partial_out.reshape(-1, half, width), everyone, 0, 0, tiled=True
    ).reshape(spread)
    (out,) = call(final_kernel, [((length, width), bf16)], (returned, stream, cols))
    return out


def solution(mesh):
    sizes = dict(mesh.shape)
    torus = Mesh(mesh.devices.reshape(8, 4, sizes["tp"] // 2, 2), ("z", "x", "y", "c"))
    return jax.shard_map(
        body,
        mesh=torus,
        in_specs=(
            P(SP, TP),
            P(SP, TP),
            P(SP, TP),
            P(SP, TP),
            P(SP, TP),
            P(None, TP, SP),
            P(None, TP, SP),
            P(None, TP),
            P(None, TP),
            P(None, TP),
            P(None, TP),
            P(TP),
            P(None, TP),
            P(),
            P(SP, None),
            P(SP),
            P(SP, None),
            P(SP, None, TP),
            P(SP, None, TP),
            P(SP, TP, None),
        ),
        out_specs=P(SP, TP),
        check_vma=False,
    )
```
